512 devices in a mesh: grp: 2 (over y), dp: 8 (over x), kv: 16 (over z), tp: 2 (over core).
Axes of the slice: x: 8, y: 2, z: 16, core: 2. Of those that a mesh axis runs over, the one named last changes fastest.
The devices are a block of a 8x8x16 slice.
Arguments:
- tokens: bfloat16 [128, 2048], P(('grp', 'dp'), 'kv'), parts along dimension 0, may hold values from -110 to 110
- attend_gain: float32 [2048], P('kv'), may hold values from 0.1 to 1.9
- query_weight: bfloat16 [2048, 2048], P('kv', 'tp'), may hold values from -0.125 to 0.125
- cache_keys: bfloat16 [128, 6144, 2, 128], P(('grp', 'dp'), 'kv', 'tp'), parts along dimension 0, may hold values from -1600 to 1600
- cache_values: bfloat16 [128, 6144, 2, 128], P(('grp', 'dp'), 'kv', 'tp'), parts along dimension 0, may hold values from -6 to 6
- head_lambda: float32 [16], P('tp'), may hold values from 0.3 to 0.8
- head_gain: float32 [128], replicated, may hold values from 0.1 to 1.9
- output_weight: bfloat16 [2048, 2048], P('tp', 'kv'), may hold values from -0.125 to 0.125
- mixer_gain: float32 [2048], P('kv'), may hold values from 0.1 to 1.9
- gate_weight: bfloat16 [2048, 5632], P('kv', 'tp'), may hold values from -0.125 to 0.125
- up_weight: bfloat16 [2048, 5632], P('kv', 'tp'), may hold values from -0.125 to 0.125
- down_weight: bfloat16 [5632, 2048], P('tp', 'kv'), may hold values from -0.078125 to 0.078125
Outputs:
- layer_out: bfloat16 [128, 2048], P(('grp', 'dp'), 'kv'), parts along dimension 0
The draws below stay inside these ranges and needn't reach their ends.
There are 2 independent parts, one for each index of `grp`. The reference program is written for one: setup_inputs(seed, part) draws one part's arguments, and reference() takes and returns one part's arrays. A program takes and returns all parts, laid end to end along the dimension named above; an argument that names none is the same for every part. Nothing has to cross between parts.
All inputs are finite; a program needn't handle non-finite values.
Results may differ from the reference program's by a relative error of at most 0.025.
Values may be sent and summed in bfloat16 or wider, within the bound.
No kernel may reach another device: no remote copies, remote signals or barrier semaphores. Data moves between devices by JAX's collectives and lax.ppermute only.
A program may use at most 64 MiB of HBM per device.

```python
import jax
import jax.numpy as jnp
from jax import lax

D = 2048
H = 16
KVH = 2
HD = 64
VD = 128
FF = 5632
GROUP = 8
BATCH = 64
CTX = 6144
N_TP = 2


def draw_tokens(key, part):
    columns = jnp.arange(D, dtype=jnp.float32)
    column_scale = 0.4 * 10.0 ** (columns / D)
    roughness = jax.random.uniform(jax.random.fold_in(key, 1), (D,), jnp.float32, 0.5, 1.5)
    values = jnp.clip(jax.random.normal(key, (BATCH, D), jnp.float32), -6.0, 6.0)
    return (values * column_scale * roughness).astype(jnp.bfloat16)


def draw_cache_keys(key, part):
    drawn = jnp.clip(jax.random.normal(key, (BATCH, CTX, KVH, 2 * HD), jnp.float32), -6.0, 6.0) * 1.7
    return drawn.astype(jnp.bfloat16)


def levels(key, dims, split, smallest, high):
    level = 1.0
    for dim, parts in split:
        draws = jax.random.uniform(jax.random.fold_in(jax.random.fold_in(key, 6), dim), (parts,), jnp.float32, smallest / len(split), high / len(split))
        level = level * jnp.repeat(jnp.exp(draws), dims[dim] // parts).reshape((-1,) + (1,) * (len(dims) - 1 - dim))
    return level


def noise(stream_key, shape, deviation, most, cuts=(), kind=jnp.bfloat16):
    values = jax.random.normal(stream_key, shape, jnp.float32) * deviation
    if len(cuts) > 0:
        values = levels(stream_key, shape, cuts, -0.22, 0.18) * values
    return jnp.clip(values, min=-most, max=most).astype(kind)


def setup_inputs(seed: int = 0, part: int = 0) -> dict:
    key_list = jax.random.split(jax.random.key(seed), 13)
    own_keys = jax.random.split(jax.random.fold_in(key_list[12], part), 13)
    return {
        "tokens": draw_tokens(jax.random.fold_in(jax.random.fold_in(key_list[12], part), 71), part),
        "attend_gain": jnp.clip(1.0 + 0.18 * jax.random.normal(key_list[1], (D,), jnp.float32), 0.1, 1.9),
        "query_weight": noise(key_list[2], (D, H * 2 * HD), D ** -0.5, 0.125, ((0, 16), (1, 2))),
        "cache_keys": draw_cache_keys(jax.random.fold_in(jax.random.fold_in(key_list[12], part), 71), part),
        "cache_values": noise(own_keys[4], (BATCH, CTX, KVH, VD), 1.0, 6.0, ((0, 8), (1, 16), (2, 2))),
        "head_lambda": jnp.clip(0.3 + 0.5 * jax.random.uniform(key_list[5], (H,), jnp.float32) ** levels(key_list[5], (H,), ((0, 2),), -0.2, 0.2), 0.3, 0.8),
        "head_gain": jnp.clip(1.0 + 0.18 * jax.random.normal(key_list[6], (VD,), jnp.float32), 0.1, 1.9),
        "output_weight": noise(key_list[7], (H * VD, D), (H * VD) ** -0.5, 0.125, ((0, 2), (1, 16))),
        "mixer_gain": jnp.clip(1.0 + 0.18 * jax.random.normal(key_list[8], (D,), jnp.float32), 0.1, 1.9),
        "gate_weight": noise(key_list[9], (D, FF), D ** -0.5, 0.125, ((0, 16), (1, 2))),
        "up_weight": noise(key_list[10], (D, FF), D ** -0.5, 0.125, ((0, 16), (1, 2))),
        "down_weight": noise(key_list[11], (FF, D), FF ** -0.5, 0.078125, ((0, 2), (1, 16))),
    }


ROPE_BASE = 500000.0
EPSILON = 1e-06
KEEP_SCALE = 0.8

def rotate(query, position):
    half_dim = query.shape[-1] // 2
    frequency = ROPE_BASE ** (-jnp.arange(half_dim, dtype=jnp.float32) * 2.0 / query.shape[-1])
    angles = position * frequency
    cosine_part = jnp.cos(angles)
    sine_part = jnp.sin(angles)
    first_half = query[..., :half_dim]
    second_half = query[..., half_dim:]
    return jnp.concatenate([first_half * cosine_part - second_half * sine_part, second_half * cosine_part + first_half * sine_part], axis=-1)

def group_sum(left, right, pieces):
    width = left.shape[1] // pieces
    running = jnp.zeros((left.shape[0], right.shape[1]), jnp.float32)
    for block_index in range(pieces):
        product = jnp.dot(left[:, block_index * width:(block_index + 1) * width], right[block_index * width:(block_index + 1) * width], preferred_element_type=jnp.float32)
        rounded = lax.optimization_barrier(product.astype(jnp.bfloat16))
        running = running + rounded.astype(jnp.float32)
    return running

def attend(arrays):
    query_row, key_row, value_row = arrays
    scores = jnp.einsum('kgcd,pkcd->kgcp', query_row.astype(jnp.float32), key_row.astype(jnp.float32)) * HD ** (-0.5)
    row_max = lax.optimization_barrier(jnp.max(scores, axis=-1, keepdims=True))
    exponent = jnp.exp(scores - row_max)
    row_total = lax.optimization_barrier(jnp.sum(exponent, axis=-1))
    rounded = lax.optimization_barrier(exponent.astype(jnp.bfloat16))
    weighted = jnp.einsum('kgcp,pke->kgce', rounded.astype(jnp.float32), value_row.astype(jnp.float32))
    return weighted / row_total[..., None]

def reference(tokens, attend_gain, query_weight, cache_keys, cache_values, head_lambda, head_gain, output_weight, mixer_gain, gate_weight, up_weight, down_weight):
    tok_float = tokens.astype(jnp.float32)
    scaled = (tok_float * attend_gain).astype(jnp.bfloat16)
    attend_scale = lax.rsqrt(lax.optimization_barrier(jnp.mean(tok_float * tok_float, axis=1, keepdims=True)) + EPSILON)
    query = attend_scale * jnp.dot(scaled, query_weight, preferred_element_type=jnp.float32)
    query = rotate(query.reshape(BATCH, KVH, GROUP, 2, HD), jnp.asarray(CTX, jnp.float32))
    query = lax.optimization_barrier(query.astype(jnp.bfloat16))
    key_block = cache_keys.reshape(BATCH, CTX, KVH, 2, HD)
    averaged = lax.map(attend, (query, key_block, cache_values))
    lambda_grid = head_lambda.reshape(KVH, GROUP)[None, :, :, None]
    difference = averaged[:, :, :, 0] - lambda_grid * averaged[:, :, :, 1]
    normed = difference * lax.rsqrt(lax.optimization_barrier(jnp.mean(difference * difference, axis=-1, keepdims=True)) + EPSILON)
    heads_out = (normed * head_gain * KEEP_SCALE).astype(jnp.bfloat16).reshape(BATCH, H * VD)
    middle = (tok_float + group_sum(heads_out, output_weight, N_TP)).astype(jnp.bfloat16)
    mid_float = middle.astype(jnp.float32)
    mixer_in = (mid_float * mixer_gain).astype(jnp.bfloat16)
    mixer_scale = lax.rsqrt(lax.optimization_barrier(jnp.mean(mid_float * mid_float, axis=1, keepdims=True)) + EPSILON)
    gate = mixer_scale * jnp.dot(mixer_in, gate_weight, preferred_element_type=jnp.float32)
    up_value = mixer_scale * jnp.dot(mixer_in, up_weight, preferred_element_type=jnp.float32)
    hidden = (jax.nn.silu(gate) * up_value).astype(jnp.bfloat16)
    mixed = group_sum(hidden, down_weight, N_TP)
    return (mid_float + mixed).astype(jnp.bfloat16)
```

```python
import jax
import jax.numpy as jnp
from jax import lax
from jax.sharding import PartitionSpec as P

HD = 64
VD = 128
LANES = 128

ROPE_BASE = 500000.0
EPSILON = 1e-06
KEEP_SCALE = 0.8


def split(value, terms):
    parts = []
    for _ in range(terms):
        part = value.astype(jnp.bfloat16)
        parts.append(part)
        value = value - part.astype(jnp.float32)
    return parts


def rotate(query, position):
    half_dim = query.shape[-1] // 2
    frequency = ROPE_BASE ** (-jnp.arange(half_dim, dtype=jnp.float32) * 2.0 / query.shape[-1])
    angles = position * frequency
    cosine_part = jnp.cos(angles)
    sine_part = jnp.sin(angles)
    first_half = query[..., :half_dim]
    second_half = query[..., half_dim:]
    return jnp.concatenate(
        [
            first_half * cosine_part - second_half * sine_part,
            second_half * cosine_part + first_half * sine_part,
        ],
        axis=-1,
    )


def pack_softmax(row_max, row_total, weighted):
    terms = split(row_max, 3) + split(row_total, 2)
    extra = jnp.stack(terms + [jnp.zeros_like(terms[0])] * (8 - len(terms)))
    return jnp.concatenate([weighted.astype(jnp.bfloat16), extra], axis=0)


def combine_softmax(parts):
    rows = parts.shape[1] - 8
    extra = parts[:, rows:].astype(jnp.float32)
    maxima = extra[:, 0] + extra[:, 1] + extra[:, 2]
    totals = extra[:, 3] + extra[:, 4]
    joint = jnp.max(maxima, axis=0)
    factor = jnp.exp(maxima - joint)
    total = jnp.sum(totals * factor, axis=0)
    weighted = jnp.sum(parts[:, :rows].astype(jnp.float32) * factor[:, :, None], axis=0)
    return joint, total, weighted


def on_device(
    tokens,
    attend_gain,
    query_weight,
    cache_keys,
    cache_values,
    head_lambda,
    head_gain,
    output_weight,
    mixer_gain,
    gate_weight,
    up_weight,
    down_weight,
):
    kv_size = lax.axis_size("kv")
    seq_rows, features_here = tokens.shape
    features = features_here * kv_size
    heads_here = head_lambda.shape[0]
    kv_local = cache_keys.shape[2]
    group_size = heads_here // kv_local
    positions = cache_keys.shape[1]
    context = positions * kv_size
    rows = seq_rows * heads_here * 2
    strided = [list(range(k, kv_size, 2)) for k in range(2)]
    pairs = [[k, k + 1] for k in range(0, kv_size, 2)]

    def to_all(array, groups, count):
        copies = jnp.broadcast_to(array[None], (count, *array.shape))
        return lax.all_to_all(copies, "kv", 0, 0, axis_index_groups=groups, tiled=True)

    tok_float = tokens.astype(jnp.float32)
    scaled = (tok_float * attend_gain).astype(jnp.bfloat16)
    partial_query = jnp.dot(scaled, query_weight, preferred_element_type=jnp.float32)
    squares = jnp.sum(tok_float * tok_float, axis=1, keepdims=True)
    high, low = split(squares, 2)
    sent = jnp.concatenate(
        [partial_query.astype(jnp.bfloat16), high, low, jnp.zeros((seq_rows, LANES - 2), jnp.bfloat16)],
        axis=1,
    )
    summed = to_all(sent, None, kv_size).astype(jnp.float32).sum(axis=0)
    width = partial_query.shape[1]
    total_squares = summed[:, width : width + 1] + summed[:, width + 1 : width + 2]
    attend_scale = lax.rsqrt(total_squares / features + EPSILON)
    query = (attend_scale * summed[:, :width]).reshape(seq_rows, kv_local, group_size, 2, HD)
    query = rotate(query, jnp.asarray(context, jnp.float32)).astype(jnp.bfloat16)
    key_block = cache_keys.reshape(seq_rows, positions, kv_local, 2, HD)
    scores = jnp.einsum(
        "skgcd,spkcd->skgcp", query, key_block, preferred_element_type=jnp.float32
    ) * HD ** (-0.5)
    row_max = jnp.max(scores, axis=-1)
    exponent = jnp.exp(scores - row_max[..., None])
    row_total = jnp.sum(exponent, axis=-1)
    weighted = jnp.einsum(
        "skgcp,spke->skgce",
        exponent.astype(jnp.bfloat16),
        cache_values,
        preferred_element_type=jnp.float32,
    )
    part = pack_softmax(row_max.reshape(rows), row_total.reshape(rows), weighted.reshape(rows, VD))
    part = pack_softmax(*combine_softmax(to_all(part, strided, kv_size // 2)))
    part = lax.all_gather(part, "kv", axis_index_groups=pairs)
    _, row_total, weighted = combine_softmax(part)
    averaged = (weighted / row_total[:, None]).reshape(seq_rows, heads_here, 2, VD)
    difference = averaged[:, :, 0] - head_lambda[None, :, None] * averaged[:, :, 1]
    normed = difference * lax.rsqrt(
        jnp.mean(difference * difference, axis=-1, keepdims=True) + EPSILON
    )
    heads_out = (
        (normed * head_gain * KEEP_SCALE).astype(jnp.bfloat16).reshape(seq_rows, heads_here * VD)
    )
    attended = jnp.dot(heads_out, output_weight, preferred_element_type=jnp.float32)
    attended = lax.all_gather(attended.astype(jnp.bfloat16), "tp").astype(jnp.float32).sum(axis=0)
    middle = (tok_float + attended).astype(jnp.bfloat16)
    mid_float = middle.astype(jnp.float32)
    mixer_in = (mid_float * mixer_gain).astype(jnp.bfloat16)
    gate_part = jnp.dot(mixer_in, gate_weight, preferred_element_type=jnp.float32)
    up_part = jnp.dot(mixer_in, up_weight, preferred_element_type=jnp.float32)
    hidden_here = gate_part.shape[1]
    share = hidden_here // kv_size
    padded = -(-(2 * share + 2) // LANES) * LANES
    high, low = split(jnp.sum(mid_float * mid_float, axis=1, keepdims=True), 2)

    def cut(array):
        return array.astype(jnp.bfloat16).reshape(seq_rows, kv_size, share).transpose(1, 0, 2)

    def copies(array, lanes):
        return jnp.broadcast_to(array[None], (kv_size, seq_rows, lanes))

    sent = jnp.concatenate(
        [
            cut(gate_part),
            cut(up_part),
            copies(high, 1),
            copies(low, 1),
            jnp.zeros((kv_size, seq_rows, padded - 2 * share - 2), jnp.bfloat16),
        ],
        axis=2,
    )
    summed = lax.all_to_all(sent, "kv", 0, 0, tiled=True).astype(jnp.float32).sum(axis=0)
    total_squares = summed[:, 2 * share : 2 * share + 1] + summed[:, 2 * share + 1 : 2 * share + 2]
    mixer_scale = lax.rsqrt(total_squares / features + EPSILON)
    gate = mixer_scale * summed[:, :share]
    up = mixer_scale * summed[:, share : 2 * share]
    hidden_share = (jax.nn.silu(gate) * up).astype(jnp.bfloat16)
    hidden = to_all(hidden_share, None, kv_size).transpose(1, 0, 2).reshape(seq_rows, hidden_here)
    projected = jnp.dot(hidden, down_weight, preferred_element_type=jnp.float32)
    mixed = lax.all_gather(projected.astype(jnp.bfloat16), "tp").astype(jnp.float32).sum(axis=0)
    return (mid_float + mixed).astype(jnp.bfloat16)


def solution(mesh):
    return jax.shard_map(
        on_device,
        mesh=mesh,
        in_specs=(
            P(("grp", "dp"), "kv"),
            P("kv"),
            P("kv", "tp"),
            P(("grp", "dp"), "kv", "tp", None),
            P(("grp", "dp"), "kv", "tp", None),
            P("tp"),
            P(),
            P("tp", "kv"),
            P("kv"),
            P("kv", "tp"),
            P("kv", "tp"),
            P("tp", "kv"),
        ),
        out_specs=P(("grp", "dp"), "kv"),
        check_vma=False,
    )
```

```python
import functools

import jax
import jax.numpy as jnp
import numpy as np
from jax import lax
from jax.experimental import pallas as pl
from jax.experimental.pallas import tpu as pltpu
from jax.sharding import PartitionSpec as P

HD = 64
VD = 128
LANES = 128
EXTRA = 8

ROPE_BASE = 500000.0
EPSILON = 1e-06
KEEP_SCALE = 0.8
F32 = jnp.float32
BF16 = jnp.bfloat16


def split(value, terms):
    parts = []
    for _ in range(terms):
        part = value.astype(BF16).astype(F32)
        parts.append(part)
        value = value - part
    return parts


def lanes_of(columns, rows, width):
    lane = lax.broadcasted_iota(jnp.int32, (rows, width), 1)
    out = jnp.zeros((rows, width), F32)
    for k, column in enumerate(columns):
        out = jnp.where(lane == k, column, out)
    return out


def rows_of(lines, width):
    row = lax.broadcasted_iota(jnp.int32, (EXTRA, width), 0)
    out = jnp.zeros((EXTRA, width), F32)
    for k, line in enumerate(lines):
        out = jnp.where(row == k, line, out)
    return out


def turned(rows):
    pad = jnp.zeros((LANES - rows.shape[0], LANES), F32)
    return jnp.concatenate([rows, pad], axis=0).T


def query_kernel(tokens, gain, weight, out):
    tok = tokens[...].astype(F32)
    scaled = (tok * gain[...]).astype(BF16)
    partial = jnp.dot(scaled, weight[...], preferred_element_type=F32)
    squares = jnp.sum(tok * tok, axis=1, keepdims=True)
    extra = lanes_of(split(squares, 2), tok.shape[0], LANES)
    sent = jnp.concatenate([partial.astype(BF16), extra.astype(BF16)], axis=1)
    for k in range(out.shape[0]):
        out[k] = sent


def attend_kernel(features, parts, table, keys, values, out, turned_query):
    count, seq_rows, width = parts.shape
    width -= LANES
    total = parts[0].astype(F32)
    for k in range(1, count):
        total = total + parts[k].astype(F32)
    squares = total[:, width : width + 1] + total[:, width + 1 : width + 2]
    scale = lax.rsqrt(squares / features + EPSILON)
    heads = width // (2 * HD)
    lane = lax.broadcasted_iota(jnp.int32, (seq_rows, LANES), 1)
    first = lane % HD < HD // 2
    cosine, sine = table[0:1], table[1:2]
    for g in range(heads):
        part = total[:, g * LANES : (g + 1) * LANES] * scale
        other = jnp.where(first, pltpu.roll(part, LANES - HD // 2, 1), pltpu.roll(part, HD // 2, 1))
        turned_query[g * seq_rows : (g + 1) * seq_rows] = part * cosine + other * sine
    map_zero = lax.broadcasted_iota(jnp.int32, (heads, LANES), 1) < HD
    maxima, totals = [], []
    for s in range(seq_rows):
        part = turned_query[pl.ds(s, heads, stride=seq_rows)]
        both = jnp.concatenate(
            [jnp.where(map_zero, part, 0.0), jnp.where(map_zero, 0.0, part)], axis=0
        ).astype(BF16)
        scores = lax.dot_general(
            both, keys[s], (((1,), (1,)), ((), ())), preferred_element_type=F32
        ) * HD ** (-0.5)
        row_max = jnp.max(scores, axis=1, keepdims=True)
        exponent = jnp.exp(scores - row_max)
        maxima.append(row_max)
        totals.append(jnp.sum(exponent, axis=1, keepdims=True))
        weighted = jnp.dot(exponent.astype(BF16), values[s], preferred_element_type=F32)
        out[s * 2 * heads : (s + 1) * 2 * heads] = weighted.astype(BF16)
    rows = 2 * heads * seq_rows
    both = lanes_of(
        [jnp.concatenate(maxima, axis=0), jnp.concatenate(totals, axis=0)], rows, LANES
    ).T
    lines = split(both[0:1], 3) + split(both[1:2], 2)
    out[rows:] = rows_of(lines, rows).astype(BF16)


def pair_kernel(odd, parts, out, joined):
    rows = parts.shape[1] - EXTRA
    half = rows // 2
    extra = [parts[k, rows:].astype(F32) for k in range(2)]
    maxima = [e[0:1] + e[1:2] + e[2:3] for e in extra]
    totals = [e[3:4] + e[4:5] for e in extra]
    joint = jnp.maximum(maxima[0], maxima[1])
    factors = [jnp.exp(m - joint) for m in maxima]
    total = totals[0] * factors[0] + totals[1] * factors[1]
    columns = turned(rows_of(factors, rows))
    joined[...] = (
        parts[0, :rows].astype(F32) * columns[:, 0:1] + parts[1, :rows].astype(F32) * columns[:, 1:2]
    )
    own = jnp.where(odd[...] > 0, joined[half:], joined[:half]).astype(BF16)
    lines = rows_of(split(joint, 3) + split(total, 2), rows).astype(BF16)
    sent = jnp.concatenate([own, lines], axis=0)
    for k in range(out.shape[0]):
        out[k] = sent


def heads_kernel(parts, lambdas, gain, weight, out, normed):
    count = parts.shape[0] // 2
    half = parts.shape[1] - EXTRA
    rows = 2 * half
    heads = lambdas.shape[1]
    seq_rows = rows // (2 * heads)
    square = (heads, heads)
    diagonal = lax.broadcasted_iota(jnp.int32, square, 0) == lax.broadcasted_iota(jnp.int32, square, 1)
    lambda_column = jnp.sum(jnp.where(diagonal, lambdas[...], 0.0), axis=1, keepdims=True)
    extra = [parts[2 * k, half:].astype(F32) for k in range(count)]
    maxima = jnp.concatenate([e[0:1] + e[1:2] + e[2:3] for e in extra], axis=0)
    totals = jnp.concatenate([e[3:4] + e[4:5] for e in extra], axis=0)
    joint = jnp.max(maxima, axis=0, keepdims=True)
    factors = jnp.exp(maxima - joint)
    factors = factors / jnp.sum(totals * factors, axis=0, keepdims=True)
    columns = turned(factors)
    for s in range(seq_rows):
        block = slice(s * 2 * heads, (s + 1) * 2 * heads)
        which, row = divmod(s * 2 * heads, half)
        averaged = jnp.zeros((2 * heads, VD), F32)
        for k in range(count):
            part = parts[2 * k + which, row : row + 2 * heads].astype(F32)
            averaged = averaged + part * columns[block, k : k + 1]
        difference = averaged[:heads] - lambda_column * averaged[heads:]
        mean = jnp.mean(difference * difference, axis=1, keepdims=True)
        normed[s * heads : (s + 1) * heads] = (
            difference * lax.rsqrt(mean + EPSILON) * gain[...] * KEEP_SCALE
        )
    heads_out = jnp.concatenate(
        [normed[pl.ds(g, seq_rows, stride=heads)].astype(BF16) for g in range(heads)], axis=1
    )
    out[...] = jnp.dot(heads_out, weight[...], preferred_element_type=F32).astype(BF16)


def window(array, start, width):
    low = start // LANES * LANES
    tiles = -(-(start - low + width) // LANES) * LANES
    part = array[:, low : low + tiles]
    if start > low:
        part = pltpu.roll(part, tiles - (start - low), 1)
    return part


def gate_kernel(attended, tokens, gain, gate_weight, up_weight, out, middle):
    seq_rows = tokens.shape[0]
    total = attended[:seq_rows].astype(F32) + attended[seq_rows:].astype(F32)
    mid = (tokens[...].astype(F32) + total).astype(BF16)
    middle[...] = mid
    mid = mid.astype(F32)
    mixer_in = (mid * gain[...]).astype(BF16)
    gate = jnp.dot(mixer_in, gate_weight[...], preferred_element_type=F32)
    up = jnp.dot(mixer_in, up_weight[...], preferred_element_type=F32)
    squares = jnp.sum(mid * mid, axis=1, keepdims=True)
    high, low = split(squares, 2)
    count, _, width = out.shape
    share = gate.shape[1] // count
    lane = lax.broadcasted_iota(jnp.int32, (seq_rows, width), 1)
    for k in range(count):
        parts = []
        for array in (gate, up):
            part = window(array, k * share, share)[:, :width]
            if part.shape[1] < width:
                pad = jnp.zeros((seq_rows, width - part.shape[1]), F32)
                part = jnp.concatenate([part, pad], axis=1)
            parts.append(part)
        both = jnp.where(lane < share, parts[0], pltpu.roll(parts[1], share, 1))
        both = jnp.where(lane == 2 * share, high, both)
        both = jnp.where(lane == 2 * share + 1, low, both)
        out[k] = both.astype(BF16)


def hidden_kernel(features, parts, out):
    count, _, width = parts.shape
    share = out.shape[2]
    total = parts[0].astype(F32)
    for k in range(1, count):
        total = total + parts[k].astype(F32)
    squares = total[:, 2 * share : 2 * share + 1] + total[:, 2 * share + 1 : 2 * share + 2]
    scale = lax.rsqrt(squares / features + EPSILON)
    scaled = total * scale
    gate = scaled[:, :share]
    up = pltpu.roll(scaled, width - share, 1)[:, :share]
    hidden = (gate / (1.0 + jnp.exp(-gate)) * up).astype(BF16)
    for k in range(count):
        out[k] = hidden


def down_kernel(hidden, weight, out):
    count, seq_rows, share = hidden.shape
    total = jnp.zeros(out.shape, F32)
    for k in range(count):
        total = total + jnp.dot(
            hidden[k], weight[k * share : (k + 1) * share], preferred_element_type=F32
        )
    out[...] = total.astype(BF16)


def final_kernel(parts, middle, out):
    seq_rows = middle.shape[0]
    mixed = parts[:seq_rows].astype(F32) + parts[seq_rows:].astype(F32)
    out[...] = (middle[...].astype(F32) + mixed).astype(BF16)


def rotation(context):
    frequency = ROPE_BASE ** (-np.arange(HD // 2) * 2.0 / HD)
    angles = context * frequency
    cosine, sine = np.cos(angles), np.sin(angles)
    table = [np.tile(cosine, LANES // (HD // 2)), np.tile(np.concatenate([-sine, sine]), LANES // HD)]
    return np.stack(table + [np.zeros(LANES)] * 6).astype(np.float32)


def on_device(
    tokens,
    attend_gain,
    query_weight,
    cache_keys,
    cache_values,
    head_lambda,
    head_gain,
    output_weight,
    mixer_gain,
    gate_weight,
    up_weight,
    down_weight,
):
    kv_size = lax.axis_size("kv")
    seq_rows, features_here = tokens.shape
    features = features_here * kv_size
    heads = head_lambda.shape[0]
    positions = cache_keys.shape[1]
    rows = 2 * heads * seq_rows
    share = gate_weight.shape[1] // kv_size
    padded = -(-(2 * share + 2) // LANES) * LANES
    pairs = [[k, k + 1] for k in range(0, kv_size, 2)]
    odd = jnp.broadcast_to((lax.axis_index("kv") & 1).astype(F32), (1, VD))
    tokens, odd = lax.optimization_barrier((tokens, odd))
    keys = cache_keys.reshape(seq_rows, positions, 2 * HD)
    values = cache_values.reshape(seq_rows, positions, VD)

    def call(kernel, shapes, *arguments, scratch=(), last=False):
        spec = pl.BlockSpec(memory_space=pltpu.VMEM)
        space = jax.ShapeDtypeStruct if last else pltpu.VMEM
        outs = tuple(space(shape, BF16) for shape in shapes)
        results = pl.pallas_call(
            kernel,
            out_shape=outs,
            in_specs=[spec] * len(arguments),
            out_specs=(spec,) * len(outs),
            scratch_shapes=list(scratch),
        )(*(pltpu.with_memory_space_constraint(a, pltpu.VMEM) for a in arguments))
        return results[0] if len(outs) == 1 else results

    def exchange(array):
        return lax.all_to_all(array, "kv", 0, 0, tiled=True)

    sent = call(
        query_kernel,
        ((kv_size, seq_rows, query_weight.shape[1] + LANES),),
        tokens,
        attend_gain[None],
        query_weight,
    )
    part = call(
        functools.partial(attend_kernel, features),
        ((rows + EXTRA, VD),),
        exchange(sent),
        jnp.asarray(rotation(positions * kv_size)),
        keys,
        values,
        scratch=[pltpu.VMEM((heads * seq_rows, LANES), F32)],
    )
    part = lax.all_gather(part, "kv", axis_index_groups=pairs)
    sent = call(
        pair_kernel,
        ((kv_size, rows // 2 + EXTRA, VD),),
        odd,
        part,
        scratch=[pltpu.VMEM((rows, VD), F32)],
    )
    attended = call(
        heads_kernel,
        ((seq_rows, features_here),),
        exchange(sent),
        head_lambda[None],
        head_gain[None],
        output_weight,
        scratch=[pltpu.VMEM((heads * seq_rows, VD), F32)],
    )
    sent, middle = call(
        gate_kernel,
        ((kv_size, seq_rows, padded), (seq_rows, features_here)),
        lax.all_gather(attended, "tp", tiled=True),
        tokens,
        mixer_gain[None],
        gate_weight,
        up_weight,
    )
    sent = call(
        functools.partial(hidden_kernel, features),
        ((kv_size, seq_rows, share),),
        exchange(sent),
    )
    projected = call(down_kernel, ((seq_rows, features_here),), exchange(sent), down_weight)
    return call(
        final_kernel,
        ((seq_rows, features_here),),
        lax.all_gather(projected, "tp", tiled=True),
        middle,
        last=True,
    )


def solution(mesh):
    return jax.shard_map(
        on_device,
        mesh=mesh,
        in_specs=(
            P(("grp", "dp"), "kv"),
            P("kv"),
            P("kv", "tp"),
            P(("grp", "dp"), "kv", "tp", None),
            P(("grp", "dp"), "kv", "tp", None),
            P("tp"),
            P(),
            P("tp", "kv"),
            P("kv"),
            P("kv", "tp"),
            P("kv", "tp"),
            P("tp", "kv"),
        ),
        out_specs=P(("grp", "dp"), "kv"),
        check_vma=False,
    )
```

```python
import functools

import jax
import jax.numpy as jnp
import numpy as np
from jax import lax
from jax.experimental import pallas as pl
from jax.experimental.pallas import tpu as pltpu
from jax.sharding import PartitionSpec as P

HD = 64
VD = 128
LANES = 128
EXTRA = 8

KERNEL_VMEM = 8 << 20

ROPE_BASE = 500000.0
EPSILON = 1e-06
KEEP_SCALE = 0.8
F32 = jnp.float32
BF16 = jnp.bfloat16


def split(value, terms):
    parts = []
    for _ in range(terms):
        part = value.astype(BF16).astype(F32)
        parts.append(part)
        value = value - part
    return parts


def lanes_of(columns, rows, width):
    lane = lax.broadcasted_iota(jnp.int32, (rows, width), 1)
    out = jnp.zeros((rows, width), F32)
    for k, column in enumerate(columns):
        out = jnp.where(lane == k, column, out)
    return out


def rows_of(lines, width):
    row = lax.broadcasted_iota(jnp.int32, (EXTRA, width), 0)
    out = jnp.zeros((EXTRA, width), F32)
    for k, line in enumerate(lines):
        out = jnp.where(row == k, line, out)
    return out


def turned(rows):
    pad = jnp.zeros((LANES - rows.shape[0], LANES), F32)
    return jnp.concatenate([rows, pad], axis=0).T


def query_kernel(tokens, gain, weight, table, out, table_here, tokens_here, gain_here, weight_here, semaphores):
    copies = [
        pltpu.make_async_copy(source, target, semaphores.at[k])
        for k, (source, target) in enumerate(
            (
                (weight, weight_here),
                (tokens, tokens_here),
                (gain, gain_here),
                (table, table_here),
            )
        )
    ]
    for copy in copies:
        copy.start()
    for copy in copies:
        copy.wait()
    tok = tokens_here[...].astype(F32)
    scaled = (tok * gain_here[...]).astype(BF16)
    partial = jnp.dot(scaled, weight_here[...], preferred_element_type=F32)
    squares = jnp.sum(tok * tok, axis=1, keepdims=True)
    width = partial.shape[1]
    out[:, :width] = partial.astype(BF16)
    out[:, width:] = lanes_of(split(squares, 2), tok.shape[0], LANES).astype(BF16)


def halves_kernel(odd, parts, out):
    total = parts[0].astype(F32) + parts[1].astype(F32)
    half = (total.shape[1] - LANES) // 2
    own = jnp.where(odd[:, :1] > 0, total[:, half : 2 * half], total[:, :half])
    extra = total[:, 2 * half :]
    squares = extra[:, 0:1] + extra[:, 1:2]
    extra = lanes_of(split(squares, 2), total.shape[0], LANES)
    sent = jnp.concatenate([own, extra], axis=1).astype(BF16)
    for k in range(out.shape[0]):
        out[k] = sent


def attend_kernel(features, fetched, parts, table, keys, values, *refs):
    sources, refs = refs[:fetched], refs[fetched:]
    out, targets, refs = refs[0], refs[1 : 1 + fetched], refs[1 + fetched :]
    values_here, turned_query, score_rows, semaphores = refs
    copies = [
        pltpu.make_async_copy(source, target, semaphores.at[k])
        for k, (source, target) in enumerate(zip((values, *sources), (values_here, *targets)))
    ]
    for copy in copies:
        copy.start()
    count, seq_rows, half = parts.shape
    half -= LANES
    sums = []
    for odd in range(2):
        total = parts[odd].astype(F32)
        for k in range(odd + 2, count, 2):
            total = total + parts[k].astype(F32)
        sums.append(total)
    squares = sums[0][:, half : half + 1] + sums[0][:, half + 1 : half + 2]
    scale = lax.rsqrt(squares / features + EPSILON)
    heads = 2 * half // (2 * HD)
    lane = lax.broadcasted_iota(jnp.int32, (seq_rows, LANES), 1)
    first = lane % HD < HD // 2
    cosine, sine = table[0:1], table[1:2]
    for g in range(heads):
        side, at = divmod(g * LANES, half)
        part = sums[side][:, at : at + LANES] * scale
        other = jnp.where(first, pltpu.roll(part, LANES - HD // 2, 1), pltpu.roll(part, HD // 2, 1))
        turned_query[g * seq_rows : (g + 1) * seq_rows] = part * cosine + other * sine
    map_zero = lax.broadcasted_iota(jnp.int32, (heads, LANES), 1) < HD
    block = 2 * heads
    for s in range(seq_rows):
        part = turned_query[pl.ds(s, heads, stride=seq_rows)]
        both = jnp.concatenate(
            [jnp.where(map_zero, part, 0.0), jnp.where(map_zero, 0.0, part)], axis=0
        ).astype(BF16)
        score_rows[s * block : (s + 1) * block] = lax.dot_general(
            both, keys[s], (((1,), (1,)), ((), ())), preferred_element_type=F32
        )
    rows = block * seq_rows
    scores = score_rows[...] * HD ** (-0.5)
    row_max = jnp.max(scores, axis=1, keepdims=True)
    exponent = jnp.exp(scores - row_max)
    row_total = jnp.sum(exponent, axis=1, keepdims=True)
    weights = exponent.astype(BF16)
    both = lanes_of([row_max, row_total], rows, LANES).T
    lines = rows_of(split(both[0:1], 3) + split(both[1:2], 2), rows)
    quarter = rows // out.shape[0]
    for k in range(out.shape[0]):
        own = lines if k == 0 else pltpu.roll(lines, rows - k * quarter, 1)
        out[k, quarter:] = own.astype(BF16)
    copies[0].wait()
    for s in range(seq_rows):
        k, at = divmod(s * block, quarter)
        out[k, at : at + block] = jnp.dot(
            weights[s * block : (s + 1) * block], values_here[s], preferred_element_type=F32
        ).astype(BF16)
    for copy in copies[1:]:
        copy.wait()


def maxima_of(parts, sources, rows):
    extra = [parts[k, rows:].astype(F32) for k in sources]
    maxima = jnp.concatenate([e[0:1] + e[1:2] + e[2:3] for e in extra], axis=0)
    totals = jnp.concatenate([e[3:4] + e[4:5] for e in extra], axis=0)
    return maxima, totals


def quarter_kernel(parts, out):
    count = parts.shape[0]
    rows = parts.shape[1] - EXTRA
    maxima, totals = maxima_of(parts, range(count), rows)
    joint = jnp.max(maxima, axis=0, keepdims=True)
    factors = jnp.exp(maxima - joint)
    total = jnp.sum(totals * factors, axis=0, keepdims=True)
    columns = turned(factors)
    joined = jnp.zeros((rows, VD), F32)
    for k in range(count):
        joined = joined + parts[k, :rows].astype(F32) * columns[:rows, k : k + 1]
    lines = rows_of(split(joint, 3) + split(total, 2), VD)
    sent = jnp.concatenate([joined, lines], axis=0).astype(BF16)
    for k in range(out.shape[0]):
        out[k] = sent


def heads_kernel(near, parts, lambdas, gain, weight, out, normed):
    far = parts.shape[0] // near
    quarter = parts.shape[1] - EXTRA
    heads = lambdas.shape[1]
    block = 2 * heads
    seq_rows = near * quarter // block
    square = (heads, heads)
    diagonal = lax.broadcasted_iota(jnp.int32, square, 0) == lax.broadcasted_iota(jnp.int32, square, 1)
    lambda_column = jnp.sum(jnp.where(diagonal, lambdas[...], 0.0), axis=1, keepdims=True)
    factors = []
    for k in range(near):
        maxima, totals = maxima_of(parts, range(k, near * far, near), quarter)
        factor = jnp.exp(maxima - jnp.max(maxima, axis=0, keepdims=True))
        factors.append(factor / jnp.sum(totals * factor, axis=0, keepdims=True))
    columns = turned(jnp.concatenate(factors, axis=0))
    for s in range(seq_rows):
        k, row = divmod(s * block, quarter)
        averaged = jnp.zeros((block, VD), F32)
        for a in range(far):
            part = parts[a * near + k, row : row + block].astype(F32)
            at = k * far + a
            averaged = averaged + part * columns[row : row + block, at : at + 1]
        difference = averaged[:heads] - lambda_column * averaged[heads:]
        mean = jnp.mean(difference * difference, axis=1, keepdims=True)
        normed[s * heads : (s + 1) * heads] = (
            difference * lax.rsqrt(mean + EPSILON) * gain[...] * KEEP_SCALE
        )
    heads_out = jnp.concatenate(
        [normed[pl.ds(g, seq_rows, stride=heads)].astype(BF16) for g in range(heads)], axis=1
    )
    out[...] = jnp.dot(heads_out, weight[...], preferred_element_type=F32).astype(BF16)


def window(array, start, width):
    low = start // LANES * LANES
    tiles = -(-(start - low + width) // LANES) * LANES
    part = array[:, low : low + tiles]
    if start > low:
        part = pltpu.roll(part, tiles - (start - low), 1)
    return part


def gate_kernel(attended, tokens, gain, gate_weight, up_weight, out, middle):
    seq_rows = tokens.shape[0]
    total = attended[:seq_rows].astype(F32) + attended[seq_rows:].astype(F32)
    mid = (tokens[...].astype(F32) + total).astype(BF16)
    middle[...] = mid
    mid = mid.astype(F32)
    mixer_in = (mid * gain[...]).astype(BF16)
    gate = jnp.dot(mixer_in, gate_weight[...], preferred_element_type=F32)
    up = jnp.dot(mixer_in, up_weight[...], preferred_element_type=F32)
    squares = jnp.sum(mid * mid, axis=1, keepdims=True)
    high, low = split(squares, 2)
    count, _, width = out.shape
    share = gate.shape[1] // count
    lane = lax.broadcasted_iota(jnp.int32, (seq_rows, width), 1)
    for k in range(count):
        parts = []
        for array in (gate, up):
            part = window(array, k * share, share)[:, :width]
            if part.shape[1] < width:
                pad = jnp.zeros((seq_rows, width - part.shape[1]), F32)
                part = jnp.concatenate([part, pad], axis=1)
            parts.append(part)
        both = jnp.where(lane < share, parts[0], pltpu.roll(parts[1], share, 1))
        both = jnp.where(lane == 2 * share, high, both)
        both = jnp.where(lane == 2 * share + 1, low, both)
        out[k] = both.astype(BF16)


def hidden_kernel(features, parts, out):
    count, _, width = parts.shape
    share = out.shape[2]
    total = parts[0].astype(F32)
    for k in range(1, count):
        total = total + parts[k].astype(F32)
    squares = total[:, 2 * share : 2 * share + 1] + total[:, 2 * share + 1 : 2 * share + 2]
    scale = lax.rsqrt(squares / features + EPSILON)
    scaled = total * scale
    gate = scaled[:, :share]
    up = pltpu.roll(scaled, width - share, 1)[:, :share]
    hidden = (gate / (1.0 + jnp.exp(-gate)) * up).astype(BF16)
    for k in range(count):
        out[k] = hidden


def down_kernel(hidden, weight, out):
    count, seq_rows, share = hidden.shape
    total = jnp.zeros(out.shape, F32)
    for k in range(count):
        total = total + jnp.dot(
            hidden[k], weight[k * share : (k + 1) * share], preferred_element_type=F32
        )
    out[...] = total.astype(BF16)


def final_kernel(parts, middle, out):
    seq_rows = middle.shape[0]
    mixed = parts[:seq_rows].astype(F32) + parts[seq_rows:].astype(F32)
    out[...] = (middle[...].astype(F32) + mixed).astype(BF16)


def rotation(context):
    frequency = ROPE_BASE ** (-np.arange(HD // 2) * 2.0 / HD)
    angles = context * frequency
    cosine, sine = np.cos(angles), np.sin(angles)
    table = [np.tile(cosine, LANES // (HD // 2)), np.tile(np.concatenate([-sine, sine]), LANES // HD)]
    return np.stack(table + [np.zeros(LANES)] * 6).astype(np.float32)


def on_device(
    tokens,
    attend_gain,
    query_weight,
    cache_keys,
    cache_values,
    head_lambda,
    head_gain,
    output_weight,
    mixer_gain,
    gate_weight,
    up_weight,
    down_weight,
):
    kv_size = lax.axis_size("kv")
    seq_rows, features_here = tokens.shape
    features = features_here * kv_size
    heads = head_lambda.shape[0]
    positions = cache_keys.shape[1]
    rows = 2 * heads * seq_rows
    share = gate_weight.shape[1] // kv_size
    padded = -(-(2 * share + 2) // LANES) * LANES
    near = 4
    pairs = [[k, k + 1] for k in range(0, kv_size, 2)]
    neighbours = [list(range(k, k + near)) for k in range(0, kv_size, near)]
    odd = jnp.broadcast_to((lax.axis_index("kv") & 1).astype(F32), (seq_rows, LANES))
    tokens, odd = lax.optimization_barrier((tokens, odd))
    keys = cache_keys.reshape(seq_rows, positions, 2 * HD)
    values = cache_values.reshape(seq_rows, positions, VD)
    width = query_weight.shape[1]

    def call(kernel, outs, here, hbm=(), scratch=(), last=False):
        spec = pl.BlockSpec(memory_space=pltpu.VMEM)
        away = pl.BlockSpec(memory_space=pltpu.HBM)
        space = jax.ShapeDtypeStruct if last else pltpu.VMEM
        outs = tuple(space(shape, kind) for shape, kind in outs)
        here = [pltpu.with_memory_space_constraint(a, pltpu.VMEM) for a in here]
        hbm = [pltpu.with_memory_space_constraint(a, pltpu.HBM) for a in hbm]
        results = pl.pallas_call(
            kernel,
            out_shape=outs,
            in_specs=[spec] * len(here) + [away] * len(hbm),
            out_specs=(spec,) * len(outs),
            scratch_shapes=list(scratch),
            compiler_params=pltpu.CompilerParams(vmem_limit_bytes=KERNEL_VMEM),
        )(*here, *hbm)
        return results[0] if len(outs) == 1 else results

    def exchange(array, groups=None):
        return lax.all_to_all(array, "kv", 0, 0, axis_index_groups=groups, tiled=True)

    gain = attend_gain[None]
    table = jnp.asarray(rotation(positions * kv_size))
    part, table = call(
        query_kernel,
        [((seq_rows, width + LANES), BF16), (table.shape, F32)],
        [],
        [tokens, gain, query_weight, table],
        scratch=[
            pltpu.VMEM(tokens.shape, BF16),
            pltpu.VMEM(gain.shape, F32),
            pltpu.VMEM(query_weight.shape, BF16),
            pltpu.SemaphoreType.DMA((4,)),
        ],
    )
    sent = call(
        halves_kernel,
        [((kv_size, seq_rows, width // 2 + LANES), BF16)],
        [odd, lax.all_gather(part, "kv", axis_index_groups=pairs)],
    )
    later = [
        output_weight,
        gate_weight,
        up_weight,
        down_weight,
        tokens,
        head_lambda[None],
        head_gain[None],
        mixer_gain[None],
    ]
    sent, *later = call(
        functools.partial(attend_kernel, features, len(later)),
        [((near, rows // near + EXTRA, VD), BF16)] + [(a.shape, a.dtype) for a in later],
        [exchange(sent), table, keys],
        [values, *later],
        scratch=[
            pltpu.VMEM(values.shape, BF16),
            pltpu.VMEM((heads * seq_rows, LANES), F32),
            pltpu.VMEM((rows, positions), F32),
            pltpu.SemaphoreType.DMA((1 + len(later),)),
        ],
    )
    output_weight, gate_weight, up_weight, down_weight, tokens, lambdas, head_gain, mixer_gain = later
    sent = call(
        quarter_kernel,
        [((kv_size, rows // near + EXTRA, VD), BF16)],
        [exchange(sent, neighbours)],
    )
    attended = call(
        functools.partial(heads_kernel, near),
        [((seq_rows, features_here), BF16)],
        [exchange(sent), lambdas, head_gain, output_weight],
        scratch=[pltpu.VMEM((heads * seq_rows, VD), F32)],
    )
    sent, middle = call(
        gate_kernel,
        [((kv_size, seq_rows, padded), BF16), ((seq_rows, features_here), BF16)],
        [
            lax.all_gather(attended, "tp", tiled=True),
            tokens,
            mixer_gain,
            gate_weight,
            up_weight,
        ],
    )
    sent = call(
        functools.partial(hidden_kernel, features),
        [((kv_size, seq_rows, share), BF16)],
        [exchange(sent)],
    )
    projected = call(
        down_kernel, [((seq_rows, features_here), BF16)], [exchange(sent), down_weight]
    )
    return call(
        final_kernel,
        [((seq_rows, features_here), BF16)],
        [lax.all_gather(projected, "tp", tiled=True), middle],
        last=True,
    )


def solution(mesh):
    return jax.shard_map(
        on_device,
        mesh=mesh,
        in_specs=(
            P(("grp", "dp"), "kv"),
            P("kv"),
            P("kv", "tp"),
            P(("grp", "dp"), "kv", "tp", None),
            P(("grp", "dp"), "kv", "tp", None),
            P("tp"),
            P(),
            P("tp", "kv"),
            P("kv"),
            P("kv", "tp"),
            P("kv", "tp"),
            P("tp", "kv"),
        ),
        out_specs=P(("grp", "dp"), "kv"),
        check_vma=False,
    )
```

```python
import functools

import jax
import jax.numpy as jnp
import numpy as np
from jax import lax
from jax.experimental import pallas as pl
from jax.experimental.pallas import tpu as pltpu
from jax.sharding import PartitionSpec as P

HD = 64
VD = 128
LANES = 128
EXTRA = 8

KERNEL_VMEM = 8 << 20

ROPE_BASE = 500000.0
EPSILON = 1e-06
KEEP_SCALE = 0.8
F32 = jnp.float32
BF16 = jnp.bfloat16


def split(value, terms):
    parts = []
    for _ in range(terms):
        part = value.astype(BF16).astype(F32)
        parts.append(part)
        value = value - part
    return parts


def lanes_of(columns, rows, width):
    lane = lax.broadcasted_iota(jnp.int32, (rows, width), 1)
    out = jnp.zeros((rows, width), F32)
    for k, column in enumerate(columns):
        out = jnp.where(lane == k, column, out)
    return out


def rows_of(lines, width):
    row = lax.broadcasted_iota(jnp.int32, (EXTRA, width), 0)
    out = jnp.zeros((EXTRA, width), F32)
    for k, line in enumerate(lines):
        out = jnp.where(row == k, line, out)
    return out


def turned(rows):
    pad = jnp.zeros((LANES - rows.shape[0], LANES), F32)
    return jnp.concatenate([rows, pad], axis=0).T


def query_kernel(tokens, gain, weight, table, values, out, table_here, values_here, *scratch):
    tokens_here, gain_here, weight_here, semaphores = scratch
    copies = [
        pltpu.make_async_copy(source, target, semaphores.at[k])
        for k, (source, target) in enumerate(
            (
                (weight, weight_here),
                (tokens, tokens_here),
                (gain, gain_here),
                (table, table_here),
                (values, values_here),
            )
        )
    ]
    for copy in copies:
        copy.start()
    for copy in copies[:3]:
        copy.wait()
    tok = tokens_here[...].astype(F32)
    scaled = (tok * gain_here[...]).astype(BF16)
    partial = jnp.dot(scaled, weight_here[...], preferred_element_type=F32)
    squares = jnp.sum(tok * tok, axis=1, keepdims=True)
    width = partial.shape[1]
    out[:, :width] = partial.astype(BF16)
    out[:, width:] = lanes_of(split(squares, 2), tok.shape[0], LANES).astype(BF16)
    for copy in copies[3:]:
        copy.wait()


def halves_kernel(odd, parts, out):
    total = parts[0].astype(F32) + parts[1].astype(F32)
    half = (total.shape[1] - LANES) // 2
    own = jnp.where(odd[:, :1] > 0, total[:, half : 2 * half], total[:, :half])
    extra = total[:, 2 * half :]
    squares = extra[:, 0:1] + extra[:, 1:2]
    extra = lanes_of(split(squares, 2), total.shape[0], LANES)
    sent = jnp.concatenate([own, extra], axis=1).astype(BF16)
    for k in range(out.shape[0]):
        out[k] = sent


def attend_kernel(features, parts, table, keys, values, out, turned_query, score_rows):
    count, seq_rows, half = parts.shape
    half -= LANES
    sums = []
    for odd in range(2):
        total = parts[odd].astype(F32)
        for k in range(odd + 2, count, 2):
            total = total + parts[k].astype(F32)
        sums.append(total)
    squares = sums[0][:, half : half + 1] + sums[0][:, half + 1 : half + 2]
    scale = lax.rsqrt(squares / features + EPSILON)
    heads = 2 * half // (2 * HD)
    lane = lax.broadcasted_iota(jnp.int32, (seq_rows, LANES), 1)
    first = lane % HD < HD // 2
    cosine, sine = table[0:1], table[1:2]
    for g in range(heads):
        side, at = divmod(g * LANES, half)
        part = sums[side][:, at : at + LANES] * scale
        other = jnp.where(first, pltpu.roll(part, LANES - HD // 2, 1), pltpu.roll(part, HD // 2, 1))
        turned_query[g * seq_rows : (g + 1) * seq_rows] = part * cosine + other * sine
    map_zero = lax.broadcasted_iota(jnp.int32, (heads, LANES), 1) < HD
    block = 2 * heads
    for s in range(seq_rows):
        part = turned_query[pl.ds(s, heads, stride=seq_rows)]
        both = jnp.concatenate(
            [jnp.where(map_zero, part, 0.0), jnp.where(map_zero, 0.0, part)], axis=0
        ).astype(BF16)
        score_rows[s * block : (s + 1) * block] = lax.dot_general(
            both, keys[s], (((1,), (1,)), ((), ())), preferred_element_type=F32
        )
    rows = block * seq_rows
    scores = score_rows[...] * HD ** (-0.5)
    row_max = jnp.max(scores, axis=1, keepdims=True)
    exponent = jnp.exp(scores - row_max)
    row_total = jnp.sum(exponent, axis=1, keepdims=True)
    weights = exponent.astype(BF16)
    both = lanes_of([row_max, row_total], rows, LANES).T
    lines = rows_of(split(both[0:1], 3) + split(both[1:2], 2), rows)
    quarter = rows // out.shape[0]
    for k in range(out.shape[0]):
        own = lines if k == 0 else pltpu.roll(lines, rows - k * quarter, 1)
        out[k, quarter:] = own.astype(BF16)
    for s in range(seq_rows):
        k, at = divmod(s * block, quarter)
        out[k, at : at + block] = jnp.dot(
            weights[s * block : (s + 1) * block], values[s], preferred_element_type=F32
        ).astype(BF16)


def maxima_of(parts, sources, rows):
    extra = [parts[k, rows:].astype(F32) for k in sources]
    maxima = jnp.concatenate([e[0:1] + e[1:2] + e[2:3] for e in extra], axis=0)
    totals = jnp.concatenate([e[3:4] + e[4:5] for e in extra], axis=0)
    return maxima, totals


def quarter_kernel(parts, ahead, out):
    count = parts.shape[0]
    rows = parts.shape[1] - EXTRA
    maxima, totals = maxima_of(parts, range(count), rows)
    joint = jnp.max(maxima, axis=0, keepdims=True)
    factors = jnp.exp(maxima - joint)
    total = jnp.sum(totals * factors, axis=0, keepdims=True)
    columns = turned(factors)
    joined = jnp.zeros((rows, VD), F32)
    for k in range(count):
        joined = joined + parts[k, :rows].astype(F32) * columns[:rows, k : k + 1]
    lines = rows_of(split(joint, 3) + split(total, 2), VD)
    sent = jnp.concatenate([joined, lines], axis=0).astype(BF16)
    for k in range(out.shape[0]):
        out[k] = sent


def heads_kernel(near, parts, lambdas, gain, weight, out, normed):
    far = parts.shape[0] // near
    quarter = parts.shape[1] - EXTRA
    heads = lambdas.shape[1]
    block = 2 * heads
    seq_rows = near * quarter // block
    square = (heads, heads)
    diagonal = lax.broadcasted_iota(jnp.int32, square, 0) == lax.broadcasted_iota(jnp.int32, square, 1)
    lambda_column = jnp.sum(jnp.where(diagonal, lambdas[...], 0.0), axis=1, keepdims=True)
    factors = []
    for k in range(near):
        maxima, totals = maxima_of(parts, range(k, near * far, near), quarter)
        factor = jnp.exp(maxima - jnp.max(maxima, axis=0, keepdims=True))
        factors.append(factor / jnp.sum(totals * factor, axis=0, keepdims=True))
    columns = turned(jnp.concatenate(factors, axis=0))
    for s in range(seq_rows):
        k, row = divmod(s * block, quarter)
        averaged = jnp.zeros((block, VD), F32)
        for a in range(far):
            part = parts[a * near + k, row : row + block].astype(F32)
            at = k * far + a
            averaged = averaged + part * columns[row : row + block, at : at + 1]
        difference = averaged[:heads] - lambda_column * averaged[heads:]
        mean = jnp.mean(difference * difference, axis=1, keepdims=True)
        normed[s * heads : (s + 1) * heads] = (
            difference * lax.rsqrt(mean + EPSILON) * gain[...] * KEEP_SCALE
        )
    heads_out = jnp.concatenate(
        [normed[pl.ds(g, seq_rows, stride=heads)].astype(BF16) for g in range(heads)], axis=1
    )
    out[...] = jnp.dot(heads_out, weight[...], preferred_element_type=F32).astype(BF16)


def window(array, start, width):
    low = start // LANES * LANES
    tiles = -(-(start - low + width) // LANES) * LANES
    part = array[:, low : low + tiles]
    if start > low:
        part = pltpu.roll(part, tiles - (start - low), 1)
    return part


def gate_kernel(attended, tokens, gain, gate_weight, up_weight, out, middle):
    seq_rows = tokens.shape[0]
    total = attended[:seq_rows].astype(F32) + attended[seq_rows:].astype(F32)
    mid = (tokens[...].astype(F32) + total).astype(BF16)
    middle[...] = mid
    mid = mid.astype(F32)
    mixer_in = (mid * gain[...]).astype(BF16)
    gate = jnp.dot(mixer_in, gate_weight[...], preferred_element_type=F32)
    up = jnp.dot(mixer_in, up_weight[...], preferred_element_type=F32)
    squares = jnp.sum(mid * mid, axis=1, keepdims=True)
    high, low = split(squares, 2)
    count, _, width = out.shape
    share = gate.shape[1] // count
    lane = lax.broadcasted_iota(jnp.int32, (seq_rows, width), 1)
    for k in range(count):
        parts = []
        for array in (gate, up):
            part = window(array, k * share, share)[:, :width]
            if part.shape[1] < width:
                pad = jnp.zeros((seq_rows, width - part.shape[1]), F32)
                part = jnp.concatenate([part, pad], axis=1)
            parts.append(part)
        both = jnp.where(lane < share, parts[0], pltpu.roll(parts[1], share, 1))
        both = jnp.where(lane == 2 * share, high, both)
        both = jnp.where(lane == 2 * share + 1, low, both)
        out[k] = both.astype(BF16)


def hidden_kernel(features, parts, out):
    count, _, width = parts.shape
    share = out.shape[2]
    total = parts[0].astype(F32)
    for k in range(1, count):
        total = total + parts[k].astype(F32)
    squares = total[:, 2 * share : 2 * share + 1] + total[:, 2 * share + 1 : 2 * share + 2]
    scale = lax.rsqrt(squares / features + EPSILON)
    scaled = total * scale
    gate = scaled[:, :share]
    up = pltpu.roll(scaled, width - share, 1)[:, :share]
    hidden = (gate / (1.0 + jnp.exp(-gate)) * up).astype(BF16)
    for k in range(count):
        out[k] = hidden


def down_kernel(hidden, weight, out):
    count, seq_rows, share = hidden.shape
    total = jnp.zeros(out.shape, F32)
    for k in range(count):
        total = total + jnp.dot(
            hidden[k], weight[k * share : (k + 1) * share], preferred_element_type=F32
        )
    out[...] = total.astype(BF16)


def final_kernel(parts, middle, out):
    seq_rows = middle.shape[0]
    mixed = parts[:seq_rows].astype(F32) + parts[seq_rows:].astype(F32)
    out[...] = (middle[...].astype(F32) + mixed).astype(BF16)


def rotation(context):
    frequency = ROPE_BASE ** (-np.arange(HD // 2) * 2.0 / HD)
    angles = context * frequency
    cosine, sine = np.cos(angles), np.sin(angles)
    table = [np.tile(cosine, LANES // (HD // 2)), np.tile(np.concatenate([-sine, sine]), LANES // HD)]
    return np.stack(table + [np.zeros(LANES)] * 6).astype(np.float32)


def on_device(
    tokens,
    attend_gain,
    query_weight,
    cache_keys,
    cache_values,
    head_lambda,
    head_gain,
    output_weight,
    mixer_gain,
    gate_weight,
    up_weight,
    down_weight,
):
    kv_size = lax.axis_size("kv")
    seq_rows, features_here = tokens.shape
    features = features_here * kv_size
    heads = head_lambda.shape[0]
    positions = cache_keys.shape[1]
    rows = 2 * heads * seq_rows
    share = gate_weight.shape[1] // kv_size
    padded = -(-(2 * share + 2) // LANES) * LANES
    near = 4
    pairs = [[k, k + 1] for k in range(0, kv_size, 2)]
    neighbours = [list(range(k, k + near)) for k in range(0, kv_size, near)]
    odd = jnp.broadcast_to((lax.axis_index("kv") & 1).astype(F32), (seq_rows, LANES))
    tokens, odd = lax.optimization_barrier((tokens, odd))
    keys = cache_keys.reshape(seq_rows, positions, 2 * HD)
    values = cache_values.reshape(seq_rows, positions, VD)
    width = query_weight.shape[1]

    def call(kernel, outs, here, hbm=(), scratch=(), last=False):
        spec = pl.BlockSpec(memory_space=pltpu.VMEM)
        away = pl.BlockSpec(memory_space=pltpu.HBM)
        space = jax.ShapeDtypeStruct if last else pltpu.VMEM
        outs = tuple(space(shape, kind) for shape, kind in outs)
        here = [pltpu.with_memory_space_constraint(a, pltpu.VMEM) for a in here]
        hbm = [pltpu.with_memory_space_constraint(a, pltpu.HBM) for a in hbm]
        results = pl.pallas_call(
            kernel,
            out_shape=outs,
            in_specs=[spec] * len(here) + [away] * len(hbm),
            out_specs=(spec,) * len(outs),
            scratch_shapes=list(scratch),
            compiler_params=pltpu.CompilerParams(vmem_limit_bytes=KERNEL_VMEM),
        )(*here, *hbm)
        return results[0] if len(outs) == 1 else results

    def exchange(array, groups=None):
        return lax.all_to_all(array, "kv", 0, 0, axis_index_groups=groups, tiled=True)

    gain = attend_gain[None]
    table = jnp.asarray(rotation(positions * kv_size))
    part, table, values = call(
        query_kernel,
        [((seq_rows, width + LANES), BF16), (table.shape, F32), (values.shape, BF16)],
        [],
        [tokens, gain, query_weight, table, values],
        scratch=[
            pltpu.VMEM(tokens.shape, BF16),
            pltpu.VMEM(gain.shape, F32),
            pltpu.VMEM(query_weight.shape, BF16),
            pltpu.SemaphoreType.DMA((5,)),
        ],
    )
    sent = call(
        halves_kernel,
        [((kv_size, seq_rows, width // 2 + LANES), BF16)],
        [odd, lax.all_gather(part, "kv", axis_index_groups=pairs)],
    )
    sent = call(
        functools.partial(attend_kernel, features),
        [((near, rows // near + EXTRA, VD), BF16)],
        [exchange(sent), table, keys, values],
        scratch=[
            pltpu.VMEM((heads * seq_rows, LANES), F32),
            pltpu.VMEM((rows, positions), F32),
        ],
    )
    sent = call(
        quarter_kernel,
        [((kv_size, rows // near + EXTRA, VD), BF16)],
        [exchange(sent, neighbours), mixer_gain[None]],
    )
    attended = call(
        functools.partial(heads_kernel, near),
        [((seq_rows, features_here), BF16)],
        [exchange(sent), head_lambda[None], head_gain[None], output_weight],
        scratch=[pltpu.VMEM((heads * seq_rows, VD), F32)],
    )
    sent, middle = call(
        gate_kernel,
        [((kv_size, seq_rows, padded), BF16), ((seq_rows, features_here), BF16)],
        [
            lax.all_gather(attended, "tp", tiled=True),
            tokens,
            mixer_gain[None],
            gate_weight,
            up_weight,
        ],
    )
    sent = call(
        functools.partial(hidden_kernel, features),
        [((kv_size, seq_rows, share), BF16)],
        [exchange(sent)],
    )
    projected = call(
        down_kernel, [((seq_rows, features_here), BF16)], [exchange(sent), down_weight]
    )
    return call(
        final_kernel,
        [((seq_rows, features_here), BF16)],
        [lax.all_gather(projected, "tp", tiled=True), middle],
        last=True,
    )


def solution(mesh):
    return jax.shard_map(
        on_device,
        mesh=mesh,
        in_specs=(
            P(("grp", "dp"), "kv"),
            P("kv"),
            P("kv", "tp"),
            P(("grp", "dp"), "kv", "tp", None),
            P(("grp", "dp"), "kv", "tp", None),
            P("tp"),
            P(),
            P("tp", "kv"),
            P("kv"),
            P("kv", "tp"),
            P("kv", "tp"),
            P("tp", "kv"),
        ),
        out_specs=P(("grp", "dp"), "kv"),
        check_vma=False,
    )
```

```python
import functools

import jax
import jax.numpy as jnp
import numpy as np
from jax import lax
from jax.experimental import pallas as pl
from jax.experimental.pallas import tpu as pltpu
from jax.sharding import PartitionSpec as P

HD = 64
VD = 128
LANES = 128
PACKED = 2
EXTRA = 8

KERNEL_VMEM = 8 << 20

ROPE_BASE = 500000.0
EPSILON = 1e-06
KEEP_SCALE = 0.8
F32 = jnp.float32
BF16 = jnp.bfloat16


def split(value, terms):
    parts = []
    for _ in range(terms):
        part = value.astype(BF16).astype(F32)
        parts.append(part)
        value = value - part
    return parts


def lanes_of(columns, rows, width):
    lane = lax.broadcasted_iota(jnp.int32, (rows, width), 1)
    out = jnp.zeros((rows, width), F32)
    for k, column in enumerate(columns):
        out = jnp.where(lane == k, column, out)
    return out


def rows_of(lines, width):
    row = lax.broadcasted_iota(jnp.int32, (EXTRA, width), 0)
    out = jnp.zeros((EXTRA, width), F32)
    for k, line in enumerate(lines):
        out = jnp.where(row == k, line, out)
    return out


def turned(rows):
    pad = jnp.zeros((LANES - rows.shape[0], LANES), F32)
    return jnp.concatenate([rows, pad], axis=0).T


def query_kernel(tokens, gain, weight, table, values, out, table_here, values_here, *scratch):
    tokens_here, gain_here, weight_here, semaphores = scratch
    copies = [
        pltpu.make_async_copy(source, target, semaphores.at[k])
        for k, (source, target) in enumerate(
            (
                (weight, weight_here),
                (tokens, tokens_here),
                (gain, gain_here),
                (table, table_here),
                (values, values_here),
            )
        )
    ]
    for copy in copies:
        copy.start()
    for copy in copies[:3]:
        copy.wait()
    tok = tokens_here[...].astype(F32)
    scaled = (tok * gain_here[...]).astype(BF16)
    partial = jnp.dot(scaled, weight_here[...], preferred_element_type=F32)
    squares = jnp.sum(tok * tok, axis=1, keepdims=True)
    width = partial.shape[1]
    out[:, :width] = partial.astype(BF16)
    out[:, width:] = lanes_of(split(squares, 2), tok.shape[0], LANES).astype(BF16)
    for copy in copies[3:]:
        copy.wait()


def halves_kernel(odd, parts, out):
    total = parts[0].astype(F32) + parts[1].astype(F32)
    half = (total.shape[1] - LANES) // 2
    own = jnp.where(odd[:, :1] > 0, total[:, half : 2 * half], total[:, :half])
    extra = total[:, 2 * half :]
    squares = extra[:, 0:1] + extra[:, 1:2]
    seq_rows = total.shape[0]
    lane = lax.broadcasted_iota(jnp.int32, (seq_rows, LANES), 1)
    at = lax.broadcasted_iota(jnp.int32, (seq_rows, LANES), 0) // PACKED * 2
    high, low = split(squares, 2)
    extra = jnp.where(lane == at, high, jnp.where(lane == at + 1, low, 0.0))
    pieces = [own[r : r + PACKED] for r in range(0, seq_rows, PACKED)]
    pieces.append(sum(extra[r : r + PACKED] for r in range(0, seq_rows, PACKED)))
    sent = jnp.concatenate(pieces, axis=1).astype(BF16)
    for k in range(out.shape[0]):
        out[k] = sent


def attend_kernel(features, parts, table, keys, values, out, query, squares, turned_query, score_rows):
    count = parts.shape[0]
    seq_rows, width = query.shape
    half = width // 2
    for odd in range(2):
        total = parts[odd].astype(F32)
        for k in range(odd + 2, count, 2):
            total = total + parts[k].astype(F32)
        for r in range(seq_rows // PACKED):
            rows = slice(r * PACKED, (r + 1) * PACKED)
            query[rows, odd * half : (odd + 1) * half] = total[:, r * half : (r + 1) * half]
            if odd == 0:
                extra = total[:, seq_rows // PACKED * half :]
                both = extra[:, 2 * r : 2 * r + 1] + extra[:, 2 * r + 1 : 2 * r + 2]
                squares[rows] = jnp.broadcast_to(both, (PACKED, LANES))
    scale = lax.rsqrt(squares[...] / features + EPSILON)
    heads = 2 * half // (2 * HD)
    lane = lax.broadcasted_iota(jnp.int32, (seq_rows, LANES), 1)
    first = lane % HD < HD // 2
    cosine, sine = table[0:1], table[1:2]
    for g in range(heads):
        part = query[:, g * LANES : (g + 1) * LANES] * scale
        other = jnp.where(first, pltpu.roll(part, LANES - HD // 2, 1), pltpu.roll(part, HD // 2, 1))
        turned_query[g * seq_rows : (g + 1) * seq_rows] = part * cosine + other * sine
    map_zero = lax.broadcasted_iota(jnp.int32, (heads, LANES), 1) < HD
    block = 2 * heads
    for s in range(seq_rows):
        part = turned_query[pl.ds(s, heads, stride=seq_rows)]
        both = jnp.concatenate(
            [jnp.where(map_zero, part, 0.0), jnp.where(map_zero, 0.0, part)], axis=0
        ).astype(BF16)
        score_rows[s * block : (s + 1) * block] = lax.dot_general(
            both, keys[s], (((1,), (1,)), ((), ())), preferred_element_type=F32
        )
    rows = block * seq_rows
    scores = score_rows[...] * HD ** (-0.5)
    row_max = jnp.max(scores, axis=1, keepdims=True)
    exponent = jnp.exp(scores - row_max)
    row_total = jnp.sum(exponent, axis=1, keepdims=True)
    weights = exponent.astype(BF16)
    both = lanes_of([row_max, row_total], rows, LANES).T
    lines = rows_of(split(both[0:1], 3) + split(both[1:2], 2), rows)
    quarter = rows // out.shape[0]
    for k in range(out.shape[0]):
        own = lines if k == 0 else pltpu.roll(lines, rows - k * quarter, 1)
        out[k, quarter:] = own.astype(BF16)
    for s in range(seq_rows):
        k, at = divmod(s * block, quarter)
        out[k, at : at + block] = jnp.dot(
            weights[s * block : (s + 1) * block], values[s], preferred_element_type=F32
        ).astype(BF16)


def maxima_of(parts, sources, rows):
    extra = [parts[k, rows:].astype(F32) for k in sources]
    maxima = jnp.concatenate([e[0:1] + e[1:2] + e[2:3] for e in extra], axis=0)
    totals = jnp.concatenate([e[3:4] + e[4:5] for e in extra], axis=0)
    return maxima, totals


def quarter_kernel(parts, ahead, out):
    count = parts.shape[0]
    rows = parts.shape[1] - EXTRA
    maxima, totals = maxima_of(parts, range(count), rows)
    joint = jnp.max(maxima, axis=0, keepdims=True)
    factors = jnp.exp(maxima - joint)
    total = jnp.sum(totals * factors, axis=0, keepdims=True)
    columns = turned(factors)
    joined = jnp.zeros((rows, VD), F32)
    for k in range(count):
        joined = joined + parts[k, :rows].astype(F32) * columns[:rows, k : k + 1]
    lane = lax.broadcasted_iota(jnp.int32, (PACKED, VD), 1)
    row = lax.broadcasted_iota(jnp.int32, (PACKED, VD), 0)
    extra = jnp.zeros((PACKED, VD), F32)
    for k, line in enumerate(split(joint, 3) + split(total, 2)):
        at, slot = divmod(k * rows, VD)
        line = pltpu.roll(jnp.broadcast_to(line, (PACKED, VD)), slot, 1) if slot else line
        extra = jnp.where((row == at) & (lane >= slot) & (lane < slot + rows), line, extra)
    pieces = [joined[r : r + PACKED] for r in range(0, rows, PACKED)]
    sent = jnp.concatenate([*pieces, extra], axis=1).astype(BF16)
    for k in range(out.shape[0]):
        out[k] = sent


def heads_kernel(near, parts, lambdas, gain, weight, out, blocks, normed):
    count, quarter, _ = blocks.shape
    far = count // near
    heads = lambdas.shape[1]
    block = 2 * heads
    seq_rows = near * quarter // block
    square = (heads, heads)
    diagonal = lax.broadcasted_iota(jnp.int32, square, 0) == lax.broadcasted_iota(jnp.int32, square, 1)
    lambda_column = jnp.sum(jnp.where(diagonal, lambdas[...], 0.0), axis=1, keepdims=True)
    extra = []
    for j in [a * near + k for k in range(near) for a in range(far)]:
        part = parts[j].astype(F32)
        for r in range(quarter // PACKED):
            blocks[j, r * PACKED : (r + 1) * PACKED] = part[:, r * VD : (r + 1) * VD]
        extra.append(part[:, quarter // PACKED * VD :])
    extra = [jnp.concatenate([e[r : r + 1] for e in extra], axis=0) for r in range(PACKED)]
    lines = []
    for k in range(5):
        at, slot = divmod(k * quarter, VD)
        lines.append(pltpu.roll(extra[at], VD - slot, 1) if slot else extra[at])
    maxima, totals = lines[0] + lines[1] + lines[2], lines[3] + lines[4]
    factors = []
    for k in range(near):
        own = slice(k * far, (k + 1) * far)
        factor = jnp.exp(maxima[own] - jnp.max(maxima[own], axis=0, keepdims=True))
        factors.append(factor / jnp.sum(totals[own] * factor, axis=0, keepdims=True))
    columns = turned(jnp.concatenate(factors, axis=0))
    for s in range(seq_rows):
        k, row = divmod(s * block, quarter)
        averaged = jnp.zeros((block, VD), F32)
        for a in range(far):
            part = blocks[a * near + k, row : row + block]
            at = k * far + a
            averaged = averaged + part * columns[row : row + block, at : at + 1]
        difference = averaged[:heads] - lambda_column * averaged[heads:]
        mean = jnp.mean(difference * difference, axis=1, keepdims=True)
        normed[s * heads : (s + 1) * heads] = (
            difference * lax.rsqrt(mean + EPSILON) * gain[...] * KEEP_SCALE
        )
    heads_out = jnp.concatenate(
        [normed[pl.ds(g, seq_rows, stride=heads)].astype(BF16) for g in range(heads)], axis=1
    )
    out[...] = jnp.dot(heads_out, weight[...], preferred_element_type=F32).astype(BF16)


def window(array, start, width):
    low = start // LANES * LANES
    tiles = -(-(start - low + width) // LANES) * LANES
    part = array[:, low : low + tiles]
    if start > low:
        part = pltpu.roll(part, tiles - (start - low), 1)
    return part


def gate_kernel(attended, tokens, gain, gate_weight, up_weight, out, middle):
    seq_rows = tokens.shape[0]
    total = attended[:seq_rows].astype(F32) + attended[seq_rows:].astype(F32)
    mid = (tokens[...].astype(F32) + total).astype(BF16)
    middle[...] = mid
    mid = mid.astype(F32)
    mixer_in = (mid * gain[...]).astype(BF16)
    gate = jnp.dot(mixer_in, gate_weight[...], preferred_element_type=F32)
    up = jnp.dot(mixer_in, up_weight[...], preferred_element_type=F32)
    squares = jnp.sum(mid * mid, axis=1, keepdims=True)
    high, low = split(squares, 2)
    count, _, width = out.shape
    share = gate.shape[1] // count
    lane = lax.broadcasted_iota(jnp.int32, (seq_rows, width), 1)
    for k in range(count):
        parts = []
        for array in (gate, up):
            part = window(array, k * share, share)[:, :width]
            if part.shape[1] < width:
                pad = jnp.zeros((seq_rows, width - part.shape[1]), F32)
                part = jnp.concatenate([part, pad], axis=1)
            parts.append(part)
        both = jnp.where(lane < share, parts[0], pltpu.roll(parts[1], share, 1))
        both = jnp.where(lane == 2 * share, high, both)
        both = jnp.where(lane == 2 * share + 1, low, both)
        out[k] = both.astype(BF16)


def hidden_kernel(features, share, parts, out):
    count, seq_rows, width = parts.shape
    total = parts[0].astype(F32)
    for k in range(1, count):
        total = total + parts[k].astype(F32)
    squares = total[:, 2 * share : 2 * share + 1] + total[:, 2 * share + 1 : 2 * share + 2]
    scale = lax.rsqrt(squares / features + EPSILON)
    scaled = total * scale
    tiles = -(-share // LANES) * LANES
    lane = lax.broadcasted_iota(jnp.int32, (seq_rows, tiles), 1)
    gate = jnp.where(lane < share, scaled[:, :tiles], 0.0)
    up = pltpu.roll(scaled, width - share, 1)[:, :tiles]
    hidden = gate / (1.0 + jnp.exp(-gate)) * up
    lanes = out.shape[2]
    hidden = jnp.concatenate([hidden, jnp.zeros((seq_rows, lanes - hidden.shape[1]), F32)], axis=1)
    sent = hidden[:PACKED]
    for r in range(1, seq_rows // PACKED):
        sent = sent + pltpu.roll(hidden[r * PACKED : (r + 1) * PACKED], r * share, 1)
    sent = sent.astype(BF16)
    for k in range(count):
        out[k] = sent


def down_kernel(share, hidden, weight, out, blocks):
    count, _, lanes = hidden.shape
    seq_rows, tiles = blocks.shape[1:]
    for k in range(count):
        part = hidden[k].astype(F32)
        for r in range(seq_rows // PACKED):
            moved = pltpu.roll(part, lanes - r * share, 1) if r else part
            blocks[k, r * PACKED : (r + 1) * PACKED] = moved[:, :tiles]
    total = jnp.zeros(out.shape, F32)
    for k in range(count):
        total = total + jnp.dot(
            blocks[k, :, :share].astype(BF16),
            weight[k * share : (k + 1) * share],
            preferred_element_type=F32,
        )
    out[...] = total.astype(BF16)


def final_kernel(parts, middle, out):
    seq_rows = middle.shape[0]
    mixed = parts[:seq_rows].astype(F32) + parts[seq_rows:].astype(F32)
    out[...] = (middle[...].astype(F32) + mixed).astype(BF16)


def rotation(context):
    frequency = ROPE_BASE ** (-np.arange(HD // 2) * 2.0 / HD)
    angles = context * frequency
    cosine, sine = np.cos(angles), np.sin(angles)
    table = [np.tile(cosine, LANES // (HD // 2)), np.tile(np.concatenate([-sine, sine]), LANES // HD)]
    return np.stack(table + [np.zeros(LANES)] * 6).astype(np.float32)


def on_device(
    tokens,
    attend_gain,
    query_weight,
    cache_keys,
    cache_values,
    head_lambda,
    head_gain,
    output_weight,
    mixer_gain,
    gate_weight,
    up_weight,
    down_weight,
):
    kv_size = lax.axis_size("kv")
    seq_rows, features_here = tokens.shape
    features = features_here * kv_size
    heads = head_lambda.shape[0]
    positions = cache_keys.shape[1]
    rows = 2 * heads * seq_rows
    share = gate_weight.shape[1] // kv_size
    padded = -(-(2 * share + 2) // LANES) * LANES
    near = 4
    pairs = [[k, k + 1] for k in range(0, kv_size, 2)]
    neighbours = [list(range(k, k + near)) for k in range(0, kv_size, near)]
    odd = jnp.broadcast_to((lax.axis_index("kv") & 1).astype(F32), (seq_rows, LANES))
    tokens, odd = lax.optimization_barrier((tokens, odd))
    keys = cache_keys.reshape(seq_rows, positions, 2 * HD)
    values = cache_values.reshape(seq_rows, positions, VD)
    width = query_weight.shape[1]

    def call(kernel, outs, here, hbm=(), scratch=(), last=False):
        spec = pl.BlockSpec(memory_space=pltpu.VMEM)
        away = pl.BlockSpec(memory_space=pltpu.HBM)
        space = jax.ShapeDtypeStruct if last else pltpu.VMEM
        outs = tuple(space(shape, kind) for shape, kind in outs)
        here = [pltpu.with_memory_space_constraint(a, pltpu.VMEM) for a in here]
        hbm = [pltpu.with_memory_space_constraint(a, pltpu.HBM) for a in hbm]
        results = pl.pallas_call(
            kernel,
            out_shape=outs,
            in_specs=[spec] * len(here) + [away] * len(hbm),
            out_specs=(spec,) * len(outs),
            scratch_shapes=list(scratch),
            compiler_params=pltpu.CompilerParams(vmem_limit_bytes=KERNEL_VMEM),
        )(*here, *hbm)
        return results[0] if len(outs) == 1 else results

    def exchange(array, groups=None):
        return lax.all_to_all(array, "kv", 0, 0, axis_index_groups=groups, tiled=True)

    gain = attend_gain[None]
    table = jnp.asarray(rotation(positions * kv_size))
    part, table, values = call(
        query_kernel,
        [((seq_rows, width + LANES), BF16), (table.shape, F32), (values.shape, BF16)],
        [],
        [tokens, gain, query_weight, table, values],
        scratch=[
            pltpu.VMEM(tokens.shape, BF16),
            pltpu.VMEM(gain.shape, F32),
            pltpu.VMEM(query_weight.shape, BF16),
            pltpu.SemaphoreType.DMA((5,)),
        ],
    )
    sent = call(
        halves_kernel,
        [((kv_size, PACKED, seq_rows // PACKED * (width // 2) + LANES), BF16)],
        [odd, lax.all_gather(part, "kv", axis_index_groups=pairs)],
    )
    sent = call(
        functools.partial(attend_kernel, features),
        [((near, rows // near + EXTRA, VD), BF16)],
        [exchange(sent), table, keys, values],
        scratch=[
            pltpu.VMEM((seq_rows, width), F32),
            pltpu.VMEM((seq_rows, LANES), F32),
            pltpu.VMEM((heads * seq_rows, LANES), F32),
            pltpu.VMEM((rows, positions), F32),
        ],
    )
    sent = call(
        quarter_kernel,
        [((kv_size, PACKED, (rows // near // PACKED + 1) * VD), BF16)],
        [exchange(sent, neighbours), mixer_gain[None]],
    )
    attended = call(
        functools.partial(heads_kernel, near),
        [((seq_rows, features_here), BF16)],
        [exchange(sent), head_lambda[None], head_gain[None], output_weight],
        scratch=[
            pltpu.VMEM((kv_size, rows // near, VD), F32),
            pltpu.VMEM((heads * seq_rows, VD), F32),
        ],
    )
    sent, middle = call(
        gate_kernel,
        [((kv_size, seq_rows, padded), BF16), ((seq_rows, features_here), BF16)],
        [
            lax.all_gather(attended, "tp", tiled=True),
            tokens,
            mixer_gain[None],
            gate_weight,
            up_weight,
        ],
    )
    sent = call(
        functools.partial(hidden_kernel, features, share),
        [((kv_size, PACKED, -(-(seq_rows // PACKED * share) // LANES) * LANES), BF16)],
        [exchange(sent)],
    )
    projected = call(
        functools.partial(down_kernel, share),
        [((seq_rows, features_here), BF16)],
        [exchange(sent), down_weight],
        scratch=[pltpu.VMEM((kv_size, seq_rows, -(-share // LANES) * LANES), F32)],
    )
    return call(
        final_kernel,
        [((seq_rows, features_here), BF16)],
        [lax.all_gather(projected, "tp", tiled=True), middle],
        last=True,
    )


def solution(mesh):
    return jax.shard_map(
        on_device,
        mesh=mesh,
        in_specs=(
            P(("grp", "dp"), "kv"),
            P("kv"),
            P("kv", "tp"),
            P(("grp", "dp"), "kv", "tp", None),
            P(("grp", "dp"), "kv", "tp", None),
            P("tp"),
            P(),
            P("tp", "kv"),
            P("kv"),
            P("kv", "tp"),
            P("kv", "tp"),
            P("tp", "kv"),
        ),
        out_specs=P(("grp", "dp"), "kv"),
        check_vma=False,
    )
```

```python
import functools

import jax
import jax.numpy as jnp
import numpy as np
from jax import lax
from jax.experimental import pallas as pl
from jax.experimental.pallas import tpu as pltpu
from jax.sharding import PartitionSpec as P

HD = 64
VD = 128
LANES = 128
PACKED = 2
EXTRA = 8

KERNEL_VMEM = 8 << 20

ROPE_BASE = 500000.0
EPSILON = 1e-06
KEEP_SCALE = 0.8
F32 = jnp.float32
BF16 = jnp.bfloat16


def split(value, terms):
    parts = []
    for _ in range(terms):
        part = value.astype(BF16).astype(F32)
        parts.append(part)
        value = value - part
    return parts


def lanes_of(columns, rows, width):
    lane = lax.broadcasted_iota(jnp.int32, (rows, width), 1)
    out = jnp.zeros((rows, width), F32)
    for k, column in enumerate(columns):
        out = jnp.where(lane == k, column, out)
    return out


def rows_of(lines, width):
    row = lax.broadcasted_iota(jnp.int32, (EXTRA, width), 0)
    out = jnp.zeros((EXTRA, width), F32)
    for k, line in enumerate(lines):
        out = jnp.where(row == k, line, out)
    return out


def turned(rows):
    pad = jnp.zeros((LANES - rows.shape[0], LANES), F32)
    return jnp.concatenate([rows, pad], axis=0).T


def query_kernel(tokens, gain, weight, table, out, table_here, *scratch):
    tokens_here, gain_here, weight_here, semaphores = scratch
    copies = [
        pltpu.make_async_copy(source, target, semaphores.at[k])
        for k, (source, target) in enumerate(
            (
                (weight, weight_here),
                (tokens, tokens_here),
                (gain, gain_here),
                (table, table_here),
            )
        )
    ]
    for copy in copies:
        copy.start()
    for copy in copies[:3]:
        copy.wait()
    tok = tokens_here[...].astype(F32)
    scaled = (tok * gain_here[...]).astype(BF16)
    partial = jnp.dot(scaled, weight_here[...], preferred_element_type=F32)
    squares = jnp.sum(tok * tok, axis=1, keepdims=True)
    count, seq_rows, lanes = out.shape
    share = lanes - LANES
    extra = lanes_of(split(squares, 2), seq_rows, LANES).astype(BF16)
    for k in range(count):
        out[k, :, :share] = partial[:, k * share : (k + 1) * share].astype(BF16)
        out[k, :, share:] = extra
    for copy in copies[3:]:
        copy.wait()


def join_kernel(parts, out):
    total = parts[0].astype(F32)
    for k in range(1, parts.shape[0]):
        total = total + parts[k].astype(F32)
    own, extra = total[:, :-LANES], total[:, -LANES:]
    squares = extra[:, 0:1] + extra[:, 1:2]
    seq_rows = total.shape[0]
    lane = lax.broadcasted_iota(jnp.int32, (seq_rows, LANES), 1)
    at = lax.broadcasted_iota(jnp.int32, (seq_rows, LANES), 0) // PACKED * 2
    high, low = split(squares, 2)
    extra = jnp.where(lane == at, high, jnp.where(lane == at + 1, low, 0.0))
    pieces = [own[r : r + PACKED] for r in range(0, seq_rows, PACKED)]
    pieces.append(sum(extra[r : r + PACKED] for r in range(0, seq_rows, PACKED)))
    sent = jnp.concatenate(pieces, axis=1).astype(BF16)
    for k in range(out.shape[0]):
        out[k] = sent


def attend_kernel(
    features, near, parts, table, keys, values, out, query, squares, turned_query, score_rows
):
    count = parts.shape[0]
    seq_rows, width = query.shape
    share = width // near
    for side in range(near):
        total = parts[side].astype(F32)
        for k in range(side + near, count, near):
            total = total + parts[k].astype(F32)
        for r in range(seq_rows // PACKED):
            rows = slice(r * PACKED, (r + 1) * PACKED)
            query[rows, side * share : (side + 1) * share] = total[:, r * share : (r + 1) * share]
            if side == 0:
                extra = total[:, seq_rows // PACKED * share :]
                both = extra[:, 2 * r : 2 * r + 1] + extra[:, 2 * r + 1 : 2 * r + 2]
                squares[rows] = jnp.broadcast_to(both, (PACKED, LANES))
    scale = lax.rsqrt(squares[...] / features + EPSILON)
    heads = width // (2 * HD)
    lane = lax.broadcasted_iota(jnp.int32, (seq_rows, LANES), 1)
    first = lane % HD < HD // 2
    cosine, sine = table[0:1], table[1:2]
    for g in range(heads):
        part = query[:, g * LANES : (g + 1) * LANES] * scale
        other = jnp.where(first, pltpu.roll(part, LANES - HD // 2, 1), pltpu.roll(part, HD // 2, 1))
        turned_query[g * seq_rows : (g + 1) * seq_rows] = part * cosine + other * sine
    map_zero = lax.broadcasted_iota(jnp.int32, (heads, LANES), 1) < HD
    block = 2 * heads
    for s in range(seq_rows):
        part = turned_query[pl.ds(s, heads, stride=seq_rows)]
        both = jnp.concatenate(
            [jnp.where(map_zero, part, 0.0), jnp.where(map_zero, 0.0, part)], axis=0
        ).astype(BF16)
        score_rows[s * block : (s + 1) * block] = lax.dot_general(
            both, keys[s], (((1,), (1,)), ((), ())), preferred_element_type=F32
        )
    rows = block * seq_rows
    scores = score_rows[...] * HD ** (-0.5)
    row_max = jnp.max(scores, axis=1, keepdims=True)
    exponent = jnp.exp(scores - row_max)
    row_total = jnp.sum(exponent, axis=1, keepdims=True)
    weights = exponent.astype(BF16)
    both = lanes_of([row_max, row_total], rows, LANES).T
    lines = rows_of(split(both[0:1], 3) + split(both[1:2], 2), rows)
    quarter = rows // out.shape[0]
    for k in range(out.shape[0]):
        own = lines if k == 0 else pltpu.roll(lines, rows - k * quarter, 1)
        out[k, quarter:] = own.astype(BF16)
    for s in range(seq_rows):
        k, at = divmod(s * block, quarter)
        out[k, at : at + block] = jnp.dot(
            weights[s * block : (s + 1) * block], values[s], preferred_element_type=F32
        ).astype(BF16)


def maxima_of(parts, sources, rows):
    extra = [parts[k, rows:].astype(F32) for k in sources]
    maxima = jnp.concatenate([e[0:1] + e[1:2] + e[2:3] for e in extra], axis=0)
    totals = jnp.concatenate([e[3:4] + e[4:5] for e in extra], axis=0)
    return maxima, totals


def quarter_kernel(parts, ahead, out):
    count = parts.shape[0]
    rows = parts.shape[1] - EXTRA
    maxima, totals = maxima_of(parts, range(count), rows)
    joint = jnp.max(maxima, axis=0, keepdims=True)
    factors = jnp.exp(maxima - joint)
    total = jnp.sum(totals * factors, axis=0, keepdims=True)
    columns = turned(factors)
    joined = jnp.zeros((rows, VD), F32)
    for k in range(count):
        joined = joined + parts[k, :rows].astype(F32) * columns[:rows, k : k + 1]
    lane = lax.broadcasted_iota(jnp.int32, (PACKED, VD), 1)
    row = lax.broadcasted_iota(jnp.int32, (PACKED, VD), 0)
    extra = jnp.zeros((PACKED, VD), F32)
    for k, line in enumerate(split(joint, 3) + split(total, 2)):
        at, slot = divmod(k * rows, VD)
        line = pltpu.roll(jnp.broadcast_to(line, (PACKED, VD)), slot, 1) if slot else line
        extra = jnp.where((row == at) & (lane >= slot) & (lane < slot + rows), line, extra)
    pieces = [joined[r : r + PACKED] for r in range(0, rows, PACKED)]
    sent = jnp.concatenate([*pieces, extra], axis=1).astype(BF16)
    for k in range(out.shape[0]):
        out[k] = sent


def heads_kernel(near, parts, lambdas, gain, weight, out, blocks, normed):
    count, quarter, _ = blocks.shape
    far = count // near
    heads = lambdas.shape[1]
    block = 2 * heads
    seq_rows = near * quarter // block
    square = (heads, heads)
    diagonal = lax.broadcasted_iota(jnp.int32, square, 0) == lax.broadcasted_iota(jnp.int32, square, 1)
    lambda_column = jnp.sum(jnp.where(diagonal, lambdas[...], 0.0), axis=1, keepdims=True)
    extra = []
    for j in [a * near + k for k in range(near) for a in range(far)]:
        part = parts[j].astype(F32)
        for r in range(quarter // PACKED):
            blocks[j, r * PACKED : (r + 1) * PACKED] = part[:, r * VD : (r + 1) * VD]
        extra.append(part[:, quarter // PACKED * VD :])
    extra = [jnp.concatenate([e[r : r + 1] for e in extra], axis=0) for r in range(PACKED)]
    lines = []
    for k in range(5):
        at, slot = divmod(k * quarter, VD)
        lines.append(pltpu.roll(extra[at], VD - slot, 1) if slot else extra[at])
    maxima, totals = lines[0] + lines[1] + lines[2], lines[3] + lines[4]
    factors = []
    for k in range(near):
        own = slice(k * far, (k + 1) * far)
        factor = jnp.exp(maxima[own] - jnp.max(maxima[own], axis=0, keepdims=True))
        factors.append(factor / jnp.sum(totals[own] * factor, axis=0, keepdims=True))
    columns = turned(jnp.concatenate(factors, axis=0))
    for s in range(seq_rows):
        k, row = divmod(s * block, quarter)
        averaged = jnp.zeros((block, VD), F32)
        for a in range(far):
            part = blocks[a * near + k, row : row + block]
            at = k * far + a
            averaged = averaged + part * columns[row : row + block, at : at + 1]
        difference = averaged[:heads] - lambda_column * averaged[heads:]
        mean = jnp.mean(difference * difference, axis=1, keepdims=True)
        normed[s * heads : (s + 1) * heads] = (
            difference * lax.rsqrt(mean + EPSILON) * gain[...] * KEEP_SCALE
        )
    heads_out = jnp.concatenate(
        [normed[pl.ds(g, seq_rows, stride=heads)].astype(BF16) for g in range(heads)], axis=1
    )
    out[...] = jnp.dot(heads_out, weight[...], preferred_element_type=F32).astype(BF16)


def window(array, start, width):
    low = start // LANES * LANES
    tiles = -(-(start - low + width) // LANES) * LANES
    part = array[:, low : low + tiles]
    if start > low:
        part = pltpu.roll(part, tiles - (start - low), 1)
    return part


def gate_kernel(attended, tokens, gain, gate_weight, up_weight, out, middle):
    seq_rows = tokens.shape[0]
    total = attended[:seq_rows].astype(F32) + attended[seq_rows:].astype(F32)
    mid = (tokens[...].astype(F32) + total).astype(BF16)
    middle[...] = mid
    mid = mid.astype(F32)
    mixer_in = (mid * gain[...]).astype(BF16)
    gate = jnp.dot(mixer_in, gate_weight[...], preferred_element_type=F32)
    up = jnp.dot(mixer_in, up_weight[...], preferred_element_type=F32)
    squares = jnp.sum(mid * mid, axis=1, keepdims=True)
    high, low = split(squares, 2)
    count, _, width = out.shape
    share = gate.shape[1] // count
    lane = lax.broadcasted_iota(jnp.int32, (seq_rows, width), 1)
    for k in range(count):
        parts = []
        for array in (gate, up):
            part = window(array, k * share, share)[:, :width]
            if part.shape[1] < width:
                pad = jnp.zeros((seq_rows, width - part.shape[1]), F32)
                part = jnp.concatenate([part, pad], axis=1)
            parts.append(part)
        both = jnp.where(lane < share, parts[0], pltpu.roll(parts[1], share, 1))
        both = jnp.where(lane == 2 * share, high, both)
        both = jnp.where(lane == 2 * share + 1, low, both)
        out[k] = both.astype(BF16)


def hidden_kernel(features, share, parts, out):
    count, seq_rows, width = parts.shape
    total = parts[0].astype(F32)
    for k in range(1, count):
        total = total + parts[k].astype(F32)
    squares = total[:, 2 * share : 2 * share + 1] + total[:, 2 * share + 1 : 2 * share + 2]
    scale = lax.rsqrt(squares / features + EPSILON)
    scaled = total * scale
    tiles = -(-share // LANES) * LANES
    lane = lax.broadcasted_iota(jnp.int32, (seq_rows, tiles), 1)
    gate = jnp.where(lane < share, scaled[:, :tiles], 0.0)
    up = pltpu.roll(scaled, width - share, 1)[:, :tiles]
    hidden = gate / (1.0 + jnp.exp(-gate)) * up
    lanes = out.shape[2]
    hidden = jnp.concatenate([hidden, jnp.zeros((seq_rows, lanes - hidden.shape[1]), F32)], axis=1)
    sent = hidden[:PACKED]
    for r in range(1, seq_rows // PACKED):
        sent = sent + pltpu.roll(hidden[r * PACKED : (r + 1) * PACKED], r * share, 1)
    sent = sent.astype(BF16)
    for k in range(count):
        out[k] = sent


def down_kernel(share, hidden, weight, out, blocks):
    count, _, lanes = hidden.shape
    seq_rows, tiles = blocks.shape[1:]
    for k in range(count):
        part = hidden[k].astype(F32)
        for r in range(seq_rows // PACKED):
            moved = pltpu.roll(part, lanes - r * share, 1) if r else part
            blocks[k, r * PACKED : (r + 1) * PACKED] = moved[:, :tiles]
    total = jnp.zeros(out.shape, F32)
    for k in range(count):
        total = total + jnp.dot(
            blocks[k, :, :share].astype(BF16),
            weight[k * share : (k + 1) * share],
            preferred_element_type=F32,
        )
    out[...] = total.astype(BF16)


def final_kernel(parts, middle, out):
    seq_rows = middle.shape[0]
    mixed = parts[:seq_rows].astype(F32) + parts[seq_rows:].astype(F32)
    out[...] = (middle[...].astype(F32) + mixed).astype(BF16)


def rotation(context):
    frequency = ROPE_BASE ** (-np.arange(HD // 2) * 2.0 / HD)
    angles = context * frequency
    cosine, sine = np.cos(angles), np.sin(angles)
    table = [np.tile(cosine, LANES // (HD // 2)), np.tile(np.concatenate([-sine, sine]), LANES // HD)]
    return np.stack(table + [np.zeros(LANES)] * 6).astype(np.float32)


def on_device(
    tokens,
    attend_gain,
    query_weight,
    cache_keys,
    cache_values,
    head_lambda,
    head_gain,
    output_weight,
    mixer_gain,
    gate_weight,
    up_weight,
    down_weight,
):
    kv_size = lax.axis_size("kv")
    seq_rows, features_here = tokens.shape
    features = features_here * kv_size
    heads = head_lambda.shape[0]
    positions = cache_keys.shape[1]
    rows = 2 * heads * seq_rows
    share = gate_weight.shape[1] // kv_size
    padded = -(-(2 * share + 2) // LANES) * LANES
    near = 4
    neighbours = [list(range(k, k + near)) for k in range(0, kv_size, near)]
    keys = cache_keys.reshape(seq_rows, positions, 2 * HD)
    values = cache_values.reshape(seq_rows, positions, VD)
    width = query_weight.shape[1]

    def call(kernel, outs, here, hbm=(), scratch=(), last=False, cost=None):
        spec = pl.BlockSpec(memory_space=pltpu.VMEM)
        away = pl.BlockSpec(memory_space=pltpu.HBM)
        space = jax.ShapeDtypeStruct if last else pltpu.VMEM
        outs = tuple(space(shape, kind) for shape, kind in outs)
        here = [pltpu.with_memory_space_constraint(a, pltpu.VMEM) for a in here]
        hbm = [pltpu.with_memory_space_constraint(a, pltpu.HBM) for a in hbm]
        results = pl.pallas_call(
            kernel,
            out_shape=outs,
            in_specs=[spec] * len(here) + [away] * len(hbm),
            out_specs=(spec,) * len(outs),
            scratch_shapes=list(scratch),
            compiler_params=pltpu.CompilerParams(vmem_limit_bytes=KERNEL_VMEM),
            cost_estimate=cost,
        )(*here, *hbm)
        return results[0] if len(outs) == 1 else results

    def exchange(array, groups=None):
        return lax.all_to_all(array, "kv", 0, 0, axis_index_groups=groups, tiled=True)

    gain = attend_gain[None]
    table = jnp.asarray(rotation(positions * kv_size))
    part, table = call(
        query_kernel,
        [((near, seq_rows, width // near + LANES), BF16), (table.shape, F32)],
        [],
        [tokens, gain, query_weight, table],
        scratch=[
            pltpu.VMEM(tokens.shape, BF16),
            pltpu.VMEM(gain.shape, F32),
            pltpu.VMEM(query_weight.shape, BF16),
            pltpu.SemaphoreType.DMA((4,)),
        ],
    )
    sent = call(
        join_kernel,
        [((kv_size, PACKED, seq_rows // PACKED * (width // near) + LANES), BF16)],
        [exchange(part, neighbours)],
        cost=pl.CostEstimate(flops=10**9, bytes_accessed=10**7, transcendentals=0),
    )
    sent = call(
        functools.partial(attend_kernel, features, near),
        [((near, rows // near + EXTRA, VD), BF16)],
        [exchange(sent), table, keys, values],
        scratch=[
            pltpu.VMEM((seq_rows, width), F32),
            pltpu.VMEM((seq_rows, LANES), F32),
            pltpu.VMEM((heads * seq_rows, LANES), F32),
            pltpu.VMEM((rows, positions), F32),
        ],
    )
    sent = call(
        quarter_kernel,
        [((kv_size, PACKED, (rows // near // PACKED + 1) * VD), BF16)],
        [exchange(sent, neighbours), mixer_gain[None]],
    )
    attended = call(
        functools.partial(heads_kernel, near),
        [((seq_rows, features_here), BF16)],
        [exchange(sent), head_lambda[None], head_gain[None], output_weight],
        scratch=[
            pltpu.VMEM((kv_size, rows // near, VD), F32),
            pltpu.VMEM((heads * seq_rows, VD), F32),
        ],
    )
    sent, middle = call(
        gate_kernel,
        [((kv_size, seq_rows, padded), BF16), ((seq_rows, features_here), BF16)],
        [
            lax.all_gather(attended, "tp", tiled=True),
            tokens,
            mixer_gain[None],
            gate_weight,
            up_weight,
        ],
    )
    sent = call(
        functools.partial(hidden_kernel, features, share),
        [((kv_size, PACKED, -(-(seq_rows // PACKED * share) // LANES) * LANES), BF16)],
        [exchange(sent)],
    )
    projected = call(
        functools.partial(down_kernel, share),
        [((seq_rows, features_here), BF16)],
        [exchange(sent), down_weight],
        scratch=[pltpu.VMEM((kv_size, seq_rows, -(-share // LANES) * LANES), F32)],
    )
    return call(
        final_kernel,
        [((seq_rows, features_here), BF16)],
        [lax.all_gather(projected, "tp", tiled=True), middle],
        last=True,
    )


def solution(mesh):
    return jax.shard_map(
        on_device,
        mesh=mesh,
        in_specs=(
            P(("grp", "dp"), "kv"),
            P("kv"),
            P("kv", "tp"),
            P(("grp", "dp"), "kv", "tp", None),
            P(("grp", "dp"), "kv", "tp", None),
            P("tp"),
            P(),
            P("tp", "kv"),
            P("kv"),
            P("kv", "tp"),
            P("kv", "tp"),
            P("tp", "kv"),
        ),
        out_specs=P(("grp", "dp"), "kv"),
        check_vma=False,
    )
```

```python
import functools

import jax
import jax.numpy as jnp
import numpy as np
from jax import lax
from jax.experimental import pallas as pl
from jax.experimental.pallas import tpu as pltpu
from jax.sharding import PartitionSpec as P

HD = 64
VD = 128
LANES = 128
PACKED = 2
TERMS = 5
EXTRA = 8

KERNEL_VMEM = 8 << 20

ROPE_BASE = 500000.0
EPSILON = 1e-06
KEEP_SCALE = 0.8
F32 = jnp.float32
BF16 = jnp.bfloat16


def split(value, terms):
    parts = []
    for _ in range(terms):
        part = value.astype(BF16).astype(F32)
        parts.append(part)
        value = value - part
    return parts


def lanes_of(columns, rows, width):
    lane = lax.broadcasted_iota(jnp.int32, (rows, width), 1)
    out = jnp.zeros((rows, width), F32)
    for k, column in enumerate(columns):
        out = jnp.where(lane == k, column, out)
    return out


def rows_of(lines, width):
    row = lax.broadcasted_iota(jnp.int32, (EXTRA, width), 0)
    out = jnp.zeros((EXTRA, width), F32)
    for k, line in enumerate(lines):
        out = jnp.where(row == k, line, out)
    return out


def turned(rows):
    pad = jnp.zeros((LANES - rows.shape[0], LANES), F32)
    return jnp.concatenate([rows, pad], axis=0).T


def query_kernel(tokens, gain, weight, table, out, table_here, *scratch):
    tokens_here, gain_here, weight_here, semaphores = scratch
    copies = [
        pltpu.make_async_copy(source, target, semaphores.at[k])
        for k, (source, target) in enumerate(
            (
                (weight, weight_here),
                (tokens, tokens_here),
                (gain, gain_here),
                (table, table_here),
            )
        )
    ]
    for copy in copies:
        copy.start()
    for copy in copies[:3]:
        copy.wait()
    tok = tokens_here[...].astype(F32)
    scaled = (tok * gain_here[...]).astype(BF16)
    partial = jnp.dot(scaled, weight_here[...], preferred_element_type=F32)
    squares = jnp.sum(tok * tok, axis=1, keepdims=True)
    width = partial.shape[1]
    out[:, :width] = partial.astype(BF16)
    out[:, width:] = lanes_of(split(squares, 2), tok.shape[0], LANES).astype(BF16)
    for copy in copies[3:]:
        copy.wait()


def halves_kernel(odd, parts, out):
    total = parts[0].astype(F32) + parts[1].astype(F32)
    half = (total.shape[1] - LANES) // 2
    own = jnp.where(odd[:, :1] > 0, total[:, half : 2 * half], total[:, :half])
    extra = total[:, 2 * half :]
    squares = extra[:, 0:1] + extra[:, 1:2]
    seq_rows = total.shape[0]
    lane = lax.broadcasted_iota(jnp.int32, (seq_rows, LANES), 1)
    at = lax.broadcasted_iota(jnp.int32, (seq_rows, LANES), 0) // PACKED * 2
    high, low = split(squares, 2)
    extra = jnp.where(lane == at, high, jnp.where(lane == at + 1, low, 0.0))
    pieces = [own[r : r + PACKED] for r in range(0, seq_rows, PACKED)]
    pieces.append(sum(extra[r : r + PACKED] for r in range(0, seq_rows, PACKED)))
    sent = jnp.concatenate(pieces, axis=1).astype(BF16)
    for k in range(out.shape[0]):
        out[k] = sent


def attend_kernel(features, parts, table, keys, values, out, query, squares, turned_query, score_rows):
    count = parts.shape[0]
    seq_rows, width = query.shape
    half = width // 2
    for odd in range(2):
        total = parts[odd].astype(F32)
        for k in range(odd + 2, count, 2):
            total = total + parts[k].astype(F32)
        for r in range(seq_rows // PACKED):
            rows = slice(r * PACKED, (r + 1) * PACKED)
            query[rows, odd * half : (odd + 1) * half] = total[:, r * half : (r + 1) * half]
            if odd == 0:
                extra = total[:, seq_rows // PACKED * half :]
                both = extra[:, 2 * r : 2 * r + 1] + extra[:, 2 * r + 1 : 2 * r + 2]
                squares[rows] = jnp.broadcast_to(both, (PACKED, LANES))
    scale = lax.rsqrt(squares[...] / features + EPSILON)
    heads = 2 * half // (2 * HD)
    lane = lax.broadcasted_iota(jnp.int32, (seq_rows, LANES), 1)
    first = lane % HD < HD // 2
    cosine, sine = table[0:1], table[1:2]
    for g in range(heads):
        part = query[:, g * LANES : (g + 1) * LANES] * scale
        other = jnp.where(first, pltpu.roll(part, LANES - HD // 2, 1), pltpu.roll(part, HD // 2, 1))
        turned_query[g * seq_rows : (g + 1) * seq_rows] = part * cosine + other * sine
    map_zero = lax.broadcasted_iota(jnp.int32, (heads, LANES), 1) < HD
    block = 2 * heads
    for s in range(seq_rows):
        part = turned_query[pl.ds(s, heads, stride=seq_rows)]
        both = jnp.concatenate(
            [jnp.where(map_zero, part, 0.0), jnp.where(map_zero, 0.0, part)], axis=0
        ).astype(BF16)
        score_rows[s * block : (s + 1) * block] = lax.dot_general(
            both, keys[s], (((1,), (1,)), ((), ())), preferred_element_type=F32
        )
    rows = block * seq_rows
    scores = score_rows[...] * HD ** (-0.5)
    row_max = jnp.max(scores, axis=1, keepdims=True)
    exponent = jnp.exp(scores - row_max)
    row_total = jnp.sum(exponent, axis=1, keepdims=True)
    weights = exponent.astype(BF16)
    both = lanes_of([row_max, row_total], rows, LANES).T
    out[rows:] = rows_of(split(both[0:1], 3) + split(both[1:2], 2), rows).astype(BF16)
    for s in range(seq_rows):
        out[s * block : (s + 1) * block] = jnp.dot(
            weights[s * block : (s + 1) * block], values[s], preferred_element_type=F32
        ).astype(BF16)


def maxima_of(parts, sources, rows):
    extra = [parts[k, rows:].astype(F32) for k in sources]
    maxima = jnp.concatenate([e[0:1] + e[1:2] + e[2:3] for e in extra], axis=0)
    totals = jnp.concatenate([e[3:4] + e[4:5] for e in extra], axis=0)
    return maxima, totals


def pair_kernel(odd, parts, out, joined):
    count = parts.shape[0]
    rows = parts.shape[1] - EXTRA
    half = rows // 2
    maxima, totals = maxima_of(parts, range(count), rows)
    joint = jnp.max(maxima, axis=0, keepdims=True)
    factors = jnp.exp(maxima - joint)
    total = jnp.sum(totals * factors, axis=0, keepdims=True)
    columns = turned(factors)
    both = jnp.zeros((rows, VD), F32)
    for k in range(count):
        both = both + parts[k, :rows].astype(F32) * columns[:, k : k + 1]
    joined[...] = jnp.where(odd[:1] > 0, both[half:], both[:half])
    lines = rows_of(split(joint, 3) + split(total, 2), VD)
    lines = jnp.where(odd[...] > 0, pltpu.roll(lines, VD - half, 1), lines)
    width = out.shape[2] - half // PACKED * VD
    lane = lax.broadcasted_iota(jnp.int32, (PACKED, width), 1)
    row = lax.broadcasted_iota(jnp.int32, (PACKED, width), 0)
    extra = jnp.zeros((PACKED, width), F32)
    for k in range(TERMS):
        at, slot = divmod(k * half, width)
        line = jnp.broadcast_to(lines[k : k + 1], (PACKED, VD))
        line = pltpu.roll(line, slot % VD, 1) if slot % VD else line
        line = jnp.concatenate([line] * (width // VD), axis=1)
        extra = jnp.where((row == at) & (lane >= slot) & (lane < slot + half), line, extra)
    pieces = [joined[r : r + PACKED] for r in range(0, half, PACKED)]
    sent = jnp.concatenate([*pieces, extra], axis=1).astype(BF16)
    for k in range(out.shape[0]):
        out[k] = sent


def heads_kernel(near, parts, lambdas, gain, weight, ahead, out, blocks, normed):
    count, quarter, _ = blocks.shape
    far = count // near
    heads = lambdas.shape[1]
    block = 2 * heads
    seq_rows = near * quarter // block
    square = (heads, heads)
    diagonal = lax.broadcasted_iota(jnp.int32, square, 0) == lax.broadcasted_iota(jnp.int32, square, 1)
    lambda_column = jnp.sum(jnp.where(diagonal, lambdas[...], 0.0), axis=1, keepdims=True)
    extra = []
    for j in [a * near + k for k in range(near) for a in range(far)]:
        part = parts[j].astype(F32)
        for r in range(quarter // PACKED):
            blocks[j, r * PACKED : (r + 1) * PACKED] = part[:, r * VD : (r + 1) * VD]
        extra.append(part[:, quarter // PACKED * VD :])
    extra = [jnp.concatenate([e[r : r + 1] for e in extra], axis=0) for r in range(PACKED)]
    lines = []
    width = extra[0].shape[1]
    for k in range(TERMS):
        at, slot = divmod(k * quarter, width)
        line = pltpu.roll(extra[at], width - slot, 1) if slot else extra[at]
        lines.append(line[:, :VD])
    maxima, totals = lines[0] + lines[1] + lines[2], lines[3] + lines[4]
    factors = []
    for k in range(near):
        own = slice(k * far, (k + 1) * far)
        factor = jnp.exp(maxima[own] - jnp.max(maxima[own], axis=0, keepdims=True))
        factors.append(factor / jnp.sum(totals[own] * factor, axis=0, keepdims=True))
    columns = turned(jnp.concatenate(factors, axis=0))
    for s in range(seq_rows):
        k, row = divmod(s * block, quarter)
        averaged = jnp.zeros((block, VD), F32)
        for a in range(far):
            part = blocks[a * near + k, row : row + block]
            at = k * far + a
            averaged = averaged + part * columns[row : row + block, at : at + 1]
        difference = averaged[:heads] - lambda_column * averaged[heads:]
        mean = jnp.mean(difference * difference, axis=1, keepdims=True)
        normed[s * heads : (s + 1) * heads] = (
            difference * lax.rsqrt(mean + EPSILON) * gain[...] * KEEP_SCALE
        )
    heads_out = jnp.concatenate(
        [normed[pl.ds(g, seq_rows, stride=heads)].astype(BF16) for g in range(heads)], axis=1
    )
    out[...] = jnp.dot(heads_out, weight[...], preferred_element_type=F32).astype(BF16)


def window(array, start, width):
    low = start // LANES * LANES
    tiles = -(-(start - low + width) // LANES) * LANES
    part = array[:, low : low + tiles]
    if start > low:
        part = pltpu.roll(part, tiles - (start - low), 1)
    return part


def gate_kernel(attended, tokens, gain, gate_weight, up_weight, out, middle):
    seq_rows = tokens.shape[0]
    total = attended[:seq_rows].astype(F32) + attended[seq_rows:].astype(F32)
    mid = (tokens[...].astype(F32) + total).astype(BF16)
    middle[...] = mid
    mid = mid.astype(F32)
    mixer_in = (mid * gain[...]).astype(BF16)
    gate = jnp.dot(mixer_in, gate_weight[...], preferred_element_type=F32)
    up = jnp.dot(mixer_in, up_weight[...], preferred_element_type=F32)
    squares = jnp.sum(mid * mid, axis=1, keepdims=True)
    high, low = split(squares, 2)
    count, _, width = out.shape
    share = gate.shape[1] // count
    lane = lax.broadcasted_iota(jnp.int32, (seq_rows, width), 1)
    for k in range(count):
        parts = []
        for array in (gate, up):
            part = window(array, k * share, share)[:, :width]
            if part.shape[1] < width:
                pad = jnp.zeros((seq_rows, width - part.shape[1]), F32)
                part = jnp.concatenate([part, pad], axis=1)
            parts.append(part)
        both = jnp.where(lane < share, parts[0], pltpu.roll(parts[1], share, 1))
        both = jnp.where(lane == 2 * share, high, both)
        both = jnp.where(lane == 2 * share + 1, low, both)
        out[k] = both.astype(BF16)


def hidden_kernel(features, share, parts, out):
    count, seq_rows, width = parts.shape
    total = parts[0].astype(F32)
    for k in range(1, count):
        total = total + parts[k].astype(F32)
    squares = total[:, 2 * share : 2 * share + 1] + total[:, 2 * share + 1 : 2 * share + 2]
    scale = lax.rsqrt(squares / features + EPSILON)
    scaled = total * scale
    tiles = -(-share // LANES) * LANES
    lane = lax.broadcasted_iota(jnp.int32, (seq_rows, tiles), 1)
    gate = jnp.where(lane < share, scaled[:, :tiles], 0.0)
    up = pltpu.roll(scaled, width - share, 1)[:, :tiles]
    hidden = gate / (1.0 + jnp.exp(-gate)) * up
    lanes = out.shape[2]
    hidden = jnp.concatenate([hidden, jnp.zeros((seq_rows, lanes - hidden.shape[1]), F32)], axis=1)
    sent = hidden[:PACKED]
    for r in range(1, seq_rows // PACKED):
        sent = sent + pltpu.roll(hidden[r * PACKED : (r + 1) * PACKED], r * share, 1)
    sent = sent.astype(BF16)
    for k in range(count):
        out[k] = sent


def down_kernel(share, hidden, weight, out, blocks):
    count, _, lanes = hidden.shape
    seq_rows, tiles = blocks.shape[1:]
    for k in range(count):
        part = hidden[k].astype(F32)
        for r in range(seq_rows // PACKED):
            moved = pltpu.roll(part, lanes - r * share, 1) if r else part
            blocks[k, r * PACKED : (r + 1) * PACKED] = moved[:, :tiles]
    total = jnp.zeros(out.shape, F32)
    for k in range(count):
        total = total + jnp.dot(
            blocks[k, :, :share].astype(BF16),
            weight[k * share : (k + 1) * share],
            preferred_element_type=F32,
        )
    out[...] = total.astype(BF16)


def final_kernel(parts, middle, out):
    seq_rows = middle.shape[0]
    mixed = parts[:seq_rows].astype(F32) + parts[seq_rows:].astype(F32)
    out[...] = (middle[...].astype(F32) + mixed).astype(BF16)


def rotation(context):
    frequency = ROPE_BASE ** (-np.arange(HD // 2) * 2.0 / HD)
    angles = context * frequency
    cosine, sine = np.cos(angles), np.sin(angles)
    table = [np.tile(cosine, LANES // (HD // 2)), np.tile(np.concatenate([-sine, sine]), LANES // HD)]
    return np.stack(table + [np.zeros(LANES)] * 6).astype(np.float32)


def on_device(
    tokens,
    attend_gain,
    query_weight,
    cache_keys,
    cache_values,
    head_lambda,
    head_gain,
    output_weight,
    mixer_gain,
    gate_weight,
    up_weight,
    down_weight,
):
    kv_size = lax.axis_size("kv")
    seq_rows, features_here = tokens.shape
    features = features_here * kv_size
    heads = head_lambda.shape[0]
    positions = cache_keys.shape[1]
    rows = 2 * heads * seq_rows
    share = gate_weight.shape[1] // kv_size
    padded = -(-(2 * share + 2) // LANES) * LANES
    near = 2
    pairs = [[k, k + 1] for k in range(0, kv_size, 2)]
    extra = -(-TERMS * rows // near // PACKED // (2 * LANES)) * 2 * LANES
    odd = jnp.broadcast_to((lax.axis_index("kv") & 1).astype(F32), (seq_rows, LANES))
    tokens, odd = lax.optimization_barrier((tokens, odd))
    keys = cache_keys.reshape(seq_rows, positions, 2 * HD)
    values = cache_values.reshape(seq_rows, positions, VD)
    width = query_weight.shape[1]

    def call(kernel, outs, here, hbm=(), scratch=(), last=False, cost=None):
        spec = pl.BlockSpec(memory_space=pltpu.VMEM)
        away = pl.BlockSpec(memory_space=pltpu.HBM)
        space = jax.ShapeDtypeStruct if last else pltpu.VMEM
        outs = tuple(space(shape, kind) for shape, kind in outs)
        here = [pltpu.with_memory_space_constraint(a, pltpu.VMEM) for a in here]
        hbm = [pltpu.with_memory_space_constraint(a, pltpu.HBM) for a in hbm]
        results = pl.pallas_call(
            kernel,
            out_shape=outs,
            in_specs=[spec] * len(here) + [away] * len(hbm),
            out_specs=(spec,) * len(outs),
            scratch_shapes=list(scratch),
            compiler_params=pltpu.CompilerParams(vmem_limit_bytes=KERNEL_VMEM),
            cost_estimate=cost,
        )(*here, *hbm)
        return results[0] if len(outs) == 1 else results

    def exchange(array, groups=None):
        return lax.all_to_all(array, "kv", 0, 0, axis_index_groups=groups, tiled=True)

    gain = attend_gain[None]
    table = jnp.asarray(rotation(positions * kv_size))
    part, table = call(
        query_kernel,
        [((seq_rows, width + LANES), BF16), (table.shape, F32)],
        [],
        [tokens, gain, query_weight, table],
        scratch=[
            pltpu.VMEM(tokens.shape, BF16),
            pltpu.VMEM(gain.shape, F32),
            pltpu.VMEM(query_weight.shape, BF16),
            pltpu.SemaphoreType.DMA((4,)),
        ],
    )
    sent = call(
        halves_kernel,
        [((kv_size, PACKED, seq_rows // PACKED * (width // 2) + LANES), BF16)],
        [odd, lax.all_gather(part, "kv", axis_index_groups=pairs)],
        cost=pl.CostEstimate(flops=10**9, bytes_accessed=10**7, transcendentals=0),
    )
    sent = call(
        functools.partial(attend_kernel, features),
        [((rows + EXTRA, VD), BF16)],
        [exchange(sent), table, keys, values],
        scratch=[
            pltpu.VMEM((seq_rows, width), F32),
            pltpu.VMEM((seq_rows, LANES), F32),
            pltpu.VMEM((heads * seq_rows, LANES), F32),
            pltpu.VMEM((rows, positions), F32),
        ],
    )
    sent = call(
        pair_kernel,
        [((kv_size, PACKED, rows // near // PACKED * VD + extra), BF16)],
        [odd, lax.all_gather(sent, "kv", axis_index_groups=pairs)],
        scratch=[pltpu.VMEM((rows // near, VD), F32)],
    )
    attended = call(
        functools.partial(heads_kernel, near),
        [((seq_rows, features_here), BF16)],
        [exchange(sent), head_lambda[None], head_gain[None], output_weight, mixer_gain[None]],
        scratch=[
            pltpu.VMEM((kv_size, rows // near, VD), F32),
            pltpu.VMEM((heads * seq_rows, VD), F32),
        ],
    )
    sent, middle = call(
        gate_kernel,
        [((kv_size, seq_rows, padded), BF16), ((seq_rows, features_here), BF16)],
        [
            lax.all_gather(attended, "tp", tiled=True),
            tokens,
            mixer_gain[None],
            gate_weight,
            up_weight,
        ],
    )
    sent = call(
        functools.partial(hidden_kernel, features, share),
        [((kv_size, PACKED, -(-(seq_rows // PACKED * share) // LANES) * LANES), BF16)],
        [exchange(sent)],
    )
    projected = call(
        functools.partial(down_kernel, share),
        [((seq_rows, features_here), BF16)],
        [exchange(sent), down_weight],
        scratch=[pltpu.VMEM((kv_size, seq_rows, -(-share // LANES) * LANES), F32)],
    )
    return call(
        final_kernel,
        [((seq_rows, features_here), BF16)],
        [lax.all_gather(projected, "tp", tiled=True), middle],
        last=True,
    )


def solution(mesh):
    return jax.shard_map(
        on_device,
        mesh=mesh,
        in_specs=(
            P(("grp", "dp"), "kv"),
            P("kv"),
            P("kv", "tp"),
            P(("grp", "dp"), "kv", "tp", None),
            P(("grp", "dp"), "kv", "tp", None),
            P("tp"),
            P(),
            P("tp", "kv"),
            P("kv"),
            P("kv", "tp"),
            P("kv", "tp"),
            P("tp", "kv"),
        ),
        out_specs=P(("grp", "dp"), "kv"),
        check_vma=False,
    )
```

```python
import functools

import jax
import jax.numpy as jnp
import numpy as np
from jax import lax
from jax.experimental import pallas as pl
from jax.experimental.pallas import tpu as pltpu
from jax.sharding import PartitionSpec as P

HD = 64
VD = 128
LANES = 128
PACKED = 2
TERMS = 3
EXTRA = 8

KERNEL_VMEM = 8 << 20

ROPE_BASE = 500000.0
EPSILON = 1e-06
KEEP_SCALE = 0.8
F32 = jnp.float32
BF16 = jnp.bfloat16


def split(value, terms):
    parts = []
    for _ in range(terms):
        part = value.astype(BF16).astype(F32)
        parts.append(part)
        value = value - part
    return parts


def lanes_of(columns, rows, width):
    lane = lax.broadcasted_iota(jnp.int32, (rows, width), 1)
    out = jnp.zeros((rows, width), F32)
    for k, column in enumerate(columns):
        out = jnp.where(lane == k, column, out)
    return out


def rows_of(lines, width):
    row = lax.broadcasted_iota(jnp.int32, (EXTRA, width), 0)
    out = jnp.zeros((EXTRA, width), F32)
    for k, line in enumerate(lines):
        out = jnp.where(row == k, line, out)
    return out


def turned(rows):
    pad = jnp.zeros((LANES - rows.shape[0], LANES), F32)
    return jnp.concatenate([rows, pad], axis=0).T


def query_kernel(tokens, gain, weight, table, out, table_here, *scratch):
    tokens_here, gain_here, weight_here, semaphores = scratch
    copies = [
        pltpu.make_async_copy(source, target, semaphores.at[k])
        for k, (source, target) in enumerate(
            (
                (weight, weight_here),
                (tokens, tokens_here),
                (gain, gain_here),
                (table, table_here),
            )
        )
    ]
    for copy in copies:
        copy.start()
    for copy in copies[:3]:
        copy.wait()
    tok = tokens_here[...].astype(F32)
    scaled = (tok * gain_here[...]).astype(BF16)
    partial = jnp.dot(scaled, weight_here[...], preferred_element_type=F32)
    squares = jnp.sum(tok * tok, axis=1, keepdims=True)
    width = partial.shape[1]
    out[:, :width] = partial.astype(BF16)
    out[:, width:] = lanes_of(split(squares, 2), tok.shape[0], LANES).astype(BF16)
    for copy in copies[3:]:
        copy.wait()


def halves_kernel(odd, parts, out):
    total = parts[0].astype(F32) + parts[1].astype(F32)
    half = (total.shape[1] - LANES) // 2
    own = jnp.where(odd[:, :1] > 0, total[:, half : 2 * half], total[:, :half])
    extra = total[:, 2 * half :]
    squares = extra[:, 0:1] + extra[:, 1:2]
    seq_rows = total.shape[0]
    lane = lax.broadcasted_iota(jnp.int32, (seq_rows, LANES), 1)
    at = lax.broadcasted_iota(jnp.int32, (seq_rows, LANES), 0) // PACKED * 2
    high, low = split(squares, 2)
    extra = jnp.where(lane == at, high, jnp.where(lane == at + 1, low, 0.0))
    pieces = [own[r : r + PACKED] for r in range(0, seq_rows, PACKED)]
    pieces.append(sum(extra[r : r + PACKED] for r in range(0, seq_rows, PACKED)))
    sent = jnp.concatenate(pieces, axis=1).astype(BF16)
    for k in range(out.shape[0]):
        out[k] = sent


def attend_kernel(features, parts, table, keys, values, out, query, squares, turned_query, score_rows):
    count = parts.shape[0]
    seq_rows, width = query.shape
    half = width // 2
    for odd in range(2):
        total = parts[odd].astype(F32)
        for k in range(odd + 2, count, 2):
            total = total + parts[k].astype(F32)
        for r in range(seq_rows // PACKED):
            rows = slice(r * PACKED, (r + 1) * PACKED)
            query[rows, odd * half : (odd + 1) * half] = total[:, r * half : (r + 1) * half]
            if odd == 0:
                extra = total[:, seq_rows // PACKED * half :]
                both = extra[:, 2 * r : 2 * r + 1] + extra[:, 2 * r + 1 : 2 * r + 2]
                squares[rows] = jnp.broadcast_to(both, (PACKED, LANES))
    scale = lax.rsqrt(squares[...] / features + EPSILON)
    heads = 2 * half // (2 * HD)
    lane = lax.broadcasted_iota(jnp.int32, (seq_rows, LANES), 1)
    first = lane % HD < HD // 2
    cosine, sine = table[0:1], table[1:2]
    for g in range(heads):
        part = query[:, g * LANES : (g + 1) * LANES] * scale
        other = jnp.where(first, pltpu.roll(part, LANES - HD // 2, 1), pltpu.roll(part, HD // 2, 1))
        turned_query[g * seq_rows : (g + 1) * seq_rows] = part * cosine + other * sine
    map_zero = lax.broadcasted_iota(jnp.int32, (heads, LANES), 1) < HD
    block = 2 * heads
    for s in range(seq_rows):
        part = turned_query[pl.ds(s, heads, stride=seq_rows)]
        both = jnp.concatenate(
            [jnp.where(map_zero, part, 0.0), jnp.where(map_zero, 0.0, part)], axis=0
        ).astype(BF16)
        score_rows[s * block : (s + 1) * block] = lax.dot_general(
            both, keys[s], (((1,), (1,)), ((), ())), preferred_element_type=F32
        )
    rows = block * seq_rows
    scores = score_rows[...] * HD ** (-0.5)
    row_max = jnp.max(scores, axis=1, keepdims=True)
    exponent = jnp.exp(scores - row_max)
    row_total = jnp.sum(exponent, axis=1, keepdims=True)
    weights = exponent.astype(BF16)
    both = lanes_of([row_max, row_total], rows, LANES).T
    out[rows:] = rows_of(split(both[0:1], 3) + split(both[1:2], 2), rows).astype(BF16)
    for s in range(seq_rows):
        out[s * block : (s + 1) * block] = jnp.dot(
            weights[s * block : (s + 1) * block], values[s], preferred_element_type=F32
        ).astype(BF16)


def maxima_of(parts, sources, rows):
    extra = [parts[k, rows:].astype(F32) for k in sources]
    maxima = jnp.concatenate([e[0:1] + e[1:2] + e[2:3] for e in extra], axis=0)
    totals = jnp.concatenate([e[3:4] + e[4:5] for e in extra], axis=0)
    return maxima, totals


def pair_kernel(odd, parts, out, joined):
    count = parts.shape[0]
    rows = parts.shape[1] - EXTRA
    half = rows // 2
    maxima, totals = maxima_of(parts, range(count), rows)
    joint = jnp.max(maxima, axis=0, keepdims=True)
    factors = jnp.exp(maxima - joint)
    total = jnp.sum(totals * factors, axis=0, keepdims=True)
    columns = turned(factors / total)
    both = jnp.zeros((rows, VD), F32)
    for k in range(count):
        both = both + parts[k, :rows].astype(F32) * columns[:, k : k + 1]
    joined[...] = jnp.where(odd[:1] > 0, both[half:], both[:half])
    lines = rows_of(split(joint + jnp.log(total), TERMS), VD)
    lines = jnp.where(odd[...] > 0, pltpu.roll(lines, VD - half, 1), lines)
    width = out.shape[2] - half // PACKED * VD
    lane = lax.broadcasted_iota(jnp.int32, (PACKED, width), 1)
    row = lax.broadcasted_iota(jnp.int32, (PACKED, width), 0)
    extra = jnp.zeros((PACKED, width), F32)
    for k in range(TERMS):
        at, slot = divmod(k * half, width)
        line = jnp.broadcast_to(lines[k : k + 1], (PACKED, VD))
        line = pltpu.roll(line, slot % VD, 1) if slot % VD else line
        line = jnp.concatenate([line] * (width // VD), axis=1)
        extra = jnp.where((row == at) & (lane >= slot) & (lane < slot + half), line, extra)
    pieces = [joined[r : r + PACKED] for r in range(0, half, PACKED)]
    sent = jnp.concatenate([*pieces, extra], axis=1).astype(BF16)
    for k in range(out.shape[0]):
        out[k] = sent


def heads_kernel(near, parts, lambdas, gain, weight, ahead, out, blocks, normed):
    count, quarter, _ = blocks.shape
    far = count // near
    heads = lambdas.shape[1]
    block = 2 * heads
    seq_rows = near * quarter // block
    square = (heads, heads)
    diagonal = lax.broadcasted_iota(jnp.int32, square, 0) == lax.broadcasted_iota(jnp.int32, square, 1)
    lambda_column = jnp.sum(jnp.where(diagonal, lambdas[...], 0.0), axis=1, keepdims=True)
    extra = []
    for j in [a * near + k for k in range(near) for a in range(far)]:
        part = parts[j].astype(F32)
        for r in range(quarter // PACKED):
            blocks[j, r * PACKED : (r + 1) * PACKED] = part[:, r * VD : (r + 1) * VD]
        extra.append(part[:, quarter // PACKED * VD :])
    extra = [jnp.concatenate([e[r : r + 1] for e in extra], axis=0) for r in range(PACKED)]
    lines = []
    width = extra[0].shape[1]
    for k in range(TERMS):
        at, slot = divmod(k * quarter, width)
        line = pltpu.roll(extra[at], width - slot, 1) if slot else extra[at]
        lines.append(line[:, :VD])
    exponents = lines[0] + lines[1] + lines[2]
    factors = []
    for k in range(near):
        own = exponents[k * far : (k + 1) * far]
        factor = jnp.exp(own - jnp.max(own, axis=0, keepdims=True))
        factors.append(factor / jnp.sum(factor, axis=0, keepdims=True))
    columns = turned(jnp.concatenate(factors, axis=0))
    for s in range(seq_rows):
        k, row = divmod(s * block, quarter)
        averaged = jnp.zeros((block, VD), F32)
        for a in range(far):
            part = blocks[a * near + k, row : row + block]
            at = k * far + a
            averaged = averaged + part * columns[row : row + block, at : at + 1]
        difference = averaged[:heads] - lambda_column * averaged[heads:]
        mean = jnp.mean(difference * difference, axis=1, keepdims=True)
        normed[s * heads : (s + 1) * heads] = (
            difference * lax.rsqrt(mean + EPSILON) * gain[...] * KEEP_SCALE
        )
    heads_out = jnp.concatenate(
        [normed[pl.ds(g, seq_rows, stride=heads)].astype(BF16) for g in range(heads)], axis=1
    )
    out[...] = jnp.dot(heads_out, weight[...], preferred_element_type=F32).astype(BF16)


def window(array, start, width):
    low = start // LANES * LANES
    tiles = -(-(start - low + width) // LANES) * LANES
    part = array[:, low : low + tiles]
    if start > low:
        part = pltpu.roll(part, tiles - (start - low), 1)
    return part


def gate_kernel(attended, tokens, gain, gate_weight, up_weight, out, middle):
    seq_rows = tokens.shape[0]
    total = attended[:seq_rows].astype(F32) + attended[seq_rows:].astype(F32)
    mid = (tokens[...].astype(F32) + total).astype(BF16)
    middle[...] = mid
    mid = mid.astype(F32)
    mixer_in = (mid * gain[...]).astype(BF16)
    gate = jnp.dot(mixer_in, gate_weight[...], preferred_element_type=F32)
    up = jnp.dot(mixer_in, up_weight[...], preferred_element_type=F32)
    squares = jnp.sum(mid * mid, axis=1, keepdims=True)
    high, low = split(squares, 2)
    count, _, width = out.shape
    share = gate.shape[1] // count
    lane = lax.broadcasted_iota(jnp.int32, (seq_rows, width), 1)
    for k in range(count):
        parts = []
        for array in (gate, up):
            part = window(array, k * share, share)[:, :width]
            if part.shape[1] < width:
                pad = jnp.zeros((seq_rows, width - part.shape[1]), F32)
                part = jnp.concatenate([part, pad], axis=1)
            parts.append(part)
        both = jnp.where(lane < share, parts[0], pltpu.roll(parts[1], share, 1))
        both = jnp.where(lane == 2 * share, high, both)
        both = jnp.where(lane == 2 * share + 1, low, both)
        out[k] = both.astype(BF16)


def hidden_kernel(features, share, parts, out):
    count, seq_rows, width = parts.shape
    total = parts[0].astype(F32)
    for k in range(1, count):
        total = total + parts[k].astype(F32)
    squares = total[:, 2 * share : 2 * share + 1] + total[:, 2 * share + 1 : 2 * share + 2]
    scale = lax.rsqrt(squares / features + EPSILON)
    scaled = total * scale
    tiles = -(-share // LANES) * LANES
    lane = lax.broadcasted_iota(jnp.int32, (seq_rows, tiles), 1)
    gate = jnp.where(lane < share, scaled[:, :tiles], 0.0)
    up = pltpu.roll(scaled, width - share, 1)[:, :tiles]
    hidden = gate / (1.0 + jnp.exp(-gate)) * up
    lanes = out.shape[2]
    hidden = jnp.concatenate([hidden, jnp.zeros((seq_rows, lanes - hidden.shape[1]), F32)], axis=1)
    sent = hidden[:PACKED]
    for r in range(1, seq_rows // PACKED):
        sent = sent + pltpu.roll(hidden[r * PACKED : (r + 1) * PACKED], r * share, 1)
    sent = sent.astype(BF16)
    for k in range(count):
        out[k] = sent


def down_kernel(share, hidden, weight, out, blocks):
    count, _, lanes = hidden.shape
    seq_rows, tiles = blocks.shape[1:]
    for k in range(count):
        part = hidden[k].astype(F32)
        for r in range(seq_rows // PACKED):
            moved = pltpu.roll(part, lanes - r * share, 1) if r else part
            blocks[k, r * PACKED : (r + 1) * PACKED] = moved[:, :tiles]
    total = jnp.zeros(out.shape, F32)
    for k in range(count):
        total = total + jnp.dot(
            blocks[k, :, :share].astype(BF16),
            weight[k * share : (k + 1) * share],
            preferred_element_type=F32,
        )
    out[...] = total.astype(BF16)


def final_kernel(parts, middle, out):
    seq_rows = middle.shape[0]
    mixed = parts[:seq_rows].astype(F32) + parts[seq_rows:].astype(F32)
    out[...] = (middle[...].astype(F32) + mixed).astype(BF16)


def rotation(context):
    frequency = ROPE_BASE ** (-np.arange(HD // 2) * 2.0 / HD)
    angles = context * frequency
    cosine, sine = np.cos(angles), np.sin(angles)
    table = [np.tile(cosine, LANES // (HD // 2)), np.tile(np.concatenate([-sine, sine]), LANES // HD)]
    return np.stack(table + [np.zeros(LANES)] * 6).astype(np.float32)


def on_device(
    tokens,
    attend_gain,
    query_weight,
    cache_keys,
    cache_values,
    head_lambda,
    head_gain,
    output_weight,
    mixer_gain,
    gate_weight,
    up_weight,
    down_weight,
):
    kv_size = lax.axis_size("kv")
    seq_rows, features_here = tokens.shape
    features = features_here * kv_size
    heads = head_lambda.shape[0]
    positions = cache_keys.shape[1]
    rows = 2 * heads * seq_rows
    share = gate_weight.shape[1] // kv_size
    padded = -(-(2 * share + 2) // LANES) * LANES
    near = 2
    pairs = [[k, k + 1] for k in range(0, kv_size, 2)]
    extra = -(-TERMS * rows // near // PACKED // LANES) * LANES
    odd = jnp.broadcast_to((lax.axis_index("kv") & 1).astype(F32), (seq_rows, LANES))
    tokens, odd = lax.optimization_barrier((tokens, odd))
    keys = cache_keys.reshape(seq_rows, positions, 2 * HD)
    values = cache_values.reshape(seq_rows, positions, VD)
    width = query_weight.shape[1]

    def call(kernel, outs, here, hbm=(), scratch=(), last=False, cost=None):
        spec = pl.BlockSpec(memory_space=pltpu.VMEM)
        away = pl.BlockSpec(memory_space=pltpu.HBM)
        space = jax.ShapeDtypeStruct if last else pltpu.VMEM
        outs = tuple(space(shape, kind) for shape, kind in outs)
        here = [pltpu.with_memory_space_constraint(a, pltpu.VMEM) for a in here]
        hbm = [pltpu.with_memory_space_constraint(a, pltpu.HBM) for a in hbm]
        results = pl.pallas_call(
            kernel,
            out_shape=outs,
            in_specs=[spec] * len(here) + [away] * len(hbm),
            out_specs=(spec,) * len(outs),
            scratch_shapes=list(scratch),
            compiler_params=pltpu.CompilerParams(vmem_limit_bytes=KERNEL_VMEM),
            cost_estimate=cost,
        )(*here, *hbm)
        return results[0] if len(outs) == 1 else results

    def exchange(array, groups=None):
        return lax.all_to_all(array, "kv", 0, 0, axis_index_groups=groups, tiled=True)

    gain = attend_gain[None]
    table = jnp.asarray(rotation(positions * kv_size))
    part, table = call(
        query_kernel,
        [((seq_rows, width + LANES), BF16), (table.shape, F32)],
        [],
        [tokens, gain, query_weight, table],
        scratch=[
            pltpu.VMEM(tokens.shape, BF16),
            pltpu.VMEM(gain.shape, F32),
            pltpu.VMEM(query_weight.shape, BF16),
            pltpu.SemaphoreType.DMA((4,)),
        ],
    )
    sent = call(
        halves_kernel,
        [((kv_size, PACKED, seq_rows // PACKED * (width // 2) + LANES), BF16)],
        [odd, lax.all_gather(part, "kv", axis_index_groups=pairs)],
        cost=pl.CostEstimate(flops=10**9, bytes_accessed=10**7, transcendentals=0),
    )
    sent = call(
        functools.partial(attend_kernel, features),
        [((rows + EXTRA, VD), BF16)],
        [exchange(sent), table, keys, values],
        scratch=[
            pltpu.VMEM((seq_rows, width), F32),
            pltpu.VMEM((seq_rows, LANES), F32),
            pltpu.VMEM((heads * seq_rows, LANES), F32),
            pltpu.VMEM((rows, positions), F32),
        ],
    )
    sent = call(
        pair_kernel,
        [((kv_size, PACKED, rows // near // PACKED * VD + extra), BF16)],
        [odd, lax.all_gather(sent, "kv", axis_index_groups=pairs)],
        scratch=[pltpu.VMEM((rows // near, VD), F32)],
    )
    attended = call(
        functools.partial(heads_kernel, near),
        [((seq_rows, features_here), BF16)],
        [exchange(sent), head_lambda[None], head_gain[None], output_weight, mixer_gain[None]],
        scratch=[
            pltpu.VMEM((kv_size, rows // near, VD), F32),
            pltpu.VMEM((heads * seq_rows, VD), F32),
        ],
    )
    sent, middle = call(
        gate_kernel,
        [((kv_size, seq_rows, padded), BF16), ((seq_rows, features_here), BF16)],
        [
            lax.all_gather(attended, "tp", tiled=True),
            tokens,
            mixer_gain[None],
            gate_weight,
            up_weight,
        ],
    )
    sent = call(
        functools.partial(hidden_kernel, features, share),
        [((kv_size, PACKED, -(-(seq_rows // PACKED * share) // LANES) * LANES), BF16)],
        [exchange(sent)],
    )
    projected = call(
        functools.partial(down_kernel, share),
        [((seq_rows, features_here), BF16)],
        [exchange(sent), down_weight],
        scratch=[pltpu.VMEM((kv_size, seq_rows, -(-share // LANES) * LANES), F32)],
    )
    return call(
        final_kernel,
        [((seq_rows, features_here), BF16)],
        [lax.all_gather(projected, "tp", tiled=True), middle],
        last=True,
    )


def solution(mesh):
    return jax.shard_map(
        on_device,
        mesh=mesh,
        in_specs=(
            P(("grp", "dp"), "kv"),
            P("kv"),
            P("kv", "tp"),
            P(("grp", "dp"), "kv", "tp", None),
            P(("grp", "dp"), "kv", "tp", None),
            P("tp"),
            P(),
            P("tp", "kv"),
            P("kv"),
            P("kv", "tp"),
            P("kv", "tp"),
            P("tp", "kv"),
        ),
        out_specs=P(("grp", "dp"), "kv"),
        check_vma=False,
    )
```

```python
import functools

import jax
import jax.numpy as jnp
import numpy as np
from jax import lax
from jax.experimental import pallas as pl
from jax.experimental.pallas import tpu as pltpu
from jax.sharding import PartitionSpec as P

HD = 64
VD = 128
LANES = 128
PACKED = 2
TERMS = 3
EXTRA = 8

KERNEL_VMEM = 8 << 20

ROPE_BASE = 500000.0
EPSILON = 1e-06
KEEP_SCALE = 0.8
F32 = jnp.float32
BF16 = jnp.bfloat16


def split(value, terms):
    parts = []
    for _ in range(terms):
        part = value.astype(BF16).astype(F32)
        parts.append(part)
        value = value - part
    return parts


def lanes_of(columns, rows, width):
    lane = lax.broadcasted_iota(jnp.int32, (rows, width), 1)
    out = jnp.zeros((rows, width), F32)
    for k, column in enumerate(columns):
        out = jnp.where(lane == k, column, out)
    return out


def rows_of(lines, width):
    row = lax.broadcasted_iota(jnp.int32, (EXTRA, width), 0)
    out = jnp.zeros((EXTRA, width), F32)
    for k, line in enumerate(lines):
        out = jnp.where(row == k, line, out)
    return out


def turned(rows):
    pad = jnp.zeros((LANES - rows.shape[0], LANES), F32)
    return jnp.concatenate([rows, pad], axis=0).T


def query_kernel(tokens, gain, weight, table, out, table_here, *scratch):
    tokens_here, gain_here, weight_here, semaphores = scratch
    copies = [
        pltpu.make_async_copy(source, target, semaphores.at[k])
        for k, (source, target) in enumerate(
            (
                (weight, weight_here),
                (tokens, tokens_here),
                (gain, gain_here),
                (table, table_here),
            )
        )
    ]
    for copy in copies:
        copy.start()
    for copy in copies[:3]:
        copy.wait()
    tok = tokens_here[...].astype(F32)
    scaled = (tok * gain_here[...]).astype(BF16)
    partial = jnp.dot(scaled, weight_here[...], preferred_element_type=F32)
    squares = jnp.sum(tok * tok, axis=1, keepdims=True)
    seq_rows = tok.shape[0]
    lane = lax.broadcasted_iota(jnp.int32, (seq_rows, LANES), 1)
    at = lax.broadcasted_iota(jnp.int32, (seq_rows, LANES), 0) // PACKED * 2
    high, low = split(squares, 2)
    extra = jnp.where(lane == at, high, jnp.where(lane == at + 1, low, 0.0))
    pieces = [partial[r : r + PACKED] for r in range(0, seq_rows, PACKED)]
    pieces.append(sum(extra[r : r + PACKED] for r in range(0, seq_rows, PACKED)))
    sent = jnp.concatenate(pieces, axis=1).astype(BF16)
    for k in range(out.shape[0]):
        out[k] = sent
    for copy in copies[3:]:
        copy.wait()


def attend_kernel(features, parts, table, keys, values, out, query, squares, turned_query, score_rows):
    count = parts.shape[0]
    seq_rows, width = query.shape
    total = parts[0].astype(F32)
    for k in range(1, count):
        total = total + parts[k].astype(F32)
    extra = total[:, seq_rows // PACKED * width :]
    for r in range(seq_rows // PACKED):
        rows = slice(r * PACKED, (r + 1) * PACKED)
        query[rows] = total[:, r * width : (r + 1) * width]
        both = extra[:, 2 * r : 2 * r + 1] + extra[:, 2 * r + 1 : 2 * r + 2]
        squares[rows] = jnp.broadcast_to(both, (PACKED, LANES))
    scale = lax.rsqrt(squares[...] / features + EPSILON)
    heads = width // (2 * HD)
    lane = lax.broadcasted_iota(jnp.int32, (seq_rows, LANES), 1)
    first = lane % HD < HD // 2
    cosine, sine = table[0:1], table[1:2]
    for g in range(heads):
        part = query[:, g * LANES : (g + 1) * LANES] * scale
        other = jnp.where(first, pltpu.roll(part, LANES - HD // 2, 1), pltpu.roll(part, HD // 2, 1))
        turned_query[g * seq_rows : (g + 1) * seq_rows] = part * cosine + other * sine
    map_zero = lax.broadcasted_iota(jnp.int32, (heads, LANES), 1) < HD
    block = 2 * heads
    for s in range(seq_rows):
        part = turned_query[pl.ds(s, heads, stride=seq_rows)]
        both = jnp.concatenate(
            [jnp.where(map_zero, part, 0.0), jnp.where(map_zero, 0.0, part)], axis=0
        ).astype(BF16)
        score_rows[s * block : (s + 1) * block] = lax.dot_general(
            both, keys[s], (((1,), (1,)), ((), ())), preferred_element_type=F32
        )
    rows = block * seq_rows
    scores = score_rows[...] * HD ** (-0.5)
    row_max = jnp.max(scores, axis=1, keepdims=True)
    exponent = jnp.exp(scores - row_max)
    row_total = jnp.sum(exponent, axis=1, keepdims=True)
    weights = exponent.astype(BF16)
    both = lanes_of([row_max, row_total], rows, LANES).T
    out[rows:] = rows_of(split(both[0:1], 3) + split(both[1:2], 2), rows).astype(BF16)
    for s in range(seq_rows):
        out[s * block : (s + 1) * block] = jnp.dot(
            weights[s * block : (s + 1) * block], values[s], preferred_element_type=F32
        ).astype(BF16)


def maxima_of(parts, sources, rows):
    extra = [parts[k, rows:].astype(F32) for k in sources]
    maxima = jnp.concatenate([e[0:1] + e[1:2] + e[2:3] for e in extra], axis=0)
    totals = jnp.concatenate([e[3:4] + e[4:5] for e in extra], axis=0)
    return maxima, totals


def pair_kernel(odd, parts, out, joined):
    count = parts.shape[0]
    rows = parts.shape[1] - EXTRA
    half = rows // 2
    maxima, totals = maxima_of(parts, range(count), rows)
    joint = jnp.max(maxima, axis=0, keepdims=True)
    factors = jnp.exp(maxima - joint)
    total = jnp.sum(totals * factors, axis=0, keepdims=True)
    columns = turned(factors / total)
    both = jnp.zeros((rows, VD), F32)
    for k in range(count):
        both = both + parts[k, :rows].astype(F32) * columns[:, k : k + 1]
    joined[...] = jnp.where(odd[:1] > 0, both[half:], both[:half])
    lines = rows_of(split(joint + jnp.log(total), TERMS), VD)
    lines = jnp.where(odd[...] > 0, pltpu.roll(lines, VD - half, 1), lines)
    width = out.shape[2] - half // PACKED * VD
    lane = lax.broadcasted_iota(jnp.int32, (PACKED, width), 1)
    row = lax.broadcasted_iota(jnp.int32, (PACKED, width), 0)
    extra = jnp.zeros((PACKED, width), F32)
    for k in range(TERMS):
        at, slot = divmod(k * half, width)
        line = jnp.broadcast_to(lines[k : k + 1], (PACKED, VD))
        line = pltpu.roll(line, slot % VD, 1) if slot % VD else line
        line = jnp.concatenate([line] * (width // VD), axis=1)
        extra = jnp.where((row == at) & (lane >= slot) & (lane < slot + half), line, extra)
    pieces = [joined[r : r + PACKED] for r in range(0, half, PACKED)]
    sent = jnp.concatenate([*pieces, extra], axis=1).astype(BF16)
    for k in range(out.shape[0]):
        out[k] = sent


def heads_kernel(near, parts, lambdas, gain, weight, ahead, out, blocks, normed):
    count, quarter, _ = blocks.shape
    far = count // near
    heads = lambdas.shape[1]
    block = 2 * heads
    seq_rows = near * quarter // block
    square = (heads, heads)
    diagonal = lax.broadcasted_iota(jnp.int32, square, 0) == lax.broadcasted_iota(jnp.int32, square, 1)
    lambda_column = jnp.sum(jnp.where(diagonal, lambdas[...], 0.0), axis=1, keepdims=True)
    extra = []
    for j in [a * near + k for k in range(near) for a in range(far)]:
        part = parts[j].astype(F32)
        for r in range(quarter // PACKED):
            blocks[j, r * PACKED : (r + 1) * PACKED] = part[:, r * VD : (r + 1) * VD]
        extra.append(part[:, quarter // PACKED * VD :])
    extra = [jnp.concatenate([e[r : r + 1] for e in extra], axis=0) for r in range(PACKED)]
    lines = []
    width = extra[0].shape[1]
    for k in range(TERMS):
        at, slot = divmod(k * quarter, width)
        line = pltpu.roll(extra[at], width - slot, 1) if slot else extra[at]
        lines.append(line[:, :VD])
    exponents = lines[0] + lines[1] + lines[2]
    factors = []
    for k in range(near):
        own = exponents[k * far : (k + 1) * far]
        factor = jnp.exp(own - jnp.max(own, axis=0, keepdims=True))
        factors.append(factor / jnp.sum(factor, axis=0, keepdims=True))
    columns = turned(jnp.concatenate(factors, axis=0))
    for s in range(seq_rows):
        k, row = divmod(s * block, quarter)
        averaged = jnp.zeros((block, VD), F32)
        for a in range(far):
            part = blocks[a * near + k, row : row + block]
            at = k * far + a
            averaged = averaged + part * columns[row : row + block, at : at + 1]
        difference = averaged[:heads] - lambda_column * averaged[heads:]
        mean = jnp.mean(difference * difference, axis=1, keepdims=True)
        normed[s * heads : (s + 1) * heads] = (
            difference * lax.rsqrt(mean + EPSILON) * gain[...] * KEEP_SCALE
        )
    heads_out = jnp.concatenate(
        [normed[pl.ds(g, seq_rows, stride=heads)].astype(BF16) for g in range(heads)], axis=1
    )
    out[...] = jnp.dot(heads_out, weight[...], preferred_element_type=F32).astype(BF16)


def window(array, start, width):
    low = start // LANES * LANES
    tiles = -(-(start - low + width) // LANES) * LANES
    part = array[:, low : low + tiles]
    if start > low:
        part = pltpu.roll(part, tiles - (start - low), 1)
    return part


def gate_kernel(attended, tokens, gain, gate_weight, up_weight, out, middle):
    seq_rows = tokens.shape[0]
    total = attended[:seq_rows].astype(F32) + attended[seq_rows:].astype(F32)
    mid = (tokens[...].astype(F32) + total).astype(BF16)
    middle[...] = mid
    mid = mid.astype(F32)
    mixer_in = (mid * gain[...]).astype(BF16)
    gate = jnp.dot(mixer_in, gate_weight[...], preferred_element_type=F32)
    up = jnp.dot(mixer_in, up_weight[...], preferred_element_type=F32)
    squares = jnp.sum(mid * mid, axis=1, keepdims=True)
    high, low = split(squares, 2)
    count, _, width = out.shape
    share = gate.shape[1] // count
    lane = lax.broadcasted_iota(jnp.int32, (seq_rows, width), 1)
    for k in range(count):
        parts = []
        for array in (gate, up):
            part = window(array, k * share, share)[:, :width]
            if part.shape[1] < width:
                pad = jnp.zeros((seq_rows, width - part.shape[1]), F32)
                part = jnp.concatenate([part, pad], axis=1)
            parts.append(part)
        both = jnp.where(lane < share, parts[0], pltpu.roll(parts[1], share, 1))
        both = jnp.where(lane == 2 * share, high, both)
        both = jnp.where(lane == 2 * share + 1, low, both)
        out[k] = both.astype(BF16)


def hidden_kernel(features, share, parts, out):
    count, seq_rows, width = parts.shape
    total = parts[0].astype(F32)
    for k in range(1, count):
        total = total + parts[k].astype(F32)
    squares = total[:, 2 * share : 2 * share + 1] + total[:, 2 * share + 1 : 2 * share + 2]
    scale = lax.rsqrt(squares / features + EPSILON)
    scaled = total * scale
    tiles = -(-share // LANES) * LANES
    lane = lax.broadcasted_iota(jnp.int32, (seq_rows, tiles), 1)
    gate = jnp.where(lane < share, scaled[:, :tiles], 0.0)
    up = pltpu.roll(scaled, width - share, 1)[:, :tiles]
    hidden = gate / (1.0 + jnp.exp(-gate)) * up
    lanes = out.shape[2]
    hidden = jnp.concatenate([hidden, jnp.zeros((seq_rows, lanes - hidden.shape[1]), F32)], axis=1)
    sent = hidden[:PACKED]
    for r in range(1, seq_rows // PACKED):
        sent = sent + pltpu.roll(hidden[r * PACKED : (r + 1) * PACKED], r * share, 1)
    sent = sent.astype(BF16)
    for k in range(count):
        out[k] = sent


def down_kernel(share, hidden, weight, out, blocks):
    count, _, lanes = hidden.shape
    seq_rows, tiles = blocks.shape[1:]
    for k in range(count):
        part = hidden[k].astype(F32)
        for r in range(seq_rows // PACKED):
            moved = pltpu.roll(part, lanes - r * share, 1) if r else part
            blocks[k, r * PACKED : (r + 1) * PACKED] = moved[:, :tiles]
    total = jnp.zeros(out.shape, F32)
    for k in range(count):
        total = total + jnp.dot(
            blocks[k, :, :share].astype(BF16),
            weight[k * share : (k + 1) * share],
            preferred_element_type=F32,
        )
    out[...] = total.astype(BF16)


def final_kernel(parts, middle, out):
    seq_rows = middle.shape[0]
    mixed = parts[:seq_rows].astype(F32) + parts[seq_rows:].astype(F32)
    out[...] = (middle[...].astype(F32) + mixed).astype(BF16)


def rotation(context):
    frequency = ROPE_BASE ** (-np.arange(HD // 2) * 2.0 / HD)
    angles = context * frequency
    cosine, sine = np.cos(angles), np.sin(angles)
    table = [np.tile(cosine, LANES // (HD // 2)), np.tile(np.concatenate([-sine, sine]), LANES // HD)]
    return np.stack(table + [np.zeros(LANES)] * 6).astype(np.float32)


def on_device(
    tokens,
    attend_gain,
    query_weight,
    cache_keys,
    cache_values,
    head_lambda,
    head_gain,
    output_weight,
    mixer_gain,
    gate_weight,
    up_weight,
    down_weight,
):
    kv_size = lax.axis_size("kv")
    seq_rows, features_here = tokens.shape
    features = features_here * kv_size
    heads = head_lambda.shape[0]
    positions = cache_keys.shape[1]
    rows = 2 * heads * seq_rows
    share = gate_weight.shape[1] // kv_size
    padded = -(-(2 * share + 2) // LANES) * LANES
    near = 2
    pairs = [[k, k + 1] for k in range(0, kv_size, 2)]
    extra = -(-TERMS * rows // near // PACKED // LANES) * LANES
    odd = jnp.broadcast_to((lax.axis_index("kv") & 1).astype(F32), (seq_rows, LANES))
    tokens, odd = lax.optimization_barrier((tokens, odd))
    keys = cache_keys.reshape(seq_rows, positions, 2 * HD)
    values = cache_values.reshape(seq_rows, positions, VD)
    width = query_weight.shape[1]

    def call(kernel, outs, here, hbm=(), scratch=(), last=False, cost=None):
        spec = pl.BlockSpec(memory_space=pltpu.VMEM)
        away = pl.BlockSpec(memory_space=pltpu.HBM)
        space = jax.ShapeDtypeStruct if last else pltpu.VMEM
        outs = tuple(space(shape, kind) for shape, kind in outs)
        here = [pltpu.with_memory_space_constraint(a, pltpu.VMEM) for a in here]
        hbm = [pltpu.with_memory_space_constraint(a, pltpu.HBM) for a in hbm]
        results = pl.pallas_call(
            kernel,
            out_shape=outs,
            in_specs=[spec] * len(here) + [away] * len(hbm),
            out_specs=(spec,) * len(outs),
            scratch_shapes=list(scratch),
            compiler_params=pltpu.CompilerParams(vmem_limit_bytes=KERNEL_VMEM),
            cost_estimate=cost,
        )(*here, *hbm)
        return results[0] if len(outs) == 1 else results

    def exchange(array, groups=None):
        return lax.all_to_all(array, "kv", 0, 0, axis_index_groups=groups, tiled=True)

    gain = attend_gain[None]
    table = jnp.asarray(rotation(positions * kv_size))
    sent, table = call(
        query_kernel,
        [((kv_size, PACKED, seq_rows // PACKED * width + LANES), BF16), (table.shape, F32)],
        [],
        [tokens, gain, query_weight, table],
        scratch=[
            pltpu.VMEM(tokens.shape, BF16),
            pltpu.VMEM(gain.shape, F32),
            pltpu.VMEM(query_weight.shape, BF16),
            pltpu.SemaphoreType.DMA((4,)),
        ],
        cost=pl.CostEstimate(flops=10**9, bytes_accessed=10**7, transcendentals=0),
    )
    sent = call(
        functools.partial(attend_kernel, features),
        [((rows + EXTRA, VD), BF16)],
        [exchange(sent), table, keys, values],
        scratch=[
            pltpu.VMEM((seq_rows, width), F32),
            pltpu.VMEM((seq_rows, LANES), F32),
            pltpu.VMEM((heads * seq_rows, LANES), F32),
            pltpu.VMEM((rows, positions), F32),
        ],
    )
    sent = call(
        pair_kernel,
        [((kv_size, PACKED, rows // near // PACKED * VD + extra), BF16)],
        [odd, lax.all_gather(sent, "kv", axis_index_groups=pairs)],
        scratch=[pltpu.VMEM((rows // near, VD), F32)],
    )
    attended = call(
        functools.partial(heads_kernel, near),
        [((seq_rows, features_here), BF16)],
        [exchange(sent), head_lambda[None], head_gain[None], output_weight, mixer_gain[None]],
        scratch=[
            pltpu.VMEM((kv_size, rows // near, VD), F32),
            pltpu.VMEM((heads * seq_rows, VD), F32),
        ],
    )
    sent, middle = call(
        gate_kernel,
        [((kv_size, seq_rows, padded), BF16), ((seq_rows, features_here), BF16)],
        [
            lax.all_gather(attended, "tp", tiled=True),
            tokens,
            mixer_gain[None],
            gate_weight,
            up_weight,
        ],
    )
    sent = call(
        functools.partial(hidden_kernel, features, share),
        [((kv_size, PACKED, -(-(seq_rows // PACKED * share) // LANES) * LANES), BF16)],
        [exchange(sent)],
    )
    projected = call(
        functools.partial(down_kernel, share),
        [((seq_rows, features_here), BF16)],
        [exchange(sent), down_weight],
        scratch=[pltpu.VMEM((kv_size, seq_rows, -(-share // LANES) * LANES), F32)],
    )
    return call(
        final_kernel,
        [((seq_rows, features_here), BF16)],
        [lax.all_gather(projected, "tp", tiled=True), middle],
        last=True,
    )


def solution(mesh):
    return jax.shard_map(
        on_device,
        mesh=mesh,
        in_specs=(
            P(("grp", "dp"), "kv"),
            P("kv"),
            P("kv", "tp"),
            P(("grp", "dp"), "kv", "tp", None),
            P(("grp", "dp"), "kv", "tp", None),
            P("tp"),
            P(),
            P("tp", "kv"),
            P("kv"),
            P("kv", "tp"),
            P("kv", "tp"),
            P("tp", "kv"),
        ),
        out_specs=P(("grp", "dp"), "kv"),
        check_vma=False,
    )
```

```python
import functools

import jax
import jax.numpy as jnp
import numpy as np
from jax import lax
from jax.experimental import pallas as pl
from jax.experimental.pallas import tpu as pltpu
from jax.sharding import PartitionSpec as P

HD = 64
VD = 128
LANES = 128
PACKED = 2
TERMS = 3
EXTRA = 8

KERNEL_VMEM = 8 << 20

ROPE_BASE = 500000.0
EPSILON = 1e-06
KEEP_SCALE = 0.8
F32 = jnp.float32
BF16 = jnp.bfloat16


def split(value, terms):
    parts = []
    for _ in range(terms):
        part = value.astype(BF16).astype(F32)
        parts.append(part)
        value = value - part
    return parts


def lanes_of(columns, rows, width):
    lane = lax.broadcasted_iota(jnp.int32, (rows, width), 1)
    out = jnp.zeros((rows, width), F32)
    for k, column in enumerate(columns):
        out = jnp.where(lane == k, column, out)
    return out


def rows_of(lines, width):
    row = lax.broadcasted_iota(jnp.int32, (EXTRA, width), 0)
    out = jnp.zeros((EXTRA, width), F32)
    for k, line in enumerate(lines):
        out = jnp.where(row == k, line, out)
    return out


def turned(rows):
    pad = jnp.zeros((LANES - rows.shape[0], LANES), F32)
    return jnp.concatenate([rows, pad], axis=0).T


def query_kernel(tokens, gain, weight, table, out, table_here, *scratch):
    tokens_here, gain_here, weight_here, semaphores = scratch
    copies = [
        pltpu.make_async_copy(source, target, semaphores.at[k])
        for k, (source, target) in enumerate(
            (
                (weight, weight_here),
                (tokens, tokens_here),
                (gain, gain_here),
                (table, table_here),
            )
        )
    ]
    for copy in copies:
        copy.start()
    for copy in copies[:3]:
        copy.wait()
    tok = tokens_here[...].astype(F32)
    scaled = (tok * gain_here[...]).astype(BF16)
    partial = jnp.dot(scaled, weight_here[...], preferred_element_type=F32)
    squares = jnp.sum(tok * tok, axis=1, keepdims=True)
    width = partial.shape[1]
    out[:, :width] = partial.astype(BF16)
    out[:, width:] = lanes_of(split(squares, 2), tok.shape[0], LANES).astype(BF16)
    for copy in copies[3:]:
        copy.wait()


def halves_kernel(odd, parts, out):
    total = parts[0].astype(F32) + parts[1].astype(F32)
    half = (total.shape[1] - LANES) // 2
    own = jnp.where(odd[:, :1] > 0, total[:, half : 2 * half], total[:, :half])
    extra = total[:, 2 * half :]
    squares = extra[:, 0:1] + extra[:, 1:2]
    seq_rows = total.shape[0]
    lane = lax.broadcasted_iota(jnp.int32, (seq_rows, LANES), 1)
    at = lax.broadcasted_iota(jnp.int32, (seq_rows, LANES), 0) // PACKED * 2
    high, low = split(squares, 2)
    extra = jnp.where(lane == at, high, jnp.where(lane == at + 1, low, 0.0))
    pieces = [own[r : r + PACKED] for r in range(0, seq_rows, PACKED)]
    pieces.append(sum(extra[r : r + PACKED] for r in range(0, seq_rows, PACKED)))
    sent = jnp.concatenate(pieces, axis=1).astype(BF16)
    for k in range(out.shape[0]):
        out[k] = sent


def attend_kernel(features, parts, table, keys, values, out, query, squares, turned_query, score_rows):
    count = parts.shape[0]
    seq_rows, width = query.shape
    half = width // 2
    for odd in range(2):
        total = parts[odd].astype(F32)
        for k in range(odd + 2, count, 2):
            total = total + parts[k].astype(F32)
        for r in range(seq_rows // PACKED):
            rows = slice(r * PACKED, (r + 1) * PACKED)
            query[rows, odd * half : (odd + 1) * half] = total[:, r * half : (r + 1) * half]
            if odd == 0:
                extra = total[:, seq_rows // PACKED * half :]
                both = extra[:, 2 * r : 2 * r + 1] + extra[:, 2 * r + 1 : 2 * r + 2]
                squares[rows] = jnp.broadcast_to(both, (PACKED, LANES))
    scale = lax.rsqrt(squares[...] / features + EPSILON)
    heads = 2 * half // (2 * HD)
    lane = lax.broadcasted_iota(jnp.int32, (seq_rows, LANES), 1)
    first = lane % HD < HD // 2
    cosine, sine = table[0:1], table[1:2]
    for g in range(heads):
        part = query[:, g * LANES : (g + 1) * LANES] * scale
        other = jnp.where(first, pltpu.roll(part, LANES - HD // 2, 1), pltpu.roll(part, HD // 2, 1))
        turned_query[g * seq_rows : (g + 1) * seq_rows] = part * cosine + other * sine
    map_zero = lax.broadcasted_iota(jnp.int32, (heads, LANES), 1) < HD
    block = 2 * heads
    for s in range(seq_rows):
        part = turned_query[pl.ds(s, heads, stride=seq_rows)]
        both = jnp.concatenate(
            [jnp.where(map_zero, part, 0.0), jnp.where(map_zero, 0.0, part)], axis=0
        ).astype(BF16)
        score_rows[s * block : (s + 1) * block] = lax.dot_general(
            both, keys[s], (((1,), (1,)), ((), ())), preferred_element_type=F32
        )
    rows = block * seq_rows
    scores = score_rows[...] * HD ** (-0.5)
    row_max = jnp.max(scores, axis=1, keepdims=True)
    exponent = jnp.exp(scores - row_max)
    row_total = jnp.sum(exponent, axis=1, keepdims=True)
    weights = exponent.astype(BF16)
    both = lanes_of([row_max, row_total], rows, LANES).T
    out[rows:] = rows_of(split(both[0:1], 3) + split(both[1:2], 2), rows).astype(BF16)
    for s in range(seq_rows):
        out[s * block : (s + 1) * block] = jnp.dot(
            weights[s * block : (s + 1) * block], values[s], preferred_element_type=F32
        ).astype(BF16)


def maxima_of(parts, sources, rows):
    extra = [parts[k, rows:].astype(F32) for k in sources]
    maxima = jnp.concatenate([e[0:1] + e[1:2] + e[2:3] for e in extra], axis=0)
    totals = jnp.concatenate([e[3:4] + e[4:5] for e in extra], axis=0)
    return maxima, totals


def pair_kernel(odd, parts, out, joined):
    count = parts.shape[0]
    rows = parts.shape[1] - EXTRA
    half = rows // 2
    maxima, totals = maxima_of(parts, range(count), rows)
    joint = jnp.max(maxima, axis=0, keepdims=True)
    factors = jnp.exp(maxima - joint)
    total = jnp.sum(totals * factors, axis=0, keepdims=True)
    columns = turned(factors / total)
    both = jnp.zeros((rows, VD), F32)
    for k in range(count):
        both = both + parts[k, :rows].astype(F32) * columns[:, k : k + 1]
    joined[...] = jnp.where(odd[:1] > 0, both[half:], both[:half])
    lines = rows_of(split(joint + jnp.log(total), TERMS), VD)
    lines = jnp.where(odd[...] > 0, pltpu.roll(lines, VD - half, 1), lines)
    width = out.shape[2] - half // PACKED * VD
    lane = lax.broadcasted_iota(jnp.int32, (PACKED, width), 1)
    row = lax.broadcasted_iota(jnp.int32, (PACKED, width), 0)
    extra = jnp.zeros((PACKED, width), F32)
    for k in range(TERMS):
        at, slot = divmod(k * half, width)
        line = jnp.broadcast_to(lines[k : k + 1], (PACKED, VD))
        line = pltpu.roll(line, slot % VD, 1) if slot % VD else line
        line = jnp.concatenate([line] * (width // VD), axis=1)
        extra = jnp.where((row == at) & (lane >= slot) & (lane < slot + half), line, extra)
    pieces = [joined[r : r + PACKED] for r in range(0, half, PACKED)]
    sent = jnp.concatenate([*pieces, extra], axis=1).astype(BF16)
    for k in range(out.shape[0]):
        out[k] = sent


def heads_kernel(near, parts, lambdas, gain, weight, ahead, out, blocks, normed):
    count, quarter, _ = blocks.shape
    far = count // near
    heads = lambdas.shape[1]
    block = 2 * heads
    seq_rows = near * quarter // block
    square = (heads, heads)
    diagonal = lax.broadcasted_iota(jnp.int32, square, 0) == lax.broadcasted_iota(jnp.int32, square, 1)
    lambda_column = jnp.sum(jnp.where(diagonal, lambdas[...], 0.0), axis=1, keepdims=True)
    extra = []
    for j in [a * near + k for k in range(near) for a in range(far)]:
        part = parts[j].astype(F32)
        for r in range(quarter // PACKED):
            blocks[j, r * PACKED : (r + 1) * PACKED] = part[:, r * VD : (r + 1) * VD]
        extra.append(part[:, quarter // PACKED * VD :])
    extra = [jnp.concatenate([e[r : r + 1] for e in extra], axis=0) for r in range(PACKED)]
    lines = []
    width = extra[0].shape[1]
    for k in range(TERMS):
        at, slot = divmod(k * quarter, width)
        line = pltpu.roll(extra[at], width - slot, 1) if slot else extra[at]
        lines.append(line[:, :VD])
    exponents = lines[0] + lines[1] + lines[2]
    factors = []
    for k in range(near):
        own = exponents[k * far : (k + 1) * far]
        factor = jnp.exp(own - jnp.max(own, axis=0, keepdims=True))
        factors.append(factor / jnp.sum(factor, axis=0, keepdims=True))
    columns = turned(jnp.concatenate(factors, axis=0))
    for s in range(seq_rows):
        k, row = divmod(s * block, quarter)
        averaged = jnp.zeros((block, VD), F32)
        for a in range(far):
            part = blocks[a * near + k, row : row + block]
            at = k * far + a
            averaged = averaged + part * columns[row : row + block, at : at + 1]
        difference = averaged[:heads] - lambda_column * averaged[heads:]
        mean = jnp.mean(difference * difference, axis=1, keepdims=True)
        normed[s * heads : (s + 1) * heads] = (
            difference * lax.rsqrt(mean + EPSILON) * gain[...] * KEEP_SCALE
        )
    heads_out = jnp.concatenate(
        [normed[pl.ds(g, seq_rows, stride=heads)].astype(BF16) for g in range(heads)], axis=1
    )
    out[...] = jnp.dot(heads_out, weight[...], preferred_element_type=F32).astype(BF16)


def window(array, start, width):
    low = start // LANES * LANES
    tiles = -(-(start - low + width) // LANES) * LANES
    part = array[:, low : low + tiles]
    if start > low:
        part = pltpu.roll(part, tiles - (start - low), 1)
    return part


def gate_kernel(attended, tokens, gain, gate_weight, up_weight, out, middle):
    seq_rows = tokens.shape[0]
    total = attended[:seq_rows].astype(F32) + attended[seq_rows:].astype(F32)
    mid = (tokens[...].astype(F32) + total).astype(BF16)
    middle[...] = mid
    mid = mid.astype(F32)
    mixer_in = (mid * gain[...]).astype(BF16)
    gate = jnp.dot(mixer_in, gate_weight[...], preferred_element_type=F32)
    up = jnp.dot(mixer_in, up_weight[...], preferred_element_type=F32)
    squares = jnp.sum(mid * mid, axis=1, keepdims=True)
    high, low = split(squares, 2)
    count, _, width = out.shape
    share = gate.shape[1] // count
    lane = lax.broadcasted_iota(jnp.int32, (seq_rows, width), 1)
    for k in range(count):
        parts = []
        for array in (gate, up):
            part = window(array, k * share, share)[:, :width]
            if part.shape[1] < width:
                pad = jnp.zeros((seq_rows, width - part.shape[1]), F32)
                part = jnp.concatenate([part, pad], axis=1)
            parts.append(part)
        both = jnp.where(lane < share, parts[0], pltpu.roll(parts[1], share, 1))
        both = jnp.where(lane == 2 * share, high, both)
        both = jnp.where(lane == 2 * share + 1, low, both)
        out[k] = both.astype(BF16)


def hidden_kernel(features, share, parts, out):
    count, seq_rows, width = parts.shape
    total = parts[0].astype(F32)
    for k in range(1, count):
        total = total + parts[k].astype(F32)
    squares = total[:, 2 * share : 2 * share + 1] + total[:, 2 * share + 1 : 2 * share + 2]
    scale = lax.rsqrt(squares / features + EPSILON)
    scaled = total * scale
    tiles = -(-share // LANES) * LANES
    lane = lax.broadcasted_iota(jnp.int32, (seq_rows, tiles), 1)
    gate = jnp.where(lane < share, scaled[:, :tiles], 0.0)
    up = pltpu.roll(scaled, width - share, 1)[:, :tiles]
    hidden = gate / (1.0 + jnp.exp(-gate)) * up
    lanes = out.shape[2]
    hidden = jnp.concatenate([hidden, jnp.zeros((seq_rows, lanes - hidden.shape[1]), F32)], axis=1)
    sent = hidden[:PACKED]
    for r in range(1, seq_rows // PACKED):
        sent = sent + pltpu.roll(hidden[r * PACKED : (r + 1) * PACKED], r * share, 1)
    sent = sent.astype(BF16)
    for k in range(count):
        out[k] = sent


def down_kernel(share, hidden, weight, out, blocks):
    count, _, lanes = hidden.shape
    seq_rows, tiles = blocks.shape[1:]
    for k in range(count):
        part = hidden[k].astype(F32)
        for r in range(seq_rows // PACKED):
            moved = pltpu.roll(part, lanes - r * share, 1) if r else part
            blocks[k, r * PACKED : (r + 1) * PACKED] = moved[:, :tiles]
    total = jnp.zeros(out.shape, F32)
    for k in range(count):
        total = total + jnp.dot(
            blocks[k, :, :share].astype(BF16),
            weight[k * share : (k + 1) * share],
            preferred_element_type=F32,
        )
    out[...] = total.astype(BF16)


def rotation(context):
    frequency = ROPE_BASE ** (-np.arange(HD // 2) * 2.0 / HD)
    angles = context * frequency
    cosine, sine = np.cos(angles), np.sin(angles)
    table = [np.tile(cosine, LANES // (HD // 2)), np.tile(np.concatenate([-sine, sine]), LANES // HD)]
    return np.stack(table + [np.zeros(LANES)] * 6).astype(np.float32)


def on_device(
    tokens,
    attend_gain,
    query_weight,
    cache_keys,
    cache_values,
    head_lambda,
    head_gain,
    output_weight,
    mixer_gain,
    gate_weight,
    up_weight,
    down_weight,
):
    kv_size = lax.axis_size("kv")
    seq_rows, features_here = tokens.shape
    features = features_here * kv_size
    heads = head_lambda.shape[0]
    positions = cache_keys.shape[1]
    rows = 2 * heads * seq_rows
    share = gate_weight.shape[1] // kv_size
    padded = -(-(2 * share + 2) // LANES) * LANES
    near = 2
    pairs = [[k, k + 1] for k in range(0, kv_size, 2)]
    extra = -(-TERMS * rows // near // PACKED // LANES) * LANES
    odd = jnp.broadcast_to((lax.axis_index("kv") & 1).astype(F32), (seq_rows, LANES))
    tokens, odd = lax.optimization_barrier((tokens, odd))
    keys = cache_keys.reshape(seq_rows, positions, 2 * HD)
    values = cache_values.reshape(seq_rows, positions, VD)
    width = query_weight.shape[1]

    def call(kernel, outs, here, hbm=(), scratch=(), cost=None):
        spec = pl.BlockSpec(memory_space=pltpu.VMEM)
        away = pl.BlockSpec(memory_space=pltpu.HBM)
        outs = tuple(pltpu.VMEM(shape, kind) for shape, kind in outs)
        here = [pltpu.with_memory_space_constraint(a, pltpu.VMEM) for a in here]
        hbm = [pltpu.with_memory_space_constraint(a, pltpu.HBM) for a in hbm]
        results = pl.pallas_call(
            kernel,
            out_shape=outs,
            in_specs=[spec] * len(here) + [away] * len(hbm),
            out_specs=(spec,) * len(outs),
            scratch_shapes=list(scratch),
            compiler_params=pltpu.CompilerParams(vmem_limit_bytes=KERNEL_VMEM),
            cost_estimate=cost,
        )(*here, *hbm)
        return results[0] if len(outs) == 1 else results

    def exchange(array, groups=None):
        return lax.all_to_all(array, "kv", 0, 0, axis_index_groups=groups, tiled=True)

    gain = attend_gain[None]
    table = jnp.asarray(rotation(positions * kv_size))
    part, table = call(
        query_kernel,
        [((seq_rows, width + LANES), BF16), (table.shape, F32)],
        [],
        [tokens, gain, query_weight, table],
        scratch=[
            pltpu.VMEM(tokens.shape, BF16),
            pltpu.VMEM(gain.shape, F32),
            pltpu.VMEM(query_weight.shape, BF16),
            pltpu.SemaphoreType.DMA((4,)),
        ],
    )
    sent = call(
        halves_kernel,
        [((kv_size, PACKED, seq_rows // PACKED * (width // 2) + LANES), BF16)],
        [odd, lax.all_gather(part, "kv", axis_index_groups=pairs)],
        cost=pl.CostEstimate(flops=10**9, bytes_accessed=10**7, transcendentals=0),
    )
    sent = call(
        functools.partial(attend_kernel, features),
        [((rows + EXTRA, VD), BF16)],
        [exchange(sent), table, keys, values],
        scratch=[
            pltpu.VMEM((seq_rows, width), F32),
            pltpu.VMEM((seq_rows, LANES), F32),
            pltpu.VMEM((heads * seq_rows, LANES), F32),
            pltpu.VMEM((rows, positions), F32),
        ],
    )
    sent = call(
        pair_kernel,
        [((kv_size, PACKED, rows // near // PACKED * VD + extra), BF16)],
        [odd, lax.all_gather(sent, "kv", axis_index_groups=pairs)],
        scratch=[pltpu.VMEM((rows // near, VD), F32)],
    )
    attended = call(
        functools.partial(heads_kernel, near),
        [((seq_rows, features_here), BF16)],
        [exchange(sent), head_lambda[None], head_gain[None], output_weight, mixer_gain[None]],
        scratch=[
            pltpu.VMEM((kv_size, rows // near, VD), F32),
            pltpu.VMEM((heads * seq_rows, VD), F32),
        ],
    )
    sent, middle = call(
        gate_kernel,
        [((kv_size, seq_rows, padded), BF16), ((seq_rows, features_here), BF16)],
        [
            lax.all_gather(attended, "tp", tiled=True),
            tokens,
            mixer_gain[None],
            gate_weight,
            up_weight,
        ],
    )
    sent = call(
        functools.partial(hidden_kernel, features, share),
        [((kv_size, PACKED, -(-(seq_rows // PACKED * share) // LANES) * LANES), BF16)],
        [exchange(sent)],
    )
    projected = call(
        functools.partial(down_kernel, share),
        [((seq_rows, features_here), BF16)],
        [exchange(sent), down_weight],
        scratch=[pltpu.VMEM((kv_size, seq_rows, -(-share // LANES) * LANES), F32)],
    )
    mixed = lax.all_gather(projected, "tp").astype(F32).sum(axis=0)
    return (middle.astype(F32) + mixed).astype(BF16)


def solution(mesh):
    return jax.shard_map(
        on_device,
        mesh=mesh,
        in_specs=(
            P(("grp", "dp"), "kv"),
            P("kv"),
            P("kv", "tp"),
            P(("grp", "dp"), "kv", "tp", None),
            P(("grp", "dp"), "kv", "tp", None),
            P("tp"),
            P(),
            P("tp", "kv"),
            P("kv"),
            P("kv", "tp"),
            P("kv", "tp"),
            P("tp", "kv"),
        ),
        out_specs=P(("grp", "dp"), "kv"),
        check_vma=False,
    )
```

```python
import functools

import jax
import jax.numpy as jnp
import numpy as np
from jax import lax
from jax.experimental import pallas as pl
from jax.experimental.pallas import tpu as pltpu
from jax.sharding import PartitionSpec as P

HD = 64
VD = 128
LANES = 128
PACKED = 2
TERMS = 3
EXTRA = 8

KERNEL_VMEM = 8 << 20

ROPE_BASE = 500000.0
EPSILON = 1e-06
KEEP_SCALE = 0.8
F32 = jnp.float32
BF16 = jnp.bfloat16


def split(value, terms):
    parts = []
    for _ in range(terms):
        part = value.astype(BF16).astype(F32)
        parts.append(part)
        value = value - part
    return parts


def lanes_of(columns, rows, width):
    lane = lax.broadcasted_iota(jnp.int32, (rows, width), 1)
    out = jnp.zeros((rows, width), F32)
    for k, column in enumerate(columns):
        out = jnp.where(lane == k, column, out)
    return out


def rows_of(lines, width):
    row = lax.broadcasted_iota(jnp.int32, (EXTRA, width), 0)
    out = jnp.zeros((EXTRA, width), F32)
    for k, line in enumerate(lines):
        out = jnp.where(row == k, line, out)
    return out


def turned(rows):
    pad = jnp.zeros((LANES - rows.shape[0], LANES), F32)
    return jnp.concatenate([rows, pad], axis=0).T


def query_kernel(tokens, gain, weight, table, out, table_here, *scratch):
    tokens_here, gain_here, weight_here, semaphores = scratch
    copies = [
        pltpu.make_async_copy(source, target, semaphores.at[k])
        for k, (source, target) in enumerate(
            (
                (weight, weight_here),
                (tokens, tokens_here),
                (gain, gain_here),
                (table, table_here),
            )
        )
    ]
    for copy in copies:
        copy.start()
    for copy in copies[:3]:
        copy.wait()
    tok = tokens_here[...].astype(F32)
    scaled = (tok * gain_here[...]).astype(BF16)
    partial = jnp.dot(scaled, weight_here[...], preferred_element_type=F32)
    squares = jnp.sum(tok * tok, axis=1, keepdims=True)
    width = partial.shape[1]
    out[:, :width] = partial.astype(BF16)
    out[:, width:] = lanes_of(split(squares, 2), tok.shape[0], LANES).astype(BF16)
    for copy in copies[3:]:
        copy.wait()


def halves_kernel(odd, parts, out):
    total = parts[0].astype(F32) + parts[1].astype(F32)
    half = (total.shape[1] - LANES) // 2
    own = jnp.where(odd[:, :1] > 0, total[:, half : 2 * half], total[:, :half])
    extra = total[:, 2 * half :]
    squares = extra[:, 0:1] + extra[:, 1:2]
    seq_rows = total.shape[0]
    lane = lax.broadcasted_iota(jnp.int32, (seq_rows, LANES), 1)
    at = lax.broadcasted_iota(jnp.int32, (seq_rows, LANES), 0) // PACKED * 2
    high, low = split(squares, 2)
    extra = jnp.where(lane == at, high, jnp.where(lane == at + 1, low, 0.0))
    pieces = [own[r : r + PACKED] for r in range(0, seq_rows, PACKED)]
    pieces.append(sum(extra[r : r + PACKED] for r in range(0, seq_rows, PACKED)))
    sent = jnp.concatenate(pieces, axis=1).astype(BF16)
    for k in range(out.shape[0]):
        out[k] = sent


def attend_kernel(features, odd, parts, table, keys, values, out, kept, *scratch):
    query, squares, turned_query, score_rows = scratch
    count = parts.shape[0]
    seq_rows, width = query.shape
    half = width // 2
    for side in range(2):
        total = parts[side].astype(F32)
        for k in range(side + 2, count, 2):
            total = total + parts[k].astype(F32)
        for r in range(seq_rows // PACKED):
            rows = slice(r * PACKED, (r + 1) * PACKED)
            query[rows, side * half : (side + 1) * half] = total[:, r * half : (r + 1) * half]
            if side == 0:
                extra = total[:, seq_rows // PACKED * half :]
                both = extra[:, 2 * r : 2 * r + 1] + extra[:, 2 * r + 1 : 2 * r + 2]
                squares[rows] = jnp.broadcast_to(both, (PACKED, LANES))
    scale = lax.rsqrt(squares[...] / features + EPSILON)
    heads = 2 * half // (2 * HD)
    lane = lax.broadcasted_iota(jnp.int32, (seq_rows, LANES), 1)
    first = lane % HD < HD // 2
    cosine, sine = table[0:1], table[1:2]
    for g in range(heads):
        part = query[:, g * LANES : (g + 1) * LANES] * scale
        other = jnp.where(first, pltpu.roll(part, LANES - HD // 2, 1), pltpu.roll(part, HD // 2, 1))
        turned_query[g * seq_rows : (g + 1) * seq_rows] = part * cosine + other * sine
    map_zero = lax.broadcasted_iota(jnp.int32, (heads, LANES), 1) < HD
    block = 2 * heads
    for s in range(seq_rows):
        part = turned_query[pl.ds(s, heads, stride=seq_rows)]
        both = jnp.concatenate(
            [jnp.where(map_zero, part, 0.0), jnp.where(map_zero, 0.0, part)], axis=0
        ).astype(BF16)
        score_rows[s * block : (s + 1) * block] = lax.dot_general(
            both, keys[s], (((1,), (1,)), ((), ())), preferred_element_type=F32
        )
    rows = block * seq_rows
    scores = score_rows[...] * HD ** (-0.5)
    row_max = jnp.max(scores, axis=1, keepdims=True)
    exponent = jnp.exp(scores - row_max)
    row_total = jnp.sum(exponent, axis=1, keepdims=True)
    weights = exponent.astype(BF16)
    both = lanes_of([row_max, row_total], rows, LANES).T
    is_odd = odd[:1] > 0
    here, there = both[:EXTRA], pltpu.roll(both[:EXTRA], rows // 2, 1)
    there, here = jnp.where(is_odd, here, there), jnp.where(is_odd, there, here)
    out[rows // 2 :] = rows_of(split(there[0:1], 3) + split(there[1:2], 2), rows).astype(BF16)
    kept[rows // 2 :] = here
    for s in range(seq_rows // 2):
        early, late = (
            jnp.dot(weights[t * block : (t + 1) * block], values[t], preferred_element_type=F32)
            for t in (s, s + seq_rows // 2)
        )
        own = slice(s * block, (s + 1) * block)
        out[own] = jnp.where(is_odd, early, late).astype(BF16)
        kept[own] = jnp.where(is_odd, late, early)


def pair_kernel(odd, kept, parts, out, joined):
    half = kept.shape[0] - EXTRA
    other = jnp.where(odd[:1] > 0, parts[0].astype(F32), parts[1].astype(F32))
    extra = other[half:]
    maxima = [kept[half : half + 1], extra[0:1] + extra[1:2] + extra[2:3]]
    totals = [kept[half + 1 : half + 2], extra[3:4] + extra[4:5]]
    joint = jnp.maximum(maxima[0], maxima[1])
    factors = [jnp.exp(m - joint) for m in maxima]
    total = totals[0] * factors[0] + totals[1] * factors[1]
    columns = turned(rows_of([f / total for f in factors], VD))
    joined[...] = kept[:half] * columns[:half, 0:1] + other[:half] * columns[:half, 1:2]
    lines = rows_of(split(joint + jnp.log(total), TERMS), VD)
    width = out.shape[2] - half // PACKED * VD
    lane = lax.broadcasted_iota(jnp.int32, (PACKED, width), 1)
    row = lax.broadcasted_iota(jnp.int32, (PACKED, width), 0)
    extra = jnp.zeros((PACKED, width), F32)
    for k in range(TERMS):
        at, slot = divmod(k * half, width)
        line = jnp.broadcast_to(lines[k : k + 1], (PACKED, VD))
        line = pltpu.roll(line, slot % VD, 1) if slot % VD else line
        line = jnp.concatenate([line] * (width // VD), axis=1)
        extra = jnp.where((row == at) & (lane >= slot) & (lane < slot + half), line, extra)
    pieces = [joined[r : r + PACKED] for r in range(0, half, PACKED)]
    sent = jnp.concatenate([*pieces, extra], axis=1).astype(BF16)
    for k in range(out.shape[0]):
        out[k] = sent


def heads_kernel(near, parts, lambdas, gain, weight, ahead, out, blocks, normed):
    count, quarter, _ = blocks.shape
    far = count // near
    heads = lambdas.shape[1]
    block = 2 * heads
    seq_rows = near * quarter // block
    square = (heads, heads)
    diagonal = lax.broadcasted_iota(jnp.int32, square, 0) == lax.broadcasted_iota(jnp.int32, square, 1)
    lambda_column = jnp.sum(jnp.where(diagonal, lambdas[...], 0.0), axis=1, keepdims=True)
    extra = []
    for j in [a * near + k for k in range(near) for a in range(far)]:
        part = parts[j].astype(F32)
        for r in range(quarter // PACKED):
            blocks[j, r * PACKED : (r + 1) * PACKED] = part[:, r * VD : (r + 1) * VD]
        extra.append(part[:, quarter // PACKED * VD :])
    extra = [jnp.concatenate([e[r : r + 1] for e in extra], axis=0) for r in range(PACKED)]
    lines = []
    width = extra[0].shape[1]
    for k in range(TERMS):
        at, slot = divmod(k * quarter, width)
        line = pltpu.roll(extra[at], width - slot, 1) if slot else extra[at]
        lines.append(line[:, :VD])
    exponents = lines[0] + lines[1] + lines[2]
    factors = []
    for k in range(near):
        own = exponents[k * far : (k + 1) * far]
        factor = jnp.exp(own - jnp.max(own, axis=0, keepdims=True))
        factors.append(factor / jnp.sum(factor, axis=0, keepdims=True))
    columns = turned(jnp.concatenate(factors, axis=0))
    for s in range(seq_rows):
        k, row = divmod(s * block, quarter)
        averaged = jnp.zeros((block, VD), F32)
        for a in range(far):
            part = blocks[a * near + k, row : row + block]
            at = k * far + a
            averaged = averaged + part * columns[row : row + block, at : at + 1]
        difference = averaged[:heads] - lambda_column * averaged[heads:]
        mean = jnp.mean(difference * difference, axis=1, keepdims=True)
        normed[s * heads : (s + 1) * heads] = (
            difference * lax.rsqrt(mean + EPSILON) * gain[...] * KEEP_SCALE
        )
    heads_out = jnp.concatenate(
        [normed[pl.ds(g, seq_rows, stride=heads)].astype(BF16) for g in range(heads)], axis=1
    )
    out[...] = jnp.dot(heads_out, weight[...], preferred_element_type=F32).astype(BF16)


def window(array, start, width):
    low = start // LANES * LANES
    tiles = -(-(start - low + width) // LANES) * LANES
    part = array[:, low : low + tiles]
    if start > low:
        part = pltpu.roll(part, tiles - (start - low), 1)
    return part


def gate_kernel(attended, tokens, gain, gate_weight, up_weight, out, middle):
    seq_rows = tokens.shape[0]
    total = attended[:seq_rows].astype(F32) + attended[seq_rows:].astype(F32)
    mid = (tokens[...].astype(F32) + total).astype(BF16)
    middle[...] = mid
    mid = mid.astype(F32)
    mixer_in = (mid * gain[...]).astype(BF16)
    gate = jnp.dot(mixer_in, gate_weight[...], preferred_element_type=F32)
    up = jnp.dot(mixer_in, up_weight[...], preferred_element_type=F32)
    squares = jnp.sum(mid * mid, axis=1, keepdims=True)
    high, low = split(squares, 2)
    count, _, width = out.shape
    share = gate.shape[1] // count
    lane = lax.broadcasted_iota(jnp.int32, (seq_rows, width), 1)
    for k in range(count):
        parts = []
        for array in (gate, up):
            part = window(array, k * share, share)[:, :width]
            if part.shape[1] < width:
                pad = jnp.zeros((seq_rows, width - part.shape[1]), F32)
                part = jnp.concatenate([part, pad], axis=1)
            parts.append(part)
        both = jnp.where(lane < share, parts[0], pltpu.roll(parts[1], share, 1))
        both = jnp.where(lane == 2 * share, high, both)
        both = jnp.where(lane == 2 * share + 1, low, both)
        out[k] = both.astype(BF16)


def hidden_kernel(features, share, parts, out):
    count, seq_rows, width = parts.shape
    total = parts[0].astype(F32)
    for k in range(1, count):
        total = total + parts[k].astype(F32)
    squares = total[:, 2 * share : 2 * share + 1] + total[:, 2 * share + 1 : 2 * share + 2]
    scale = lax.rsqrt(squares / features + EPSILON)
    scaled = total * scale
    tiles = -(-share // LANES) * LANES
    lane = lax.broadcasted_iota(jnp.int32, (seq_rows, tiles), 1)
    gate = jnp.where(lane < share, scaled[:, :tiles], 0.0)
    up = pltpu.roll(scaled, width - share, 1)[:, :tiles]
    hidden = gate / (1.0 + jnp.exp(-gate)) * up
    lanes = out.shape[2]
    hidden = jnp.concatenate([hidden, jnp.zeros((seq_rows, lanes - hidden.shape[1]), F32)], axis=1)
    sent = hidden[:PACKED]
    for r in range(1, seq_rows // PACKED):
        sent = sent + pltpu.roll(hidden[r * PACKED : (r + 1) * PACKED], r * share, 1)
    sent = sent.astype(BF16)
    for k in range(count):
        out[k] = sent


def down_kernel(share, hidden, weight, out, blocks):
    count, _, lanes = hidden.shape
    seq_rows, tiles = blocks.shape[1:]
    for k in range(count):
        part = hidden[k].astype(F32)
        for r in range(seq_rows // PACKED):
            moved = pltpu.roll(part, lanes - r * share, 1) if r else part
            blocks[k, r * PACKED : (r + 1) * PACKED] = moved[:, :tiles]
    total = jnp.zeros(out.shape, F32)
    for k in range(count):
        total = total + jnp.dot(
            blocks[k, :, :share].astype(BF16),
            weight[k * share : (k + 1) * share],
            preferred_element_type=F32,
        )
    out[...] = total.astype(BF16)


def rotation(context):
    frequency = ROPE_BASE ** (-np.arange(HD // 2) * 2.0 / HD)
    angles = context * frequency
    cosine, sine = np.cos(angles), np.sin(angles)
    table = [np.tile(cosine, LANES // (HD // 2)), np.tile(np.concatenate([-sine, sine]), LANES // HD)]
    return np.stack(table + [np.zeros(LANES)] * 6).astype(np.float32)


def on_device(
    tokens,
    attend_gain,
    query_weight,
    cache_keys,
    cache_values,
    head_lambda,
    head_gain,
    output_weight,
    mixer_gain,
    gate_weight,
    up_weight,
    down_weight,
):
    kv_size = lax.axis_size("kv")
    seq_rows, features_here = tokens.shape
    features = features_here * kv_size
    heads = head_lambda.shape[0]
    positions = cache_keys.shape[1]
    rows = 2 * heads * seq_rows
    share = gate_weight.shape[1] // kv_size
    padded = -(-(2 * share + 2) // LANES) * LANES
    near = 2
    pairs = [[k, k + 1] for k in range(0, kv_size, 2)]
    extra = -(-TERMS * rows // near // PACKED // LANES) * LANES
    odd = jnp.broadcast_to((lax.axis_index("kv") & 1).astype(F32), (seq_rows, LANES))
    tokens, odd = lax.optimization_barrier((tokens, odd))
    keys = cache_keys.reshape(seq_rows, positions, 2 * HD)
    values = cache_values.reshape(seq_rows, positions, VD)
    width = query_weight.shape[1]

    def call(kernel, outs, here, hbm=(), scratch=(), cost=None):
        spec = pl.BlockSpec(memory_space=pltpu.VMEM)
        away = pl.BlockSpec(memory_space=pltpu.HBM)
        outs = tuple(pltpu.VMEM(shape, kind) for shape, kind in outs)
        here = [pltpu.with_memory_space_constraint(a, pltpu.VMEM) for a in here]
        hbm = [pltpu.with_memory_space_constraint(a, pltpu.HBM) for a in hbm]
        results = pl.pallas_call(
            kernel,
            out_shape=outs,
            in_specs=[spec] * len(here) + [away] * len(hbm),
            out_specs=(spec,) * len(outs),
            scratch_shapes=list(scratch),
            compiler_params=pltpu.CompilerParams(vmem_limit_bytes=KERNEL_VMEM),
            cost_estimate=cost,
        )(*here, *hbm)
        return results[0] if len(outs) == 1 else results

    def exchange(array, groups=None):
        return lax.all_to_all(array, "kv", 0, 0, axis_index_groups=groups, tiled=True)

    gain = attend_gain[None]
    table = jnp.asarray(rotation(positions * kv_size))
    part, table = call(
        query_kernel,
        [((seq_rows, width + LANES), BF16), (table.shape, F32)],
        [],
        [tokens, gain, query_weight, table],
        scratch=[
            pltpu.VMEM(tokens.shape, BF16),
            pltpu.VMEM(gain.shape, F32),
            pltpu.VMEM(query_weight.shape, BF16),
            pltpu.SemaphoreType.DMA((4,)),
        ],
    )
    sent = call(
        halves_kernel,
        [((kv_size, PACKED, seq_rows // PACKED * (width // 2) + LANES), BF16)],
        [odd, lax.all_gather(part, "kv", axis_index_groups=pairs)],
        cost=pl.CostEstimate(flops=10**9, bytes_accessed=10**7, transcendentals=0),
    )
    sent, kept = call(
        functools.partial(attend_kernel, features),
        [((rows // near + EXTRA, VD), kind) for kind in (BF16, F32)],
        [odd, exchange(sent), table, keys, values],
        scratch=[
            pltpu.VMEM((seq_rows, width), F32),
            pltpu.VMEM((seq_rows, LANES), F32),
            pltpu.VMEM((heads * seq_rows, LANES), F32),
            pltpu.VMEM((rows, positions), F32),
        ],
    )
    sent = call(
        pair_kernel,
        [((kv_size, PACKED, rows // near // PACKED * VD + extra), BF16)],
        [odd, kept, lax.all_gather(sent, "kv", axis_index_groups=pairs)],
        scratch=[pltpu.VMEM((rows // near, VD), F32)],
    )
    attended = call(
        functools.partial(heads_kernel, near),
        [((seq_rows, features_here), BF16)],
        [exchange(sent), head_lambda[None], head_gain[None], output_weight, mixer_gain[None]],
        scratch=[
            pltpu.VMEM((kv_size, rows // near, VD), F32),
            pltpu.VMEM((heads * seq_rows, VD), F32),
        ],
    )
    sent, middle = call(
        gate_kernel,
        [((kv_size, seq_rows, padded), BF16), ((seq_rows, features_here), BF16)],
        [
            lax.all_gather(attended, "tp", tiled=True),
            tokens,
            mixer_gain[None],
            gate_weight,
            up_weight,
        ],
    )
    sent = call(
        functools.partial(hidden_kernel, features, share),
        [((kv_size, PACKED, -(-(seq_rows // PACKED * share) // LANES) * LANES), BF16)],
        [exchange(sent)],
    )
    projected = call(
        functools.partial(down_kernel, share),
        [((seq_rows, features_here), BF16)],
        [exchange(sent), down_weight],
        scratch=[pltpu.VMEM((kv_size, seq_rows, -(-share // LANES) * LANES), F32)],
    )
    mixed = lax.all_gather(projected, "tp").astype(F32).sum(axis=0)
    return (middle.astype(F32) + mixed).astype(BF16)


def solution(mesh):
    return jax.shard_map(
        on_device,
        mesh=mesh,
        in_specs=(
            P(("grp", "dp"), "kv"),
            P("kv"),
            P("kv", "tp"),
            P(("grp", "dp"), "kv", "tp", None),
            P(("grp", "dp"), "kv", "tp", None),
            P("tp"),
            P(),
            P("tp", "kv"),
            P("kv"),
            P("kv", "tp"),
            P("kv", "tp"),
            P("tp", "kv"),
        ),
        out_specs=P(("grp", "dp"), "kv"),
        check_vma=False,
    )
```
